32 devices in a mesh: ep: 4 (over y, x), tp: 8 (over z, core).
Axes of the slice: x: 2, y: 2, z: 4, core: 2. Of those that a mesh axis runs over, the one named last changes fastest.
Arguments:
- mixer_in: bfloat16 [8192, 2048], P(('ep', 'tp')), may hold values from -6 to 6
- pre_gain: float32 [2048], replicated, may hold values from 0.1 to 1.9
- glu_value: bfloat16 [2048, 1024], P(None, 'tp'), may hold values from -0.125 to 0.125
- glu_gate: bfloat16 [2048, 1024], P(None, 'tp'), may hold values from -0.125 to 0.125
- conv_kernel: float32 [31, 1024], replicated, may hold values from -1 to 1
- chan_gain: float32 [1024], replicated, may hold values from 0.1 to 1.9
- out_weight: bfloat16 [1024, 2048], P(None, 'tp'), may hold values from -0.1875 to 0.1875
- mix_gain: float32 [2048], replicated, may hold values from 0.1 to 1.9
- expert_in: bfloat16 [1024, 2048], P(('ep', 'tp')), may hold values from -6 to 6
- ffn_gain: float32 [2048], replicated, may hold values from 0.1 to 1.9
- routing: int32 [1024, 2], P(('ep', 'tp')), may hold values from 0 to 7, all different within a row; in each aligned block of 32 rows (0 to 31, 32 to 63, ...) at most 12 rows name the same one
- route_weight: float32 [1024, 2], P(('ep', 'tp')), may hold values from 0.1 to 1
- gate_proj: bfloat16 [8, 2048, 4096], P('ep', None, 'tp'), may hold values from -0.375 to 0.375
- up_proj: bfloat16 [8, 2048, 4096], P('ep', None, 'tp'), may hold values from -0.375 to 0.375
- down_proj: bfloat16 [8, 4096, 2048], P('ep', 'tp'), may hold values from -0.09375 to 0.09375
- expert_gain: float32 [2048], replicated, may hold values from 0.1 to 1.9
Outputs:
- mixed: bfloat16 [8192, 2048], P(('ep', 'tp'))
- routed: bfloat16 [1024, 2048], P(('ep', 'tp'))
The draws below stay inside these ranges and needn't reach their ends.
Inputs may be any that keep to these rules, and one draw needn't show every extreme that they name: `routing`: each row names 2 different experts; in each aligned block of 32 rows (the rows of one device) no expert is named more than 12 times.
All inputs are finite; a program needn't handle non-finite values.
Results may differ from the reference program's by a relative error of at most 0.02.
Values may be sent and summed in bfloat16 or wider, within the bound.
A program may use at most 128 MiB of HBM per device.

```python
import math
import jax
import jax.numpy as jnp
import numpy as np
from jax import lax

D = 2048
C = 1024
FF = 4096
KERNEL = 31
TOPK = 2
SLICE = 32
EXPERTS = 8
CAPS = 12
TOKENS1 = 8192
TOKENS2 = 1024
N_EP = 4
N_TP = 8


def levels(own_key, extent, cuts, low, top_value):
    gain, own = 1.0, jax.random.fold_in(own_key, 6)
    for dim, parts in cuts:
        steps = jnp.exp(jax.random.uniform(jax.random.fold_in(own, dim), (parts,), jnp.float32, low / len(cuts), top_value / len(cuts)))
        gain = gain * jnp.repeat(steps, extent[dim] // parts).reshape([-1 if axis == dim else 1 for axis in range(len(extent))])
    return gain


def assign_block(stream_key, own, number, rows, amount, top, limit, skew):
    sequence = jax.random.permutation(stream_key, amount)
    crowded, ordinary = portions_of(amount, rows * top, limit, skew, True), portions_of(amount, rows * top, limit, skew, False)
    places = jnp.arange(amount)

    def named(lengths, offset_by):
        used = int((lengths > 0).sum())
        fixed = max(1, used // 4)
        passed = fixed + (places - fixed + offset_by * (used - fixed)) % max(1, amount - fixed)
        return jnp.zeros((amount,), jnp.int32).at[sequence[jnp.where(places < fixed, places, passed)]].set(jnp.asarray(lengths, jnp.int32))

    lengths = jnp.where(number % 4 == 0, named(crowded, number // 4), named(ordinary, number - number // 4 - 1))
    mixed = jax.random.permutation(jax.random.fold_in(own, 3), amount)
    giver, taker = mixed[0:amount // 2 * 2:2], mixed[1:amount // 2 * 2:2]
    room = jnp.minimum(lengths[giver] - 1, limit - lengths[taker]) // 2
    room = jnp.where((giver == sequence[0]) | (taker == sequence[0]) | (lengths[taker] == 0), 0, jnp.maximum(room, 0))
    passed = jax.random.randint(jax.random.fold_in(own, 4), (amount // 2,), 0, 1 << 20) % (room + 1)
    lengths = lengths.at[giver].add(-passed).at[taker].add(passed)
    items = jnp.searchsorted(jnp.cumsum(lengths), jnp.arange(rows * top), side="right").astype(jnp.int32)
    table = items.reshape(top, rows).T
    table = table[jax.random.permutation(jax.random.fold_in(own, 1), rows)]
    offset_by = jax.random.randint(jax.random.fold_in(own, 2), (rows, 1), 0, top)
    return jnp.take_along_axis(table, (jnp.arange(top)[None, :] + offset_by) % top, axis=1)


def portions_of(count, total, limit, skew, full):
    portions = [(1 << 20) // math.isqrt(grade ** skew) + 1 for grade in range(1, count + 1)]
    largest = limit if full else min(limit, max(-(-total // count), total * portions[0] // sum(portions)))
    least = 1 if total - largest >= count - 1 else 0
    counts, surplus = [largest] + [least] * (count - 1), total - largest - least * (count - 1)
    while surplus > 0:
        candidates = [i for i in range(1, count) if counts[i] < largest] or [i for i in range(1, count) if counts[i] < limit]
        whole, remaining = sum([portions[i] for i in candidates]), surplus
        for i in candidates:
            extra = min(limit - counts[i], max(1, remaining * portions[i] // whole), surplus)
            counts[i] = counts[i] + extra
            surplus = surplus - extra
    return np.array(counts)


def normal_values(own_key, dims, deviation, bound, pieces=(), kind=jnp.bfloat16):
    gain = levels(own_key, dims, pieces, -0.22, 0.18) if pieces else 1.0
    array = jax.random.normal(own_key, dims, jnp.float32) * deviation * gain
    return jnp.minimum(jnp.maximum(array, -bound), bound).astype(kind)


def setup_inputs(seed: int = 0) -> dict:
    splits = jax.random.split(jax.random.key(seed), 17)
    mixer_in = normal_values(splits[0], (TOKENS1, D), 1.0, 6.0, ((0, 32),))
    pre_gain = jnp.clip(1.0 + 0.18 * jax.random.normal(splits[1], (D,), jnp.float32), 0.1, 1.9)
    glu_value = normal_values(splits[2], (D, C), D ** -0.5, 0.125, ((1, 8),))
    glu_gate = normal_values(splits[3], (D, C), D ** -0.5, 0.125, ((1, 8),))
    conv_kernel = normal_values(splits[4], (KERNEL, C), KERNEL ** -0.5, 1.0, (), jnp.float32)
    chan_gain = jnp.clip(1.0 + 0.18 * jax.random.normal(splits[5], (C,), jnp.float32), 0.1, 1.9)
    out_weight = normal_values(splits[6], (C, D), C ** -0.5, 0.1875, ((1, 8),))
    mix_gain = jnp.clip(1.0 + 0.18 * jax.random.normal(splits[7], (D,), jnp.float32), 0.1, 1.9)
    expert_in = normal_values(splits[8], (TOKENS2, D), 1.0, 6.0, ((0, 32),))
    ffn_gain = jnp.clip(1.0 + 0.18 * jax.random.normal(splits[9], (D,), jnp.float32), 0.1, 1.9)
    routing_keys = jax.random.split(jax.random.fold_in(splits[10], 1), TOKENS2 // SLICE)
    routing_turns = jax.random.permutation(jax.random.fold_in(splits[10], 3), TOKENS2 // SLICE)
    routing = jax.vmap(lambda own, number: assign_block(jax.random.fold_in(splits[10], 2), own, number, SLICE, EXPERTS, TOPK, CAPS, 2))(routing_keys, routing_turns).reshape((TOKENS2, TOPK))
    route_weight = jnp.clip(0.1 + 0.9 * jax.random.uniform(splits[11], (TOKENS2, TOPK), jnp.float32) ** levels(splits[11], (TOKENS2, TOPK), ((0, 32),), -0.2, 0.2), 0.1, 1.0)
    gate_proj = normal_values(splits[12], (EXPERTS, D, FF), (D // 9) ** -0.5, 0.375, ((0, 4), (2, 8)))
    up_proj = normal_values(splits[13], (EXPERTS, D, FF), (D // 9) ** -0.5, 0.375, ((0, 4), (2, 8)))
    down_proj = normal_values(splits[14], (EXPERTS, FF, D), FF ** -0.5, 0.09375, ((0, 4), (1, 8)))
    expert_gain = jnp.clip(1.0 + 0.18 * jax.random.normal(splits[15], (D,), jnp.float32), 0.1, 1.9)
    return dict(mixer_in=mixer_in, pre_gain=pre_gain, glu_value=glu_value, glu_gate=glu_gate, conv_kernel=conv_kernel, chan_gain=chan_gain, out_weight=out_weight, mix_gain=mix_gain, expert_in=expert_in, ffn_gain=ffn_gain, routing=routing, route_weight=route_weight, gate_proj=gate_proj, up_proj=up_proj, down_proj=down_proj, expert_gain=expert_gain)


RMS_EPSILON = 1e-06
LAYER_EPSILON = 1e-05
CLAMP_LIMIT = 7.0
SWISH_ALPHA = 1.702

def rms_scale(values, gain_row):
    values = values.astype(jnp.float32)
    return values * lax.rsqrt(lax.optimization_barrier(jnp.mean(values * values, axis=-1, keepdims=True)) + RMS_EPSILON) * gain_row

def conv_mixer(mixer_in, pre_gain, glu_value, glu_gate, conv_kernel, chan_gain, out_weight, mix_gain):
    normed = rms_scale(mixer_in, pre_gain).astype(jnp.bfloat16)
    value_pre = jnp.dot(normed, glu_value, preferred_element_type=jnp.float32)
    gate_pre = jnp.dot(normed, glu_gate, preferred_element_type=jnp.float32)
    gated_rows = (value_pre * jax.nn.sigmoid(gate_pre)).astype(jnp.bfloat16)
    length = gated_rows.shape[0]
    padded = jnp.pad(gated_rows.astype(jnp.float32), ((KERNEL - 1, 0), (0, 0)))
    conv_sum = jnp.zeros((length, gated_rows.shape[1]), jnp.float32)
    for offset in range(KERNEL):
        conv_sum = conv_sum + conv_kernel[offset] * padded[offset:offset + length]
    row_mean = lax.optimization_barrier(jnp.mean(conv_sum, axis=-1, keepdims=True))
    centred = conv_sum - row_mean
    row_var = lax.optimization_barrier(jnp.mean(centred * centred, axis=-1, keepdims=True))
    activated = jax.nn.silu(centred * lax.rsqrt(row_var + LAYER_EPSILON) * chan_gain).astype(jnp.bfloat16)
    projected = jnp.dot(activated, out_weight, preferred_element_type=jnp.float32)
    return rms_scale(projected, mix_gain).astype(jnp.bfloat16)

def expert_layer(expert_in, ffn_gain, routing, route_weight, gate_proj, up_proj, down_proj, expert_gain):
    normed = rms_scale(expert_in, ffn_gain).astype(jnp.bfloat16)
    flat_route = routing.reshape(-1)
    flat_weight = route_weight.reshape(-1)
    capacity = N_EP * N_TP * CAPS
    hidden = gate_proj.shape[2] // N_TP

    def one_expert(running, expert):
        matches = flat_route == expert
        entry_index = jnp.nonzero(matches, size=capacity, fill_value=0)[0].astype(jnp.int32)
        live_count = jnp.sum(matches.astype(jnp.int32))
        live_slot = jnp.arange(capacity, dtype=jnp.int32) < live_count
        token_index = (entry_index // TOPK).astype(jnp.int32)
        row_block = normed[token_index]
        gate_pre = jnp.dot(row_block, gate_proj[expert], preferred_element_type=jnp.float32)
        up_pre = jnp.dot(row_block, up_proj[expert], preferred_element_type=jnp.float32)
        gate_pre = jnp.minimum(gate_pre, CLAMP_LIMIT)
        up_pre = jnp.clip(up_pre, -CLAMP_LIMIT, CLAMP_LIMIT)
        hidden_act = ((up_pre + 1.0) * gate_pre * jax.nn.sigmoid(SWISH_ALPHA * gate_pre)).astype(jnp.bfloat16)
        blocks = hidden_act.reshape(capacity, N_TP, hidden).astype(jnp.float32)
        down_block = down_proj[expert].reshape(N_TP, hidden, -1).astype(jnp.float32)
        partial_value = jnp.einsum('rnf,nfd->nrd', blocks, down_block).astype(jnp.bfloat16)
        expert_out = lax.optimization_barrier(jnp.sum(partial_value.astype(jnp.float32), axis=0)).astype(jnp.bfloat16)
        slot_weight = jnp.where(live_slot, flat_weight[entry_index], 0.0)
        running = running.at[token_index].add(slot_weight[:, None] * expert_out.astype(jnp.float32))
        return (running, None)
    start_sum = jnp.zeros(expert_in.shape, jnp.float32)
    combined, unused = lax.scan(one_expert, start_sum, jnp.arange(EXPERTS, dtype=jnp.int32))
    return rms_scale(combined, expert_gain).astype(jnp.bfloat16)

def reference(mixer_in, pre_gain, glu_value, glu_gate, conv_kernel, chan_gain, out_weight, mix_gain, expert_in, ffn_gain, routing, route_weight, gate_proj, up_proj, down_proj, expert_gain):
    mixed = conv_mixer(mixer_in, pre_gain, glu_value, glu_gate, conv_kernel, chan_gain, out_weight, mix_gain)
    routed = expert_layer(expert_in, ffn_gain, routing, route_weight, gate_proj, up_proj, down_proj, expert_gain)
    return (mixed, routed)
```

```python
import functools

import jax
import jax.numpy as jnp
from jax import lax
from jax.experimental import pallas as pl
from jax.experimental.pallas import tpu as pltpu
from jax.sharding import PartitionSpec as P

RMS_EPSILON = 1e-06
LAYER_EPSILON = 1e-05
CLAMP_LIMIT = 7.0
SWISH_ALPHA = 1.702


def passed_along(value, axis, steps):
    count = lax.axis_size(axis)
    initial, last = (max(0, -steps), min(count, count - steps))
    return lax.ppermute(value, axis, [(source, source + steps) for source in range(initial, last)])


def rms_scale(values, gain_row):
    values = values.astype(jnp.float32)
    return (
        values
        * lax.rsqrt(jnp.mean(values * values, axis=-1, keepdims=True) + RMS_EPSILON)
        * gain_row
    )


def columns(ref, owner, width, rows):
    if len(ref.shape) == 3:
        return ref.at[owner, rows, :]
    return ref.at[rows, pl.ds(pl.multiple_of(owner * width, width), width)]


def exchange_kernel(
    groups_ep,
    groups_tp,
    capacity,
    inside,
    outgoing,
    mixer_in,
    pre_gain,
    conv_kernel,
    chan_gain,
    mix_gain,
    value_own,
    gate_own,
    out_own,
    gate_hbm,
    up_hbm,
    down_hbm,
    *rest,
):
    if inside:
        mixed, returned, value_full, gate_full, out_full, *rest = rest
        normed, padded, conv, act, projected, *rest = rest
    else:
        value_full, gate_full, out_full, returned, *rest = rest
    (
    rows_all,
    hidden,
    partial,
    pair_in,
    ring_in,
    back_out,
    back_in,
    gate_vmem,
    up_vmem,
    down_vmem,
    load_sem,
    stage_sem,
    send_h,
    recv_h,
    own_sem,
    send_a,
    recv_a,
    send_r,
    recv_r,
    send_rp,
    recv_rp,
    send_w1,
    recv_w1,
    send_w2,
    recv_w2,
    send_wp,
    recv_wp,
    send_p,
    recv_p,
    send_z,
    recv_z,
    send_b,
    recv_b,
    ) = rest
    q = lax.axis_index("ep")
    t = lax.axis_index("tp")
    chips = groups_tp // 2
    z, core = t // 2, t % 2
    partner = z * 2 + 1 - core
    chunk, width = rows_all.shape[1], rows_all.shape[2]
    slots = chunk // groups_ep
    local_experts, _, units = gate_vmem.shape

    def remote(src, dst, send, recv, ep, tp):
        return pltpu.make_async_remote_copy(
            src_ref=src,
            dst_ref=dst,
            send_sem=send,
            recv_sem=recv,
            device_id=(ep, tp),
            device_id_type=pl.DeviceIdType.MESH,
        )

    barrier = pltpu.get_barrier_semaphore()
    others = [(lax.rem(q + i, groups_ep), t) for i in range(1, groups_ep)]
    others += [(q, lax.rem(z + i, chips) * 2 + core) for i in range(1, chips)]
    others += [(q, partner)]
    me, devices = q * groups_tp + t, groups_ep * groups_tp
    after, ahead = lax.rem(me + 1, devices), lax.rem(me + devices - 1, devices)
    others += [(n // groups_tp, lax.rem(n, groups_tp)) for n in (after, ahead)]

    def greet(ep, tp):
        pl.semaphore_signal(
            barrier, inc=1, device_id=(ep, tp), device_id_type=pl.DeviceIdType.MESH
        )

    for ep, tp in others:
        greet(ep, tp)

    loads = [
        pltpu.make_async_copy(src, dst, load_sem.at[i])
        for i, (src, dst) in enumerate(
            ((gate_hbm, gate_vmem), (up_hbm, up_vmem), (down_hbm, down_vmem))
        )
    ]
    weights = ((value_own, value_full), (gate_own, gate_full), (out_own, out_full))
    pl.semaphore_wait(barrier, len(others))

    def slot_rows(index):
        return pl.ds(pl.multiple_of(index * slots, slots), slots)

    own_rows = pltpu.make_async_copy(
        outgoing.at[slot_rows(q), :], rows_all.at[t, slot_rows(q), :], own_sem
    )
    own_rows.start()
    a_copies = []
    for i in range(1, groups_ep):
        there = lax.rem(q + i, groups_ep)
        copy = remote(
            outgoing.at[slot_rows(there), :],
            rows_all.at[t, slot_rows(q), :],
            send_a.at[i],
            recv_a.at[i],
            there,
            t,
        )
        copy.start()
        a_copies.append(copy)

    def sends(d, s):
        return (z >= s) & (z < chips - 1) if d == 0 else (z + s < chips) & (z > 0)

    def comes(d, s):
        return z >= 1 + s if d == 0 else z + 1 + s < chips

    def sent(d, s):
        return (z - s if d == 0 else z + s) * 2 + core

    def came(d, s):
        return sent(d, s + 1)

    def beside(d):
        return t + 2 if d == 0 else t - 2

    def quarter(k, index, cut=0):
        own = weights[k][0]
        part = own.shape[0] // groups_ep
        if cut == 0:
            return pl.ds(pl.multiple_of(index * part, part), part)
        half = part // 2
        return pl.ds(pl.multiple_of(index * part + (cut - 1) * half, half), half)

    def first_leg(k, d, s):
        own, full = weights[k]
        place = columns(full, sent(d, s), own.shape[1], quarter(k, q))
        src = own.at[quarter(k, q), :] if s == 0 else place
        return remote(src, place, send_w1.at[k, d, s], recv_w1.at[k, d, s], q, beside(d))

    flip_low = q + 1 - 2 * lax.rem(q, 2)
    flip_high = q + 2 - 4 * lax.rem(q // 2, 2)
    square = groups_ep == 4

    def second_leg(k, d, s, j):
        own, full = weights[k]
        piece, there, cut = q, lax.rem(q + j, groups_ep), 0
        if square:
            piece = (flip_high, q, q, flip_low)[j]
            there = (flip_low, flip_low, flip_high, flip_high)[j]
            cut = (2, 0, 0, 1)[j]
        place = columns(full, came(d, s), own.shape[1], quarter(k, piece, cut))
        return remote(
            place, place, send_w2.at[k, d, s, j], recv_w2.at[k, d, s, j], there, t
        )

    direct = (1, 2) if square else tuple(range(1, groups_ep))
    relayed = (0, 3) if square else ()

    def own_leg(k):
        own, full = weights[k]
        place = columns(full, t, own.shape[1], pl.ds(0, own.shape[0]))
        last = chips - 1
        return remote(own, place, send_wp.at[k, 0, last], recv_wp.at[k, 0, last], q, partner)

    def pair_leg(k, d, s):
        own, full = weights[k]
        place = columns(full, came(d, s), own.shape[1], pl.ds(0, own.shape[0]))
        return remote(place, place, send_wp.at[k, d, s], recv_wp.at[k, d, s], q, partner)

    def pass_on(k, s):
        for d in range(2):
            pl.when(sends(d, s))(lambda d=d: first_leg(k, d, s).start())

    def take(k, s):
        for d in range(2):

            @pl.when(comes(d, s))
            def _(d=d):
                first_leg(k, d, s).wait_recv()
                for j in direct:
                    second_leg(k, d, s, j).start()

    def relay(k, s):
        for d in range(2):

            @pl.when(comes(d, s))
            def _(d=d):
                for j in direct:
                    second_leg(k, d, s, j).wait_recv()
                for j in relayed:
                    second_leg(k, d, s, j).start()

    def share(k, s):
        for d in range(2):

            @pl.when(comes(d, s))
            def _(d=d):
                for j in relayed:
                    second_leg(k, d, s, j).wait_recv()
                pair_leg(k, d, s).start()

    def row_leg(d, s):
        place = rows_all.at[sent(d, s)]
        return remote(place, place, send_r.at[d, s], recv_r.at[d, s], q, beside(d))

    def row_pair(d, s):
        place = rows_all.at[came(d, s)]
        return remote(place, place, send_rp.at[d, s], recv_rp.at[d, s], q, partner)

    def own_pair():
        place, last = rows_all.at[t], chips - 1
        return remote(place, place, send_rp.at[0, last], recv_rp.at[0, last], q, partner)

    def rows_on(s):
        for d in range(2):
            pl.when(sends(d, s))(lambda d=d: row_leg(d, s).start())

    def rows_in(s):
        for d in range(2):
            pl.when(comes(d, s))(lambda d=d: row_leg(d, s).wait_recv())

    def rows_share(s):
        for d in range(2):
            pl.when(comes(d, s))(lambda d=d: row_pair(d, s).start())

    steps = chips - 1
    for k in (0,):
        pass_on(k, 0)
    stored = [
        pltpu.make_async_copy(
            own, columns(full, t, own.shape[1], pl.ds(0, own.shape[0])), stage_sem.at[k]
        )
        for k, (own, full) in enumerate(weights)
    ]
    for copy in loads + stored:
        copy.start()
    if inside:
        rim = padded.shape[0] - mixer_in.shape[0]
        length = mixer_in.shape[0]
        normed[...] = rms_scale(mixer_in[...], pre_gain[...]).astype(jnp.bfloat16)

        @pl.when(me == 0)
        def _():
            padded[pl.ds(0, rim), :] = jnp.zeros((rim, padded.shape[1]), jnp.float32)

    def halo():
        return remote(
            padded.at[pl.ds(length, rim), :],
            padded.at[pl.ds(0, rim), :],
            send_h,
            recv_h,
            after // groups_tp,
            lax.rem(after, groups_tp),
        )

    def wait_weight(k):
        stored[k].wait()
        own_leg(k).wait_recv()
        for s in range(steps):
            for d in range(2):
                pl.when(comes(d, s))(lambda d=d, s=s: pair_leg(k, d, s).wait_recv())

    def glu_stage():
        wait_weight(0)
        wait_weight(1)
        wide = min(256, value_full.shape[1])

        @pl.loop(0, value_full.shape[1] // wide)
        def _(step):
            place = pl.ds(pl.multiple_of(step * wide, wide), wide)
            rows = normed[...]
            value = jnp.dot(rows, value_full[:, place], preferred_element_type=jnp.float32)
            gate = jnp.dot(rows, gate_full[:, place], preferred_element_type=jnp.float32)
            glu = (value * jax.nn.sigmoid(gate)).astype(jnp.bfloat16)
            padded[pl.ds(rim, length), place] = glu.astype(jnp.float32)

        pl.when(me < devices - 1)(lambda: halo().start())

    def conv_stage():
        pl.when(me > 0)(lambda: halo().wait_recv())
        taps = conv_kernel.shape[0]

        @pl.loop(0, conv.shape[1] // 128)
        def _(step):
            place = pl.ds(pl.multiple_of(step * 128, 128), 128)
            total = jnp.zeros((length, 128), jnp.float32)
            for tap in range(taps):
                rows = padded[pl.ds(rim - taps + 1 + tap, length), place]
                total = total + conv_kernel[pl.ds(tap, 1), place] * rows
            conv[:, place] = total

        some = min(64, length)

        @pl.loop(0, length // some)
        def _(step):
            place = pl.ds(pl.multiple_of(step * some, some), some)
            block = conv[place, :]
            centred = block - jnp.mean(block, axis=-1, keepdims=True)
            var = jnp.mean(centred * centred, axis=-1, keepdims=True)
            scaled = centred * lax.rsqrt(var + LAYER_EPSILON) * chan_gain[...]
            act[place, :] = (scaled * jax.nn.sigmoid(scaled)).astype(jnp.bfloat16)

    def out_stage():
        wait_weight(2)
        wide = min(256, out_full.shape[1])

        @pl.loop(0, out_full.shape[1] // wide)
        def _(step):
            place = pl.ds(pl.multiple_of(step * wide, wide), wide)
            projected[:, place] = jnp.dot(
                act[...], out_full[:, place], preferred_element_type=jnp.float32
            )

        some = min(64, length)

        @pl.loop(0, length // some)
        def _(step):
            place = pl.ds(pl.multiple_of(step * some, some), some)
            mixed[place, :] = rms_scale(projected[place, :], mix_gain[...]).astype(jnp.bfloat16)

    own_rows.wait()
    for copy in a_copies:
        copy.wait_recv()
    rows_on(0)
    pass_on(1, 0)
    pass_on(2, 0)
    own_pair().start()
    for k in range(3):
        own_leg(k).start()

    take(0, 0)
    for s in range(steps):
        rows_in(s)
        if s + 1 < steps:
            rows_on(s + 1)
        rows_share(s)
        if s == min(1, steps - 1):
            take(1, 0)
            take(2, 0)
            if steps > 1:
                for k in range(3):
                    pass_on(k, 1)
            for k in range(3):
                relay(k, 0)
    own_pair().wait_recv()
    for s in range(steps):
        for d in range(2):
            pl.when(comes(d, s))(lambda d=d: row_pair(d, s).wait_recv())
    for copy in loads:
        copy.wait()

    total = groups_tp * chunk
    tile = min(256, units)
    tiles = units // tile

    @pl.loop(0, local_experts * tiles)
    def _(step):
        expert, unit = step // tiles, step % tiles
        place = pl.ds(pl.multiple_of(unit * tile, tile), tile)
        rows = rows_all[...].reshape(total, width)
        gate = jnp.dot(rows, gate_vmem[expert, :, place], preferred_element_type=jnp.float32)
        up = jnp.dot(rows, up_vmem[expert, :, place], preferred_element_type=jnp.float32)
        gate = jnp.minimum(gate, CLAMP_LIMIT)
        up = jnp.clip(up, -CLAMP_LIMIT, CLAMP_LIMIT)
        act = (up + 1.0) * gate * jax.nn.sigmoid(SWISH_ALPHA * gate)
        slot = lax.rem(lax.broadcasted_iota(jnp.int32, act.shape, 0), slots)
        mine = (slot >= expert * capacity) & (slot < (expert + 1) * capacity)
        hidden[:, pl.ds(pl.multiple_of(step * tile, tile), tile)] = jnp.where(
            mine, act, 0.0
        ).astype(jnp.bfloat16)

    for k in range(3):
        if steps > 1:
            take(k, 1)
        if steps > 2:
            pass_on(k, 2)
    for k in range(3):
        share(k, 0)

    down_tile = min(256, width)

    @pl.loop(0, width // down_tile)
    def _(step):
        place = pl.ds(pl.multiple_of(step * down_tile, down_tile), down_tile)
        weight = down_vmem[:, :, place].reshape(local_experts * units, down_tile)
        part = jnp.dot(hidden[...], weight, preferred_element_type=jnp.float32)
        partial[:, :, place] = part.astype(jnp.bfloat16).reshape(groups_tp, chunk, down_tile)

    def sum_pair(owner):
        return remote(
            partial.at[owner * 2 + 1 - core],
            pair_in.at[owner],
            send_p.at[owner],
            recv_p.at[owner],
            q,
            partner,
        )

    def sum_leg(d, owner):
        return remote(
            partial.at[owner * 2 + core],
            ring_in.at[d, owner],
            send_z.at[d, owner],
            recv_z.at[d, owner],
            q,
            beside(d),
        )

    def behind(d):
        return z > 0 if d == 0 else z < chips - 1

    def add_pair(owner):
        sum_pair(owner).wait_recv()
        place = partial.at[owner * 2 + core]
        both = place[...].astype(jnp.float32) + pair_in[owner].astype(jnp.float32)
        place[...] = both.astype(jnp.bfloat16)

    def add_line(d, owner):
        sum_leg(d, owner).wait_recv()
        place = partial.at[owner * 2 + core]
        both = place[...].astype(jnp.float32) + ring_in[d, owner].astype(jnp.float32)
        place[...] = both.astype(jnp.bfloat16)

    def send_sums(step):
        for d in range(2):
            far = z if d == 0 else chips - 1 - z
            owner = z + chips - 1 - step if d == 0 else z + step - chips + 1

            @pl.when(far <= step)
            def _(d=d, owner=owner):
                add_pair(owner)
                pl.when(behind(d))(lambda: add_line(d, owner))
                sum_leg(d, owner).start()

    order = []
    for j in range(chips):
        order += [o for o in (chips - 1 - j, j) if o not in order]
    for owner in order:
        sum_pair(owner).start()
    for s in range(2, steps):
        for k in range(3):
            take(k, s)
            if s + 1 < steps:
                pass_on(k, s + 1)
    send_sums(0)
    for k in range(3):
        if steps > 1:
            relay(k, 1)
    if steps > 1:
        send_sums(1)
    for k in range(3):
        if steps > 1:
            share(k, 1)
        for s in range(2, steps):
            relay(k, s)
    for s in range(2, steps):
        for k in range(3):
            share(k, s)
    if inside:
        glu_stage()
    for step in range(2, steps):
        send_sums(step)
    if inside:
        conv_stage()
    add_pair(z)
    if inside:
        out_stage()
    for d in range(2):
        pl.when(behind(d))(lambda d=d: add_line(d, z))
    summed = partial[t].astype(jnp.float32)
    back_out[...] = summed.astype(jnp.bfloat16)

    def back_leg(i):
        there = lax.rem(q + i, groups_ep)
        return remote(
            back_out.at[slot_rows(there), :],
            back_in.at[slot_rows(q), :],
            send_b.at[i],
            recv_b.at[i],
            there,
            t,
        )

    for i in range(1, groups_ep):
        back_leg(i).start()
    back_in[slot_rows(q), :] = back_out[slot_rows(q), :]
    for i in range(1, groups_ep):
        back_leg(i).wait_recv()
    returned[...] = back_in[...]

    for k in range(3):
        own_leg(k).wait_send()
        if not inside:
            wait_weight(k)
    if inside:
        pl.when(me < devices - 1)(lambda: halo().wait_send())
    own_pair().wait_send()
    for s in range(steps):
        for d in range(2):

            @pl.when(sends(d, s))
            def _(d=d, s=s):
                row_leg(d, s).wait_send()
                for k in range(3):
                    first_leg(k, d, s).wait_send()

            @pl.when(comes(d, s))
            def _(d=d, s=s):
                row_pair(d, s).wait_send()
                for k in range(3):
                    for j in direct + relayed:
                        second_leg(k, d, s, j).wait_send()
                    pair_leg(k, d, s).wait_send()
    for owner in range(chips):
        sum_pair(owner).wait_send()
        pl.when(z < owner)(lambda owner=owner: sum_leg(0, owner).wait_send())
        pl.when(z > owner)(lambda owner=owner: sum_leg(1, owner).wait_send())
    for i in range(1, groups_ep):
        a_copies[i - 1].wait_send()
        back_leg(i).wait_send()


def exchange(
    mixer_in,
    pre_gain,
    conv_kernel,
    chan_gain,
    mix_gain,
    outgoing,
    glu_value,
    glu_gate,
    out_weight,
    gate_proj,
    up_proj,
    down_proj,
    capacity,
):
    groups_ep, groups_tp = lax.axis_size("ep"), lax.axis_size("tp")
    chips = groups_tp // 2
    chunk, width = outgoing.shape
    units = gate_proj.shape[2] * gate_proj.shape[0]
    half = jnp.bfloat16

    def gathered(shard):
        rows, cols = shard.shape
        if cols % 128:
            return jax.ShapeDtypeStruct((groups_tp, rows, cols), half)
        return jax.ShapeDtypeStruct((rows, groups_tp * cols), half)

    own = (glu_value, glu_gate, out_weight)
    dma = pltpu.SemaphoreType.DMA
    inside = glu_value.shape[1] % 128 == 0 and out_weight.shape[1] % 128 == 0
    full_shapes = [gathered(shard) for shard in own]
    back_shape = jax.ShapeDtypeStruct((chunk, width), half)
    length, channels = mixer_in.shape[0], conv_kernel.shape[1]
    rim = -(-(conv_kernel.shape[0] - 1) // 8) * 8
    anywhere, vmem = pl.BlockSpec(memory_space=pl.ANY), pl.BlockSpec(memory_space=pltpu.VMEM)
    own_scratch = []
    if inside:
        own_scratch = [pltpu.VMEM(shape.shape, half) for shape in full_shapes] + [
            pltpu.VMEM(mixer_in.shape, half),
            pltpu.VMEM((rim + length, channels), jnp.float32),
            pltpu.VMEM((length, channels), jnp.float32),
            pltpu.VMEM((length, channels), half),
            pltpu.VMEM(mixer_in.shape, jnp.float32),
        ]
        mixer_specs = [vmem] * 5
    else:
        mixer_specs = [anywhere] * 5
    outs = pl.pallas_call(
        functools.partial(exchange_kernel, groups_ep, groups_tp, capacity, inside),
        out_shape=[jax.ShapeDtypeStruct(mixer_in.shape, half), back_shape]
        if inside
        else full_shapes + [back_shape],
        in_specs=[vmem] + mixer_specs + [anywhere] * 6,
        out_specs=[vmem] * 2 if inside else [anywhere] * 3 + [vmem],
        scratch_shapes=own_scratch
        + [
            pltpu.VMEM((groups_tp, chunk, width), half),
            pltpu.VMEM((groups_tp * chunk, units), half),
            pltpu.VMEM((groups_tp, chunk, width), half),
            pltpu.VMEM((chips, chunk, width), half),
            pltpu.VMEM((2, chips, chunk, width), half),
            pltpu.VMEM((chunk, width), half),
            pltpu.VMEM((chunk, width), half),
            pltpu.VMEM(gate_proj.shape, half),
            pltpu.VMEM(up_proj.shape, half),
            pltpu.VMEM(down_proj.shape, half),
            dma((3,)),
            dma((3,)),
            dma,
            dma,
            dma,
            dma((groups_ep,)),
            dma((groups_ep,)),
            dma((2, chips)),
            dma((2, chips)),
            dma((2, chips)),
            dma((2, chips)),
            dma((3, 2, chips)),
            dma((3, 2, chips)),
            dma((3, 2, chips, groups_ep)),
            dma((3, 2, chips, groups_ep)),
            dma((3, 2, chips)),
            dma((3, 2, chips)),
            dma((chips,)),
            dma((chips,)),
            dma((2, chips)),
            dma((2, chips)),
            dma((groups_ep,)),
            dma((groups_ep,)),
        ],
        compiler_params=pltpu.CompilerParams(
            collective_id=0, has_side_effects=True, vmem_limit_bytes=60 * 1024 * 1024
        ),
    )(
        outgoing,
        mixer_in,
        pre_gain[None],
        conv_kernel,
        chan_gain[None],
        mix_gain[None],
        *own,
        gate_proj,
        up_proj,
        down_proj,
    )
    if inside:
        return None, outs[0], outs[1]
    full = [
        value if value.ndim == 2 else value.transpose(1, 0, 2).reshape(value.shape[1], -1)
        for value in outs[:3]
    ]
    return full, None, outs[3]


def flipped(index, bit):
    return index + bit - 2 * bit * lax.rem(index // bit, 2)


def across(index, distance):
    bit = 1
    while bit <= distance:
        if distance & bit:
            index = flipped(index, bit)
        bit *= 2
    return index


def fused_kernel(
    groups_ep,
    groups_tp,
    capacity,
    expert_in,
    ffn_gain,
    routes,
    shares,
    expert_gain,
    mixer_hbm,
    pre_gain,
    conv_kernel,
    chan_gain,
    mix_gain,
    value_own,
    gate_own,
    out_own,
    gate_hbm,
    up_hbm,
    down_hbm,
    mixed,
    routed,
    value_full,
    gate_full,
    out_full,
    mixer_in,
    normed,
    padded,
    tail_out,
    tail_in,
    conv,
    act,
    projected,
    info,
    rows_all,
    picked,
    hidden,
    partial,
    pair_in,
    ring_in,
    back_in,
    gate_vmem,
    up_vmem,
    down_vmem,
    load_sem,
    stage_sem,
    send_h,
    recv_h,
    send_rz,
    recv_rz,
    send_rx,
    recv_rx,
    send_rd,
    recv_rd,
    send_rp,
    recv_rp,
    send_w1,
    recv_w1,
    send_w2,
    recv_w2,
    send_wp,
    recv_wp,
    send_p,
    recv_p,
    send_z,
    recv_z,
    send_b,
    recv_b,
):
    q = lax.axis_index("ep")
    t = lax.axis_index("tp")
    chips = groups_tp // 2
    z, core = t // 2, t % 2
    partner = z * 2 + 1 - core
    tokens, width = expert_in.shape
    slots = partial.shape[2]
    local_experts, _, units = gate_vmem.shape
    top_count = routes.shape[0]
    half_tokens = tokens // 2

    def remote(src, dst, send, recv, ep, tp):
        return pltpu.make_async_remote_copy(
            src_ref=src,
            dst_ref=dst,
            send_sem=send,
            recv_sem=recv,
            device_id=(ep, tp),
            device_id_type=pl.DeviceIdType.MESH,
        )

    barrier = pltpu.get_barrier_semaphore()
    others = [(lax.rem(q + i, groups_ep), t) for i in range(1, groups_ep)]
    others += [(q, lax.rem(z + i, chips) * 2 + core) for i in range(1, chips)]
    others += [(q, partner)]
    me, devices = q * groups_tp + t, groups_ep * groups_tp
    after, ahead = lax.rem(me + 1, devices), lax.rem(me + devices - 1, devices)
    others += [(n // groups_tp, lax.rem(n, groups_tp)) for n in (after, ahead)]
    for ep, tp in others:
        pl.semaphore_signal(
            barrier, inc=1, device_id=(ep, tp), device_id_type=pl.DeviceIdType.MESH
        )

    weights = ((value_own, value_full), (gate_own, gate_full), (out_own, out_full))
    stored = [
        pltpu.make_async_copy(
            own, columns(full, t, own.shape[1], pl.ds(0, own.shape[0])), stage_sem.at[k]
        )
        for k, (own, full) in enumerate(weights)
    ]
    mixer_load = pltpu.make_async_copy(mixer_hbm, mixer_in, load_sem.at[3])
    loads = [
        pltpu.make_async_copy(src, dst, load_sem.at[i])
        for i, (src, dst) in enumerate(
            ((gate_hbm, gate_vmem), (up_hbm, up_vmem), (down_hbm, down_vmem))
        )
    ]
    mixer_load.start()
    for copy in stored + loads:
        copy.start()

    rows_all[0, t, :, pl.ds(0, width)] = rms_scale(expert_in[...], ffn_gain[...]).astype(
        jnp.bfloat16
    )
    lanes = 128
    expert_ids = lax.broadcasted_iota(jnp.int32, (lanes, tokens), 0)
    chosen = [routes[pl.ds(k, 1), :] == expert_ids for k in range(top_count)]
    named = sum(c.astype(jnp.float32) for c in chosen)
    earlier = lax.broadcasted_iota(jnp.int32, (tokens, tokens), 0) < lax.broadcasted_iota(
        jnp.int32, (tokens, tokens), 1
    )
    rank = jnp.dot(
        named.astype(jnp.bfloat16),
        earlier.astype(jnp.float32).astype(jnp.bfloat16),
        preferred_element_type=jnp.float32,
    )
    group_ids = expert_ids // local_experts
    base = group_ids * slots + (expert_ids - group_ids * local_experts) * capacity
    spot = rank + base.astype(jnp.float32)
    facts = jnp.zeros((lanes, tokens), jnp.float32)
    for k in range(top_count):
        slot = jnp.sum(jnp.where(chosen[k], spot, 0.0), axis=0, keepdims=True)
        facts = facts + jnp.where(expert_ids == k, slot, 0.0)
        facts = facts + jnp.where(expert_ids == top_count + k, shares[pl.ds(k, 1), :], 0.0)
    info[...] = facts.T
    rows_all[0, t, :, pl.ds(width, lanes)] = info[...].astype(jnp.bfloat16)

    pl.semaphore_wait(barrier, len(others))

    def row_z(m):
        place = rows_all.at[0, t]
        return remote(place, place, send_rz.at[m], recv_rz.at[m], q, across(z, m) * 2 + core)

    def row_beside(b, m):
        owner = across(z, m) * 2 + core
        return remote(
            rows_all.at[0, owner],
            rows_all.at[1 + b, owner],
            send_rx.at[b, m],
            recv_rx.at[b, m],
            flipped(q, 1 + b),
            t,
        )

    def row_far(b, m):
        owner = across(z, m) * 2 + core
        some = pl.ds(b * half_tokens, half_tokens)
        return remote(
            rows_all.at[2 - b, owner, some, :],
            rows_all.at[3, owner, some, :],
            send_rd.at[b, m],
            recv_rd.at[b, m],
            flipped(q, 1 + b),
            t,
        )

    def row_pair(j, m):
        place = rows_all.at[j, across(z, m) * 2 + core]
        return remote(place, place, send_rp.at[j, m], recv_rp.at[j, m], q, partner)

    def rows_here(m):
        if m:
            row_z(m).wait_recv()
        for b in range(2):
            row_beside(b, m).start()
        row_pair(0, m).start()

    def rows_beside(m):
        for b in range(2):
            row_beside(b, m).wait_recv()
            row_far(1 - b, m).start()
            row_pair(1 + b, m).start()

    def rows_far(m):
        for b in range(2):
            row_far(b, m).wait_recv()
        row_pair(3, m).start()

    def sends(d, s):
        return (z >= s) & (z < chips - 1) if d == 0 else (z + s < chips) & (z > 0)

    def comes(d, s):
        return z >= 1 + s if d == 0 else z + 1 + s < chips

    def sent(d, s):
        return (z - s if d == 0 else z + s) * 2 + core

    def came(d, s):
        return sent(d, s + 1)

    def beside(d):
        return t + 2 if d == 0 else t - 2

    def quarter(k, index, cut=0):
        own = weights[k][0]
        part = own.shape[0] // groups_ep
        if cut == 0:
            return pl.ds(pl.multiple_of(index * part, part), part)
        half = part // 2
        return pl.ds(pl.multiple_of(index * part + (cut - 1) * half, half), half)

    def first_leg(k, d, s):
        own, full = weights[k]
        place = columns(full, sent(d, s), own.shape[1], quarter(k, q))
        src = own.at[quarter(k, q), :] if s == 0 else place
        return remote(src, place, send_w1.at[k, d, s], recv_w1.at[k, d, s], q, beside(d))

    flip_low, flip_high = flipped(q, 1), flipped(q, 2)
    direct, relayed = (1, 2), (0, 3)

    def second_leg(k, d, s, j):
        own, full = weights[k]
        piece = (flip_high, q, q, flip_low)[j]
        there = (flip_low, flip_low, flip_high, flip_high)[j]
        cut = (2, 0, 0, 1)[j]
        place = columns(full, came(d, s), own.shape[1], quarter(k, piece, cut))
        return remote(
            place, place, send_w2.at[k, d, s, j], recv_w2.at[k, d, s, j], there, t
        )

    def own_leg(k):
        own, full = weights[k]
        place = columns(full, t, own.shape[1], pl.ds(0, own.shape[0]))
        last = chips - 1
        return remote(own, place, send_wp.at[k, 0, last], recv_wp.at[k, 0, last], q, partner)

    def pair_leg(k, d, s):
        own, full = weights[k]
        place = columns(full, came(d, s), own.shape[1], pl.ds(0, own.shape[0]))
        return remote(place, place, send_wp.at[k, d, s], recv_wp.at[k, d, s], q, partner)

    def pass_on(k, s):
        if s < steps:
            for d in range(2):
                pl.when(sends(d, s))(lambda d=d: first_leg(k, d, s).start())

    def take(k, s):
        if s < steps:
            for d in range(2):

                @pl.when(comes(d, s))
                def _(d=d):
                    first_leg(k, d, s).wait_recv()
                    for j in direct:
                        second_leg(k, d, s, j).start()

            pass_on(k, s + 1)

    def relay(k, s):
        if s < steps:
            for d in range(2):

                @pl.when(comes(d, s))
                def _(d=d):
                    for j in direct:
                        second_leg(k, d, s, j).wait_recv()
                    for j in relayed:
                        second_leg(k, d, s, j).start()

    def share(k, s):
        if s < steps:
            for d in range(2):

                @pl.when(comes(d, s))
                def _(d=d):
                    for j in relayed:
                        second_leg(k, d, s, j).wait_recv()
                    pair_leg(k, d, s).start()

    def wait_plane(k, m):
        if m == 0:
            stored[k].wait()
            own_leg(k).wait_recv()
            return
        plane = across(z, m)
        d = (plane > z).astype(jnp.int32)
        s = (plane - z) * (2 * d - 1) - 1
        own, full = weights[k]
        place = columns(
            full, plane * 2 + 1 - core, own.shape[1], pl.ds(0, own.shape[0])
        )
        remote(
            place, place, send_wp.at[k, d, s], recv_wp.at[k, d, s], q, partner
        ).wait_recv()

    length = mixer_in.shape[0]
    rim = padded.shape[0] - length

    def norm_stage():
        mixer_load.wait()
        some = min(64, length)

        @pl.loop(0, length // some)
        def _(step):
            place = pl.ds(pl.multiple_of(step * some, some), some)
            normed[place, :] = rms_scale(mixer_in[place, :], pre_gain[...]).astype(jnp.bfloat16)

    def glu_stage(m):
        wait_plane(0, m)
        wait_plane(1, m)
        wide = 2 * value_own.shape[1]
        place = pl.ds(pl.multiple_of(across(z, m) * wide, wide), wide)
        rows = normed[...]
        value = jnp.dot(rows, value_full[:, place], preferred_element_type=jnp.float32)
        gate = jnp.dot(rows, gate_full[:, place], preferred_element_type=jnp.float32)
        glu = (value * jax.nn.sigmoid(gate)).astype(jnp.bfloat16)
        padded[pl.ds(rim, length), place] = glu.astype(jnp.float32)
        tail_out[:, place] = glu[length - rim :, :]

    def halo():
        return remote(
            tail_out, tail_in, send_h, recv_h, after // groups_tp, lax.rem(after, groups_tp)
        )

    def conv_stage():
        @pl.when(me > 0)
        def _():
            halo().wait_recv()
            padded[pl.ds(0, rim), :] = tail_in[...].astype(jnp.float32)

        @pl.when(me == 0)
        def _():
            padded[pl.ds(0, rim), :] = jnp.zeros((rim, padded.shape[1]), jnp.float32)

        taps = conv_kernel.shape[0]

        @pl.loop(0, conv.shape[1] // 128)
        def _(step):
            place = pl.ds(pl.multiple_of(step * 128, 128), 128)
            total = jnp.zeros((length, 128), jnp.float32)
            for tap in range(taps):
                rows = padded[pl.ds(rim - taps + 1 + tap, length), place]
                total = total + conv_kernel[pl.ds(tap, 1), place] * rows
            conv[:, place] = total

        some = min(64, length)

        @pl.loop(0, length // some)
        def _(step):
            place = pl.ds(pl.multiple_of(step * some, some), some)
            block = conv[place, :]
            centred = block - jnp.mean(block, axis=-1, keepdims=True)
            var = jnp.mean(centred * centred, axis=-1, keepdims=True)
            scaled = centred * lax.rsqrt(var + LAYER_EPSILON) * chan_gain[...]
            act[place, :] = (scaled * jax.nn.sigmoid(scaled)).astype(jnp.bfloat16)

    def out_stage(m):
        wait_plane(2, m)
        wide = out_own.shape[1]
        start = across(z, m) * 2 * wide
        for i in range(2):
            place = pl.ds(pl.multiple_of(start + i * wide, wide), wide)
            projected[:, place] = jnp.dot(
                act[...], out_full[:, place], preferred_element_type=jnp.float32
            )

    def mixed_stage():
        some = min(64, length)

        @pl.loop(0, length // some)
        def _(step):
            place = pl.ds(pl.multiple_of(step * some, some), some)
            mixed[place, :] = rms_scale(projected[place, :], mix_gain[...]).astype(jnp.bfloat16)

    total = groups_tp * slots
    tile = min(256, units)
    tiles = units // tile
    down_tile = min(256, width)

    def expert_stage(j):
        for m in range(chips):
            row_pair(j, m).wait_recv()
        if j == 0:
            for copy in loads:
                copy.wait()
        every = groups_tp * tokens
        block = rows_all[j].reshape(every, width + lanes)
        facts = block[:, width:].astype(jnp.float32)
        slot_ids = lax.broadcasted_iota(jnp.int32, (every, total), 1).astype(jnp.float32)
        owner = lax.broadcasted_iota(jnp.int32, (every, 1), 0) // tokens
        first = (owner * slots).astype(jnp.float32)
        low = (q * slots).astype(jnp.float32)
        pick = jnp.zeros((every, total), jnp.float32)
        for k in range(top_count):
            local = facts[:, k : k + 1] - low
            mine = (local >= 0.0) & (local < float(slots))
            target = jnp.where(mine, local + first, -1.0)
            pick = pick + (target == slot_ids).astype(jnp.float32)
        picked[...] = jnp.dot(
            pick.T.astype(jnp.bfloat16), block[:, :width], preferred_element_type=jnp.float32
        ).astype(jnp.bfloat16)

        @pl.loop(0, local_experts * tiles)
        def _(step):
            expert, unit = step // tiles, step % tiles
            place = pl.ds(pl.multiple_of(unit * tile, tile), tile)
            rows = picked[...]
            gate = jnp.dot(rows, gate_vmem[expert, :, place], preferred_element_type=jnp.float32)
            up = jnp.dot(rows, up_vmem[expert, :, place], preferred_element_type=jnp.float32)
            gate = jnp.minimum(gate, CLAMP_LIMIT)
            up = jnp.clip(up, -CLAMP_LIMIT, CLAMP_LIMIT)
            unit_act = (up + 1.0) * gate * jax.nn.sigmoid(SWISH_ALPHA * gate)
            slot = lax.rem(lax.broadcasted_iota(jnp.int32, unit_act.shape, 0), slots)
            mine = (slot >= expert * capacity) & (slot < (expert + 1) * capacity)
            hidden[:, pl.ds(pl.multiple_of(step * tile, tile), tile)] = jnp.where(
                mine, unit_act, 0.0
            ).astype(jnp.bfloat16)

        @pl.loop(0, width // down_tile)
        def _(step):
            place = pl.ds(pl.multiple_of(step * down_tile, down_tile), down_tile)
            weight = down_vmem[:, :, place].reshape(local_experts * units, down_tile)
            part = jnp.dot(hidden[...], weight, preferred_element_type=jnp.float32)
            partial[j, :, :, place] = part.astype(jnp.bfloat16).reshape(
                groups_tp, slots, down_tile
            )

        for owner in owners:
            sum_pair(j, owner).start()

    owners = []
    for i in range(chips):
        owners += [o for o in (chips - 1 - i, i) if o not in owners]

    def sum_pair(j, owner):
        return remote(
            partial.at[j, owner * 2 + 1 - core],
            pair_in.at[j, owner],
            send_p.at[j, owner],
            recv_p.at[j, owner],
            q,
            partner,
        )

    def sum_leg(j, d, owner):
        return remote(
            partial.at[j, owner * 2 + core],
            ring_in.at[j, d, owner],
            send_z.at[j, d, owner],
            recv_z.at[j, d, owner],
            q,
            beside(d),
        )

    def behind(d):
        return z > 0 if d == 0 else z < chips - 1

    def add_to(j, owner, other):
        place = partial.at[j, owner * 2 + core]
        both = place[...].astype(jnp.float32) + other[...].astype(jnp.float32)
        place[...] = both.astype(jnp.bfloat16)

    def add_pair(j, owner):
        sum_pair(j, owner).wait_recv()
        add_to(j, owner, pair_in.at[j, owner])

    def add_line(j, d, owner):
        sum_leg(j, d, owner).wait_recv()
        add_to(j, owner, ring_in.at[j, d, owner])

    def send_sums(j, step):
        for d in range(2):
            far = z if d == 0 else chips - 1 - z
            owner = z + chips - 1 - step if d == 0 else z + step - chips + 1

            @pl.when(far <= step)
            def _(d=d, owner=owner):
                add_pair(j, owner)
                pl.when(behind(d))(lambda: add_line(j, d, owner))
                sum_leg(j, d, owner).start()

    def back_leg(j):
        return remote(
            partial.at[j, t], back_in.at[j], send_b.at[j], recv_b.at[j], across(q, j), t
        )

    def own_sums(j):
        add_pair(j, z)
        for d in range(2):
            pl.when(behind(d))(lambda d=d: add_line(j, d, z))
        if j:
            back_leg(j).start()

    def routed_stage():
        facts = info[...]
        total_rows = jnp.zeros((tokens, width), jnp.float32)
        slot_ids = lax.broadcasted_iota(jnp.int32, (tokens, slots), 1)
        for j in range(groups_ep):
            if j:
                back_leg(j).wait_recv()
            block = partial[0, t] if j == 0 else back_in[j]
            low = across(q, j) * slots
            shared = jnp.zeros((tokens, slots), jnp.float32)
            for k in range(top_count):
                here = facts[:, k : k + 1] == (slot_ids + low).astype(jnp.float32)
                share_of = facts[:, top_count + k : top_count + k + 1]
                shared = shared + jnp.where(here, share_of, 0.0)
            high = shared.astype(jnp.bfloat16)
            rest = (shared - high.astype(jnp.float32)).astype(jnp.bfloat16)
            for term in (high, rest):
                total_rows = total_rows + jnp.dot(
                    term, block, preferred_element_type=jnp.float32
                )
        routed[...] = rms_scale(total_rows, expert_gain[...]).astype(jnp.bfloat16)

    steps = chips - 1
    both = (0, 1)
    for m in range(1, chips):
        row_z(m).start()
    rows_here(0)
    for k in both:
        pass_on(k, 0)
    for k in both:
        own_leg(k).start()
    norm_stage()
    for m in range(1, chips):
        rows_here(m)
        rows_beside(m - 1)
    glu_stage(0)
    own_leg(2).start()
    for k in both:
        take(k, 0)
    pass_on(2, 0)
    expert_stage(0)
    rows_beside(chips - 1)
    for m in range(chips):
        rows_far(m)
    for k in both:
        relay(k, 0)
    expert_stage(1)
    for k in both:
        take(k, 1)
    take(2, 0)
    send_sums(0, 0)
    expert_stage(2)
    send_sums(0, 1)
    send_sums(1, 0)
    for k in both:
        relay(k, 1)
        share(k, 0)
    relay(2, 0)
    for s in range(2, steps):
        for k in both:
            take(k, s)
    take(2, 1)
    expert_stage(3)
    for step in range(2, steps):
        send_sums(0, step)
    send_sums(1, 1)
    send_sums(2, 0)
    own_sums(0)
    for k in both:
        share(k, 1)
    for s in range(2, steps):
        for k in both:
            relay(k, s)
    glu_stage(1)
    for step in range(2, steps):
        send_sums(1, step)
    send_sums(2, 1)
    send_sums(3, 0)
    for s in range(2, steps):
        for k in both:
            share(k, s)
    relay(2, 1)
    for s in range(2, steps):
        take(2, s)
    own_sums(1)
    glu_stage(2)
    for step in range(2, steps):
        send_sums(2, step)
    send_sums(3, 1)
    own_sums(2)
    for m in range(3, chips):
        glu_stage(m)
    pl.when(me < devices - 1)(lambda: halo().start())
    for s in range(2, steps):
        relay(2, s)
    share(2, 0)
    for step in range(2, steps):
        send_sums(3, step)
    share(2, 1)
    own_sums(3)
    conv_stage()
    for s in range(2, steps):
        share(2, s)
    for m in range(chips):
        out_stage(m)
    mixed_stage()
    routed_stage()

    for m in range(chips):
        if m:
            row_z(m).wait_send()
        for b in range(2):
            row_beside(b, m).wait_send()
            row_far(b, m).wait_send()
        for j in range(groups_ep):
            row_pair(j, m).wait_send()
    for k in range(3):
        own_leg(k).wait_send()
    pl.when(me < devices - 1)(lambda: halo().wait_send())
    for s in range(steps):
        for d in range(2):

            @pl.when(sends(d, s))
            def _(d=d, s=s):
                for k in range(3):
                    first_leg(k, d, s).wait_send()

            @pl.when(comes(d, s))
            def _(d=d, s=s):
                for k in range(3):
                    for j in direct + relayed:
                        second_leg(k, d, s, j).wait_send()
                    pair_leg(k, d, s).wait_send()
    for j in range(groups_ep):
        for owner in range(chips):
            sum_pair(j, owner).wait_send()
            pl.when(z < owner)(lambda j=j, owner=owner: sum_leg(j, 0, owner).wait_send())
            pl.when(z > owner)(lambda j=j, owner=owner: sum_leg(j, 1, owner).wait_send())
        if j:
            back_leg(j).wait_send()


def fused(
    mixer_in,
    pre_gain,
    glu_value,
    glu_gate,
    conv_kernel,
    chan_gain,
    out_weight,
    mix_gain,
    expert_in,
    ffn_gain,
    routing,
    route_weight,
    gate_proj,
    up_proj,
    down_proj,
    expert_gain,
    capacity,
    slots,
):
    groups_ep, groups_tp = lax.axis_size("ep"), lax.axis_size("tp")
    chips = groups_tp // 2
    tokens, width = expert_in.shape
    length, channels = mixer_in.shape[0], conv_kernel.shape[1]
    units = gate_proj.shape[2] * gate_proj.shape[0]
    half, full = jnp.bfloat16, jnp.float32
    dma = pltpu.SemaphoreType.DMA
    rim = -(-(conv_kernel.shape[0] - 1) // 8) * 8
    anywhere, vmem = pl.BlockSpec(memory_space=pl.ANY), pl.BlockSpec(memory_space=pltpu.VMEM)

    def gathered(shard):
        return pltpu.VMEM((shard.shape[0], groups_tp * shard.shape[1]), half)

    return pl.pallas_call(
        functools.partial(fused_kernel, groups_ep, groups_tp, capacity),
        out_shape=[
            jax.ShapeDtypeStruct(mixer_in.shape, half),
            jax.ShapeDtypeStruct(expert_in.shape, half),
        ],
        in_specs=[vmem] * 5 + [anywhere] + [vmem] * 4 + [anywhere] * 6,
        out_specs=[vmem] * 2,
        scratch_shapes=[
            gathered(glu_value),
            gathered(glu_gate),
            gathered(out_weight),
            pltpu.VMEM(mixer_in.shape, half),
            pltpu.VMEM(mixer_in.shape, half),
            pltpu.VMEM((rim + length, channels), full),
            pltpu.VMEM((rim, channels), half),
            pltpu.VMEM((rim, channels), half),
            pltpu.VMEM((length, channels), full),
            pltpu.VMEM((length, channels), half),
            pltpu.VMEM(mixer_in.shape, full),
            pltpu.VMEM((tokens, 128), full),
            pltpu.VMEM((groups_ep, groups_tp, tokens, width + 128), half),
            pltpu.VMEM((groups_tp * slots, width), half),
            pltpu.VMEM((groups_tp * slots, units), half),
            pltpu.VMEM((groups_ep, groups_tp, slots, width), half),
            pltpu.VMEM((groups_ep, chips, slots, width), half),
            pltpu.VMEM((groups_ep, 2, chips, slots, width), half),
            pltpu.VMEM((groups_ep, slots, width), half),
            pltpu.VMEM(gate_proj.shape, half),
            pltpu.VMEM(up_proj.shape, half),
            pltpu.VMEM(down_proj.shape, half),
            dma((4,)),
            dma((3,)),
            dma,
            dma,
            dma((chips,)),
            dma((chips,)),
            dma((2, chips)),
            dma((2, chips)),
            dma((2, chips)),
            dma((2, chips)),
            dma((groups_ep, chips)),
            dma((groups_ep, chips)),
            dma((3, 2, chips)),
            dma((3, 2, chips)),
            dma((3, 2, chips, 4)),
            dma((3, 2, chips, 4)),
            dma((3, 2, chips)),
            dma((3, 2, chips)),
            dma((groups_ep, chips)),
            dma((groups_ep, chips)),
            dma((groups_ep, 2, chips)),
            dma((groups_ep, 2, chips)),
            dma((groups_ep,)),
            dma((groups_ep,)),
        ],
        compiler_params=pltpu.CompilerParams(
            collective_id=0, has_side_effects=True, vmem_limit_bytes=60 * 1024 * 1024
        ),
    )(
        expert_in,
        ffn_gain[None],
        routing.T,
        route_weight.T,
        expert_gain[None],
        mixer_in,
        pre_gain[None],
        conv_kernel,
        chan_gain[None],
        mix_gain[None],
        glu_value,
        glu_gate,
        out_weight,
        gate_proj,
        up_proj,
        down_proj,
    )


def mixer(full, mixer_in, pre_gain, conv_kernel, chan_gain, mix_gain):
    value_full, gate_full, out_full = full
    normed_mix = rms_scale(mixer_in, pre_gain).astype(jnp.bfloat16)
    value_pre = jnp.dot(normed_mix, value_full, preferred_element_type=jnp.float32)
    gate_mix = jnp.dot(normed_mix, gate_full, preferred_element_type=jnp.float32)
    gated_rows = (value_pre * jax.nn.sigmoid(gate_mix)).astype(jnp.bfloat16)
    kernel_width = conv_kernel.shape[0]
    length = gated_rows.shape[0]
    rim_rows = passed_along(gated_rows[length - (kernel_width - 1) :], ("ep", "tp"), 1)
    padded = jnp.concatenate([rim_rows, gated_rows], axis=0).astype(jnp.float32)
    conv_sum = jnp.zeros((length, gated_rows.shape[1]), jnp.float32)
    for offset in range(kernel_width):
        conv_sum = conv_sum + conv_kernel[offset] * padded[offset : offset + length]
    row_mean = jnp.mean(conv_sum, axis=-1, keepdims=True)
    centred = conv_sum - row_mean
    row_var = jnp.mean(centred * centred, axis=-1, keepdims=True)
    activated = jax.nn.silu(centred * lax.rsqrt(row_var + LAYER_EPSILON) * chan_gain).astype(
        jnp.bfloat16
    )
    projected = jnp.dot(activated, out_full, preferred_element_type=jnp.float32)
    mixed = rms_scale(projected, mix_gain).astype(jnp.bfloat16)
    return mixed


def on_device(
    mixer_in,
    pre_gain,
    glu_value,
    glu_gate,
    conv_kernel,
    chan_gain,
    out_weight,
    mix_gain,
    expert_in,
    ffn_gain,
    routing,
    route_weight,
    gate_proj,
    up_proj,
    down_proj,
    expert_gain,
):
    groups_ep = lax.axis_size("ep")
    local_experts = gate_proj.shape[0]
    experts = local_experts * groups_ep
    token_rows, top_count = routing.shape
    capacity = max(2, 3 * token_rows * top_count // (2 * experts))
    slots = -(-local_experts * capacity // 8) * 8
    chips = lax.axis_size("tp") // 2
    lined_up = all(w.shape[1] % 128 == 0 for w in (glu_value, glu_gate, out_weight))
    two_way = groups_ep == 4 and chips > 1 and chips & (chips - 1) == 0
    if lined_up and two_way and groups_ep * slots <= 256:
        return tuple(
            fused(
                mixer_in,
                pre_gain,
                glu_value,
                glu_gate,
                conv_kernel,
                chan_gain,
                out_weight,
                mix_gain,
                expert_in,
                ffn_gain,
                routing,
                route_weight,
                gate_proj,
                up_proj,
                down_proj,
                expert_gain,
                capacity,
                slots,
            )
        )
    flat_route = routing.reshape(-1)
    onehot = (flat_route[:, None] == jnp.arange(experts, dtype=jnp.int32)[None, :]).astype(
        jnp.int32
    )
    before = jnp.cumsum(onehot, axis=0) - onehot
    rank_within = jnp.sum(before * onehot, axis=1)
    slot_index = (
        flat_route // local_experts * slots + flat_route % local_experts * capacity + rank_within
    ).reshape(token_rows, top_count)
    slot_ids = jnp.arange(groups_ep * slots, dtype=jnp.int32)
    chosen = slot_index[None, :, :] == slot_ids[:, None, None]
    pick_matrix = jnp.sum(chosen.astype(jnp.float32), axis=2).astype(jnp.bfloat16)
    normed_exp = rms_scale(expert_in, ffn_gain).astype(jnp.bfloat16)
    outgoing = jnp.dot(pick_matrix, normed_exp, preferred_element_type=jnp.float32).astype(
        jnp.bfloat16
    )
    full, mixed, returned = exchange(
        mixer_in,
        pre_gain,
        conv_kernel,
        chan_gain,
        mix_gain,
        outgoing,
        glu_value,
        glu_gate,
        out_weight,
        gate_proj,
        up_proj,
        down_proj,
        capacity,
    )
    if mixed is None:
        mixed = mixer(full, mixer_in, pre_gain, conv_kernel, chan_gain, mix_gain)
    combined = jnp.zeros((token_rows, returned.shape[1]), jnp.float32)
    for column in range(top_count):
        combined = combined + route_weight[:, column][:, None] * returned[
            slot_index[:, column]
        ].astype(jnp.float32)
    routed = rms_scale(combined, expert_gain).astype(jnp.bfloat16)
    return (mixed, routed)


def solution(mesh):
    in_specs = (
        P(("ep", "tp"), None),
        P(),
        P(None, "tp"),
        P(None, "tp"),
        P(),
        P(),
        P(None, "tp"),
        P(),
        P(("ep", "tp"), None),
        P(),
        P(("ep", "tp"), None),
        P(("ep", "tp"), None),
        P("ep", None, "tp"),
        P("ep", None, "tp"),
        P("ep", "tp", None),
        P(),
    )
    out_specs = (P(("ep", "tp"), None), P(("ep", "tp"), None))
    return jax.shard_map(
        on_device, mesh=mesh, in_specs=in_specs, out_specs=out_specs, check_vma=False
    )
```

```python
import functools

import jax
import jax.numpy as jnp
from jax import lax
from jax.experimental import pallas as pl
from jax.experimental.pallas import tpu as pltpu
from jax.sharding import PartitionSpec as P

RMS_EPSILON = 1e-06
LAYER_EPSILON = 1e-05
CLAMP_LIMIT = 7.0
SWISH_ALPHA = 1.702


def passed_along(value, axis, steps):
    count = lax.axis_size(axis)
    initial, last = (max(0, -steps), min(count, count - steps))
    return lax.ppermute(value, axis, [(source, source + steps) for source in range(initial, last)])


def rms_scale(values, gain_row):
    values = values.astype(jnp.float32)
    return (
        values
        * lax.rsqrt(jnp.mean(values * values, axis=-1, keepdims=True) + RMS_EPSILON)
        * gain_row
    )


def columns(ref, owner, width, rows):
    if len(ref.shape) == 3:
        return ref.at[owner, rows, :]
    return ref.at[rows, pl.ds(pl.multiple_of(owner * width, width), width)]


def exchange_kernel(
    groups_ep,
    groups_tp,
    capacity,
    inside,
    outgoing,
    mixer_in,
    pre_gain,
    conv_kernel,
    chan_gain,
    mix_gain,
    value_own,
    gate_own,
    out_own,
    gate_hbm,
    up_hbm,
    down_hbm,
    *rest,
):
    if inside:
        mixed, returned, value_full, gate_full, out_full, *rest = rest
        normed, padded, conv, act, projected, *rest = rest
    else:
        value_full, gate_full, out_full, returned, *rest = rest
    (
    rows_all,
    hidden,
    partial,
    pair_in,
    ring_in,
    back_out,
    back_in,
    gate_vmem,
    up_vmem,
    down_vmem,
    load_sem,
    stage_sem,
    send_h,
    recv_h,
    own_sem,
    send_a,
    recv_a,
    send_r,
    recv_r,
    send_rp,
    recv_rp,
    send_w1,
    recv_w1,
    send_w2,
    recv_w2,
    send_wp,
    recv_wp,
    send_p,
    recv_p,
    send_z,
    recv_z,
    send_b,
    recv_b,
    ) = rest
    q = lax.axis_index("ep")
    t = lax.axis_index("tp")
    chips = groups_tp // 2
    z, core = t // 2, t % 2
    partner = z * 2 + 1 - core
    chunk, width = rows_all.shape[1], rows_all.shape[2]
    slots = chunk // groups_ep
    local_experts, _, units = gate_vmem.shape

    def remote(src, dst, send, recv, ep, tp):
        return pltpu.make_async_remote_copy(
            src_ref=src,
            dst_ref=dst,
            send_sem=send,
            recv_sem=recv,
            device_id=(ep, tp),
            device_id_type=pl.DeviceIdType.MESH,
        )

    barrier = pltpu.get_barrier_semaphore()
    others = [(lax.rem(q + i, groups_ep), t) for i in range(1, groups_ep)]
    others += [(q, lax.rem(z + i, chips) * 2 + core) for i in range(1, chips)]
    others += [(q, partner)]
    me, devices = q * groups_tp + t, groups_ep * groups_tp
    after, ahead = lax.rem(me + 1, devices), lax.rem(me + devices - 1, devices)
    others += [(n // groups_tp, lax.rem(n, groups_tp)) for n in (after, ahead)]

    def greet(ep, tp):
        pl.semaphore_signal(
            barrier, inc=1, device_id=(ep, tp), device_id_type=pl.DeviceIdType.MESH
        )

    for ep, tp in others:
        greet(ep, tp)

    loads = [
        pltpu.make_async_copy(src, dst, load_sem.at[i])
        for i, (src, dst) in enumerate(
            ((gate_hbm, gate_vmem), (up_hbm, up_vmem), (down_hbm, down_vmem))
        )
    ]
    weights = ((value_own, value_full), (gate_own, gate_full), (out_own, out_full))
    pl.semaphore_wait(barrier, len(others))

    def slot_rows(index):
        return pl.ds(pl.multiple_of(index * slots, slots), slots)

    own_rows = pltpu.make_async_copy(
        outgoing.at[slot_rows(q), :], rows_all.at[t, slot_rows(q), :], own_sem
    )
    own_rows.start()
    a_copies = []
    for i in range(1, groups_ep):
        there = lax.rem(q + i, groups_ep)
        copy = remote(
            outgoing.at[slot_rows(there), :],
            rows_all.at[t, slot_rows(q), :],
            send_a.at[i],
            recv_a.at[i],
            there,
            t,
        )
        copy.start()
        a_copies.append(copy)

    def sends(d, s):
        return (z >= s) & (z < chips - 1) if d == 0 else (z + s < chips) & (z > 0)

    def comes(d, s):
        return z >= 1 + s if d == 0 else z + 1 + s < chips

    def sent(d, s):
        return (z - s if d == 0 else z + s) * 2 + core

    def came(d, s):
        return sent(d, s + 1)

    def beside(d):
        return t + 2 if d == 0 else t - 2

    def quarter(k, index, cut=0):
        own = weights[k][0]
        part = own.shape[0] // groups_ep
        if cut == 0:
            return pl.ds(pl.multiple_of(index * part, part), part)
        half = part // 2
        return pl.ds(pl.multiple_of(index * part + (cut - 1) * half, half), half)

    def first_leg(k, d, s):
        own, full = weights[k]
        place = columns(full, sent(d, s), own.shape[1], quarter(k, q))
        src = own.at[quarter(k, q), :] if s == 0 else place
        return remote(src, place, send_w1.at[k, d, s], recv_w1.at[k, d, s], q, beside(d))

    flip_low = q + 1 - 2 * lax.rem(q, 2)
    flip_high = q + 2 - 4 * lax.rem(q // 2, 2)
    square = groups_ep == 4

    def second_leg(k, d, s, j):
        own, full = weights[k]
        piece, there, cut = q, lax.rem(q + j, groups_ep), 0
        if square:
            piece = (flip_high, q, q, flip_low)[j]
            there = (flip_low, flip_low, flip_high, flip_high)[j]
            cut = (2, 0, 0, 1)[j]
        place = columns(full, came(d, s), own.shape[1], quarter(k, piece, cut))
        return remote(
            place, place, send_w2.at[k, d, s, j], recv_w2.at[k, d, s, j], there, t
        )

    direct = (1, 2) if square else tuple(range(1, groups_ep))
    relayed = (0, 3) if square else ()

    def own_leg(k):
        own, full = weights[k]
        place = columns(full, t, own.shape[1], pl.ds(0, own.shape[0]))
        last = chips - 1
        return remote(own, place, send_wp.at[k, 0, last], recv_wp.at[k, 0, last], q, partner)

    def pair_leg(k, d, s):
        own, full = weights[k]
        place = columns(full, came(d, s), own.shape[1], pl.ds(0, own.shape[0]))
        return remote(place, place, send_wp.at[k, d, s], recv_wp.at[k, d, s], q, partner)

    def pass_on(k, s):
        for d in range(2):
            pl.when(sends(d, s))(lambda d=d: first_leg(k, d, s).start())

    def take(k, s):
        for d in range(2):

            @pl.when(comes(d, s))
            def _(d=d):
                first_leg(k, d, s).wait_recv()
                for j in direct:
                    second_leg(k, d, s, j).start()

    def relay(k, s):
        for d in range(2):

            @pl.when(comes(d, s))
            def _(d=d):
                for j in direct:
                    second_leg(k, d, s, j).wait_recv()
                for j in relayed:
                    second_leg(k, d, s, j).start()

    def share(k, s):
        for d in range(2):

            @pl.when(comes(d, s))
            def _(d=d):
                for j in relayed:
                    second_leg(k, d, s, j).wait_recv()
                pair_leg(k, d, s).start()

    def row_leg(d, s):
        place = rows_all.at[sent(d, s)]
        return remote(place, place, send_r.at[d, s], recv_r.at[d, s], q, beside(d))

    def row_pair(d, s):
        place = rows_all.at[came(d, s)]
        return remote(place, place, send_rp.at[d, s], recv_rp.at[d, s], q, partner)

    def own_pair():
        place, last = rows_all.at[t], chips - 1
        return remote(place, place, send_rp.at[0, last], recv_rp.at[0, last], q, partner)

    def rows_on(s):
        for d in range(2):
            pl.when(sends(d, s))(lambda d=d: row_leg(d, s).start())

    def rows_in(s):
        for d in range(2):
            pl.when(comes(d, s))(lambda d=d: row_leg(d, s).wait_recv())

    def rows_share(s):
        for d in range(2):
            pl.when(comes(d, s))(lambda d=d: row_pair(d, s).start())

    steps = chips - 1
    for k in (0,):
        pass_on(k, 0)
    stored = [
        pltpu.make_async_copy(
            own, columns(full, t, own.shape[1], pl.ds(0, own.shape[0])), stage_sem.at[k]
        )
        for k, (own, full) in enumerate(weights)
    ]
    for copy in loads + stored:
        copy.start()
    if inside:
        rim = padded.shape[0] - mixer_in.shape[0]
        length = mixer_in.shape[0]
        normed[...] = rms_scale(mixer_in[...], pre_gain[...]).astype(jnp.bfloat16)

        @pl.when(me == 0)
        def _():
            padded[pl.ds(0, rim), :] = jnp.zeros((rim, padded.shape[1]), jnp.float32)

    def halo():
        return remote(
            padded.at[pl.ds(length, rim), :],
            padded.at[pl.ds(0, rim), :],
            send_h,
            recv_h,
            after // groups_tp,
            lax.rem(after, groups_tp),
        )

    def wait_weight(k):
        stored[k].wait()
        own_leg(k).wait_recv()
        for s in range(steps):
            for d in range(2):
                pl.when(comes(d, s))(lambda d=d, s=s: pair_leg(k, d, s).wait_recv())

    def glu_stage():
        wait_weight(0)
        wait_weight(1)
        wide = min(256, value_full.shape[1])

        @pl.loop(0, value_full.shape[1] // wide)
        def _(step):
            place = pl.ds(pl.multiple_of(step * wide, wide), wide)
            rows = normed[...]
            value = jnp.dot(rows, value_full[:, place], preferred_element_type=jnp.float32)
            gate = jnp.dot(rows, gate_full[:, place], preferred_element_type=jnp.float32)
            glu = (value * jax.nn.sigmoid(gate)).astype(jnp.bfloat16)
            padded[pl.ds(rim, length), place] = glu.astype(jnp.float32)

        pl.when(me < devices - 1)(lambda: halo().start())

    def conv_stage():
        pl.when(me > 0)(lambda: halo().wait_recv())
        taps = conv_kernel.shape[0]

        @pl.loop(0, conv.shape[1] // 128)
        def _(step):
            place = pl.ds(pl.multiple_of(step * 128, 128), 128)
            total = jnp.zeros((length, 128), jnp.float32)
            for tap in range(taps):
                rows = padded[pl.ds(rim - taps + 1 + tap, length), place]
                total = total + conv_kernel[pl.ds(tap, 1), place] * rows
            conv[:, place] = total

        some = min(64, length)

        @pl.loop(0, length // some)
        def _(step):
            place = pl.ds(pl.multiple_of(step * some, some), some)
            block = conv[place, :]
            centred = block - jnp.mean(block, axis=-1, keepdims=True)
            var = jnp.mean(centred * centred, axis=-1, keepdims=True)
            scaled = centred * lax.rsqrt(var + LAYER_EPSILON) * chan_gain[...]
            act[place, :] = (scaled * jax.nn.sigmoid(scaled)).astype(jnp.bfloat16)

    def out_stage():
        wait_weight(2)
        wide = min(256, out_full.shape[1])

        @pl.loop(0, out_full.shape[1] // wide)
        def _(step):
            place = pl.ds(pl.multiple_of(step * wide, wide), wide)
            projected[:, place] = jnp.dot(
                act[...], out_full[:, place], preferred_element_type=jnp.float32
            )

        some = min(64, length)

        @pl.loop(0, length // some)
        def _(step):
            place = pl.ds(pl.multiple_of(step * some, some), some)
            mixed[place, :] = rms_scale(projected[place, :], mix_gain[...]).astype(jnp.bfloat16)

    own_rows.wait()
    for copy in a_copies:
        copy.wait_recv()
    rows_on(0)
    pass_on(1, 0)
    pass_on(2, 0)
    own_pair().start()
    for k in range(3):
        own_leg(k).start()

    take(0, 0)
    for s in range(steps):
        rows_in(s)
        if s + 1 < steps:
            rows_on(s + 1)
        rows_share(s)
        if s == min(1, steps - 1):
            take(1, 0)
            take(2, 0)
            if steps > 1:
                for k in range(3):
                    pass_on(k, 1)
            for k in range(3):
                relay(k, 0)
    own_pair().wait_recv()
    for s in range(steps):
        for d in range(2):
            pl.when(comes(d, s))(lambda d=d: row_pair(d, s).wait_recv())
    for copy in loads:
        copy.wait()

    total = groups_tp * chunk
    tile = min(256, units)
    tiles = units // tile

    @pl.loop(0, local_experts * tiles)
    def _(step):
        expert, unit = step // tiles, step % tiles
        place = pl.ds(pl.multiple_of(unit * tile, tile), tile)
        rows = rows_all[...].reshape(total, width)
        gate = jnp.dot(rows, gate_vmem[expert, :, place], preferred_element_type=jnp.float32)
        up = jnp.dot(rows, up_vmem[expert, :, place], preferred_element_type=jnp.float32)
        gate = jnp.minimum(gate, CLAMP_LIMIT)
        up = jnp.clip(up, -CLAMP_LIMIT, CLAMP_LIMIT)
        act = (up + 1.0) * gate * jax.nn.sigmoid(SWISH_ALPHA * gate)
        slot = lax.rem(lax.broadcasted_iota(jnp.int32, act.shape, 0), slots)
        mine = (slot >= expert * capacity) & (slot < (expert + 1) * capacity)
        hidden[:, pl.ds(pl.multiple_of(step * tile, tile), tile)] = jnp.where(
            mine, act, 0.0
        ).astype(jnp.bfloat16)

    for k in range(3):
        if steps > 1:
            take(k, 1)
        if steps > 2:
            pass_on(k, 2)
    for k in range(3):
        share(k, 0)

    down_tile = min(256, width)

    @pl.loop(0, width // down_tile)
    def _(step):
        place = pl.ds(pl.multiple_of(step * down_tile, down_tile), down_tile)
        weight = down_vmem[:, :, place].reshape(local_experts * units, down_tile)
        part = jnp.dot(hidden[...], weight, preferred_element_type=jnp.float32)
        partial[:, :, place] = part.astype(jnp.bfloat16).reshape(groups_tp, chunk, down_tile)

    def sum_pair(owner):
        return remote(
            partial.at[owner * 2 + 1 - core],
            pair_in.at[owner],
            send_p.at[owner],
            recv_p.at[owner],
            q,
            partner,
        )

    def sum_leg(d, owner):
        return remote(
            partial.at[owner * 2 + core],
            ring_in.at[d, owner],
            send_z.at[d, owner],
            recv_z.at[d, owner],
            q,
            beside(d),
        )

    def behind(d):
        return z > 0 if d == 0 else z < chips - 1

    def add_pair(owner):
        sum_pair(owner).wait_recv()
        place = partial.at[owner * 2 + core]
        both = place[...].astype(jnp.float32) + pair_in[owner].astype(jnp.float32)
        place[...] = both.astype(jnp.bfloat16)

    def add_line(d, owner):
        sum_leg(d, owner).wait_recv()
        place = partial.at[owner * 2 + core]
        both = place[...].astype(jnp.float32) + ring_in[d, owner].astype(jnp.float32)
        place[...] = both.astype(jnp.bfloat16)

    def send_sums(step):
        for d in range(2):
            far = z if d == 0 else chips - 1 - z
            owner = z + chips - 1 - step if d == 0 else z + step - chips + 1

            @pl.when(far <= step)
            def _(d=d, owner=owner):
                add_pair(owner)
                pl.when(behind(d))(lambda: add_line(d, owner))
                sum_leg(d, owner).start()

    order = []
    for j in range(chips):
        order += [o for o in (chips - 1 - j, j) if o not in order]
    for owner in order:
        sum_pair(owner).start()
    for s in range(2, steps):
        for k in range(3):
            take(k, s)
            if s + 1 < steps:
                pass_on(k, s + 1)
    send_sums(0)
    for k in range(3):
        if steps > 1:
            relay(k, 1)
    if steps > 1:
        send_sums(1)
    for k in range(3):
        if steps > 1:
            share(k, 1)
        for s in range(2, steps):
            relay(k, s)
    for s in range(2, steps):
        for k in range(3):
            share(k, s)
    if inside:
        glu_stage()
    for step in range(2, steps):
        send_sums(step)
    if inside:
        conv_stage()
    add_pair(z)
    if inside:
        out_stage()
    for d in range(2):
        pl.when(behind(d))(lambda d=d: add_line(d, z))
    summed = partial[t].astype(jnp.float32)
    back_out[...] = summed.astype(jnp.bfloat16)

    def back_leg(i):
        there = lax.rem(q + i, groups_ep)
        return remote(
            back_out.at[slot_rows(there), :],
            back_in.at[slot_rows(q), :],
            send_b.at[i],
            recv_b.at[i],
            there,
            t,
        )

    for i in range(1, groups_ep):
        back_leg(i).start()
    back_in[slot_rows(q), :] = back_out[slot_rows(q), :]
    for i in range(1, groups_ep):
        back_leg(i).wait_recv()
    returned[...] = back_in[...]

    for k in range(3):
        own_leg(k).wait_send()
        if not inside:
            wait_weight(k)
    if inside:
        pl.when(me < devices - 1)(lambda: halo().wait_send())
    own_pair().wait_send()
    for s in range(steps):
        for d in range(2):

            @pl.when(sends(d, s))
            def _(d=d, s=s):
                row_leg(d, s).wait_send()
                for k in range(3):
                    first_leg(k, d, s).wait_send()

            @pl.when(comes(d, s))
            def _(d=d, s=s):
                row_pair(d, s).wait_send()
                for k in range(3):
                    for j in direct + relayed:
                        second_leg(k, d, s, j).wait_send()
                    pair_leg(k, d, s).wait_send()
    for owner in range(chips):
        sum_pair(owner).wait_send()
        pl.when(z < owner)(lambda owner=owner: sum_leg(0, owner).wait_send())
        pl.when(z > owner)(lambda owner=owner: sum_leg(1, owner).wait_send())
    for i in range(1, groups_ep):
        a_copies[i - 1].wait_send()
        back_leg(i).wait_send()


def exchange(
    mixer_in,
    pre_gain,
    conv_kernel,
    chan_gain,
    mix_gain,
    outgoing,
    glu_value,
    glu_gate,
    out_weight,
    gate_proj,
    up_proj,
    down_proj,
    capacity,
):
    groups_ep, groups_tp = lax.axis_size("ep"), lax.axis_size("tp")
    chips = groups_tp // 2
    chunk, width = outgoing.shape
    units = gate_proj.shape[2] * gate_proj.shape[0]
    half = jnp.bfloat16

    def gathered(shard):
        rows, cols = shard.shape
        if cols % 128:
            return jax.ShapeDtypeStruct((groups_tp, rows, cols), half)
        return jax.ShapeDtypeStruct((rows, groups_tp * cols), half)

    own = (glu_value, glu_gate, out_weight)
    dma = pltpu.SemaphoreType.DMA
    inside = glu_value.shape[1] % 128 == 0 and out_weight.shape[1] % 128 == 0
    full_shapes = [gathered(shard) for shard in own]
    back_shape = jax.ShapeDtypeStruct((chunk, width), half)
    length, channels = mixer_in.shape[0], conv_kernel.shape[1]
    rim = -(-(conv_kernel.shape[0] - 1) // 8) * 8
    anywhere, vmem = pl.BlockSpec(memory_space=pl.ANY), pl.BlockSpec(memory_space=pltpu.VMEM)
    own_scratch = []
    if inside:
        own_scratch = [pltpu.VMEM(shape.shape, half) for shape in full_shapes] + [
            pltpu.VMEM(mixer_in.shape, half),
            pltpu.VMEM((rim + length, channels), jnp.float32),
            pltpu.VMEM((length, channels), jnp.float32),
            pltpu.VMEM((length, channels), half),
            pltpu.VMEM(mixer_in.shape, jnp.float32),
        ]
        mixer_specs = [vmem] * 5
    else:
        mixer_specs = [anywhere] * 5
    outs = pl.pallas_call(
        functools.partial(exchange_kernel, groups_ep, groups_tp, capacity, inside),
        out_shape=[jax.ShapeDtypeStruct(mixer_in.shape, half), back_shape]
        if inside
        else full_shapes + [back_shape],
        in_specs=[vmem] + mixer_specs + [anywhere] * 6,
        out_specs=[vmem] * 2 if inside else [anywhere] * 3 + [vmem],
        scratch_shapes=own_scratch
        + [
            pltpu.VMEM((groups_tp, chunk, width), half),
            pltpu.VMEM((groups_tp * chunk, units), half),
            pltpu.VMEM((groups_tp, chunk, width), half),
            pltpu.VMEM((chips, chunk, width), half),
            pltpu.VMEM((2, chips, chunk, width), half),
            pltpu.VMEM((chunk, width), half),
            pltpu.VMEM((chunk, width), half),
            pltpu.VMEM(gate_proj.shape, half),
            pltpu.VMEM(up_proj.shape, half),
            pltpu.VMEM(down_proj.shape, half),
            dma((3,)),
            dma((3,)),
            dma,
            dma,
            dma,
            dma((groups_ep,)),
            dma((groups_ep,)),
            dma((2, chips)),
            dma((2, chips)),
            dma((2, chips)),
            dma((2, chips)),
            dma((3, 2, chips)),
            dma((3, 2, chips)),
            dma((3, 2, chips, groups_ep)),
            dma((3, 2, chips, groups_ep)),
            dma((3, 2, chips)),
            dma((3, 2, chips)),
            dma((chips,)),
            dma((chips,)),
            dma((2, chips)),
            dma((2, chips)),
            dma((groups_ep,)),
            dma((groups_ep,)),
        ],
        compiler_params=pltpu.CompilerParams(
            collective_id=0, has_side_effects=True, vmem_limit_bytes=60 * 1024 * 1024
        ),
    )(
        outgoing,
        mixer_in,
        pre_gain[None],
        conv_kernel,
        chan_gain[None],
        mix_gain[None],
        *own,
        gate_proj,
        up_proj,
        down_proj,
    )
    if inside:
        return None, outs[0], outs[1]
    full = [
        value if value.ndim == 2 else value.transpose(1, 0, 2).reshape(value.shape[1], -1)
        for value in outs[:3]
    ]
    return full, None, outs[3]


def flipped(index, bit):
    return index + bit - 2 * bit * lax.rem(index // bit, 2)


def across(index, distance):
    bit = 1
    while bit <= distance:
        if distance & bit:
            index = flipped(index, bit)
        bit *= 2
    return index


def fused_kernel(
    groups_ep,
    groups_tp,
    capacity,
    expert_in_hbm,
    ffn_gain_hbm,
    routes_hbm,
    shares_hbm,
    expert_gain_hbm,
    mixer_hbm,
    pre_gain_hbm,
    conv_kernel_hbm,
    chan_gain_hbm,
    mix_gain_hbm,
    value_own,
    gate_own,
    out_own,
    gate_hbm,
    up_hbm,
    down_hbm,
    mixed,
    routed,
    expert_in,
    ffn_gain,
    routes,
    shares,
    expert_gain,
    pre_gain,
    conv_kernel,
    chan_gain,
    mix_gain,
    value_full,
    gate_full,
    out_full,
    mixer_in,
    normed,
    padded,
    tail_out,
    tail_in,
    conv,
    act,
    projected,
    info,
    rows_all,
    picked,
    hidden,
    partial,
    pair_in,
    ring_in,
    back_in,
    gate_vmem,
    up_vmem,
    down_vmem,
    load_sem,
    stage_sem,
    send_h,
    recv_h,
    send_rows,
    recv_rz,
    recv_rx,
    recv_rd,
    recv_rp,
    send_w1,
    recv_w1,
    send_w2,
    recv_w2,
    send_wp,
    recv_wp,
    send_p,
    recv_p,
    send_z,
    recv_z,
    send_b,
    recv_b,
):
    q = lax.axis_index("ep")
    t = lax.axis_index("tp")
    chips = groups_tp // 2
    z, core = t // 2, t % 2
    partner = z * 2 + 1 - core
    tokens, width = expert_in.shape
    slots = partial.shape[2]
    local_experts, _, units = gate_vmem.shape
    top_count = routes.shape[0]
    half_tokens = tokens // 2

    def remote(src, dst, send, recv, ep, tp):
        return pltpu.make_async_remote_copy(
            src_ref=src,
            dst_ref=dst,
            send_sem=send,
            recv_sem=recv,
            device_id=(ep, tp),
            device_id_type=pl.DeviceIdType.MESH,
        )

    barrier = pltpu.get_barrier_semaphore()
    others = [(lax.rem(q + i, groups_ep), t) for i in range(1, groups_ep)]
    others += [(q, lax.rem(z + i, chips) * 2 + core) for i in range(1, chips)]
    others += [(q, partner)]
    me, devices = q * groups_tp + t, groups_ep * groups_tp
    after, ahead = lax.rem(me + 1, devices), lax.rem(me + devices - 1, devices)
    others += [(n // groups_tp, lax.rem(n, groups_tp)) for n in (after, ahead)]
    for ep, tp in others:
        pl.semaphore_signal(
            barrier, inc=1, device_id=(ep, tp), device_id_type=pl.DeviceIdType.MESH
        )

    weights = ((value_own, value_full), (gate_own, gate_full), (out_own, out_full))
    stored = [
        pltpu.make_async_copy(
            own, columns(full, t, own.shape[1], pl.ds(0, own.shape[0])), stage_sem.at[k]
        )
        for k, (own, full) in enumerate(weights)
    ]
    def loaded(number, src, dst):
        return pltpu.make_async_copy(src, dst, load_sem.at[number])

    row_loads = [
        loaded(i, src, dst)
        for i, (src, dst) in enumerate(
            (
                (expert_in_hbm, expert_in),
                (ffn_gain_hbm, ffn_gain),
                (routes_hbm, routes),
                (shares_hbm, shares),
            )
        )
    ]
    mixer_loads = [
        loaded(4 + i, src, dst)
        for i, (src, dst) in enumerate(
            (
                (mixer_hbm, mixer_in),
                (pre_gain_hbm, pre_gain),
                (conv_kernel_hbm, conv_kernel),
                (chan_gain_hbm, chan_gain),
                (mix_gain_hbm, mix_gain),
                (expert_gain_hbm, expert_gain),
            )
        )
    ]
    loads = [
        loaded(10 + i, src, dst)
        for i, (src, dst) in enumerate(
            ((gate_hbm, gate_vmem), (up_hbm, up_vmem), (down_hbm, down_vmem))
        )
    ]
    for copy in row_loads + mixer_loads + stored + loads:
        copy.start()
    for copy in row_loads:
        copy.wait()

    rows_all[0, t, :, pl.ds(0, width)] = rms_scale(expert_in[...], ffn_gain[...]).astype(
        jnp.bfloat16
    )
    lanes = 128
    expert_ids = lax.broadcasted_iota(jnp.int32, (lanes, tokens), 0)
    chosen = [routes[pl.ds(k, 1), :] == expert_ids for k in range(top_count)]
    named = sum(c.astype(jnp.float32) for c in chosen)
    earlier = lax.broadcasted_iota(jnp.int32, (tokens, tokens), 0) < lax.broadcasted_iota(
        jnp.int32, (tokens, tokens), 1
    )
    rank = jnp.dot(
        named.astype(jnp.bfloat16),
        earlier.astype(jnp.float32).astype(jnp.bfloat16),
        preferred_element_type=jnp.float32,
    )
    group_ids = expert_ids // local_experts
    base = group_ids * slots + (expert_ids - group_ids * local_experts) * capacity
    spot = rank + base.astype(jnp.float32)
    facts = jnp.zeros((lanes, tokens), jnp.float32)
    for k in range(top_count):
        slot = jnp.sum(jnp.where(chosen[k], spot, 0.0), axis=0, keepdims=True)
        facts = facts + jnp.where(expert_ids == k, slot, 0.0)
        facts = facts + jnp.where(expert_ids == top_count + k, shares[pl.ds(k, 1), :], 0.0)
    info[...] = facts.T
    rows_all[0, t, :, pl.ds(width, lanes)] = info[...].astype(jnp.bfloat16)

    pl.semaphore_wait(barrier, len(others))

    def took(ref, sem):
        remote(ref, ref, sem, sem, q, partner).wait_send()

    def row_z(m):
        place = rows_all.at[0, t]
        return remote(place, place, send_rows.at[0], recv_rz.at[m], q, across(z, m) * 2 + core)

    def row_beside(b, m):
        owner = across(z, m) * 2 + core
        return remote(
            rows_all.at[0, owner],
            rows_all.at[1 + b, owner],
            send_rows.at[1],
            recv_rx.at[m],
            flipped(q, 1 + b),
            t,
        )

    def row_far(b, m):
        owner = across(z, m) * 2 + core
        some = pl.ds(b * half_tokens, half_tokens)
        return remote(
            rows_all.at[2 - b, owner, some, :],
            rows_all.at[3, owner, some, :],
            send_rows.at[2],
            recv_rd.at[m],
            flipped(q, 1 + b),
            t,
        )

    def row_pair(j, m):
        place = rows_all.at[j, across(z, m) * 2 + core]
        return remote(place, place, send_rows.at[3], recv_rp.at[j], q, partner)

    def rows_start():
        for m in range(1, chips):
            row_z(m).start()

    def rows_here(m):
        if m:
            took(rows_all.at[0, t], recv_rz.at[m])
        for b in range(2):
            row_beside(b, m).start()
        row_pair(0, m).start()

    def rows_beside(m):
        took(rows_all.at[0, pl.ds(0, 2)], recv_rx.at[m])
        for b in range(2):
            row_far(1 - b, m).start()
            row_pair(1 + b, m).start()

    def rows_far(m):
        took(rows_all.at[0, t], recv_rd.at[m])
        row_pair(3, m).start()

    def rows_left():
        took(rows_all.at[0, pl.ds(0, chips - 1)], send_rows.at[0])
        took(rows_all.at[0, pl.ds(0, 2 * chips)], send_rows.at[1])
        took(rows_all.at[0, pl.ds(0, chips)], send_rows.at[2])
        took(rows_all.at[:, pl.ds(0, chips)], send_rows.at[3])

    def sends(d, s):
        return (z >= s) & (z < chips - 1) if d == 0 else (z + s < chips) & (z > 0)

    def comes(d, s):
        return z >= 1 + s if d == 0 else z + 1 + s < chips

    def sent(d, s):
        return (z - s if d == 0 else z + s) * 2 + core

    def came(d, s):
        return sent(d, s + 1)

    def beside(d):
        return t + 2 if d == 0 else t - 2

    def quarter(k, index, cut=0):
        own = weights[k][0]
        part = own.shape[0] // groups_ep
        if cut == 0:
            return pl.ds(pl.multiple_of(index * part, part), part)
        half = part // 2
        return pl.ds(pl.multiple_of(index * part + (cut - 1) * half, half), half)

    bundles = ((0, 1), (2,))

    def first_leg(g, k, d, s):
        own, full = weights[k]
        place = columns(full, sent(d, s), own.shape[1], quarter(k, q))
        src = own.at[quarter(k, q), :] if s == 0 else place
        return remote(src, place, send_w1.at[d, s], recv_w1.at[g, d, s], q, beside(d))

    flip_low, flip_high = flipped(q, 1), flipped(q, 2)
    direct, relayed = (1, 2), (0, 3)

    def second_leg(g, k, d, s, j):
        own, full = weights[k]
        piece = (flip_high, q, q, flip_low)[j]
        there = (flip_low, flip_low, flip_high, flip_high)[j]
        cut = (2, 0, 0, 1)[j]
        place = columns(full, came(d, s), own.shape[1], quarter(k, piece, cut))
        kind = 0 if j in direct else 1
        return remote(
            place, place, send_w2.at[d, s], recv_w2.at[g, kind, d, s], there, t
        )

    def own_leg(g, k):
        own, full = weights[k]
        place = columns(full, t, own.shape[1], pl.ds(0, own.shape[0]))
        last = chips - 1
        return remote(own, place, send_wp.at[0, last], recv_wp.at[g, 0, last], q, partner)

    def pair_leg(g, k, d, s):
        own, full = weights[k]
        place = columns(full, came(d, s), own.shape[1], pl.ds(0, own.shape[0]))
        return remote(place, place, send_wp.at[d, s], recv_wp.at[g, d, s], q, partner)

    share_rows, share_wide = value_own.shape

    def took_shares(quarters, sem):
        tall = max(r for r in range(1, groups_ep + 1) if quarters % r == 0)
        rows = pl.ds(0, share_rows // groups_ep * tall)
        took(value_full.at[rows, pl.ds(0, quarters // tall * share_wide)], sem)

    def passes(g, s):
        for d in range(2):

            @pl.when(sends(d, s))
            def _(d=d):
                for k in bundles[g]:
                    first_leg(g, k, d, s).start()

    def own_legs(g):
        for k in bundles[g]:
            own_leg(g, k).start()

    def takes(g, s):
        for d in range(2):

            @pl.when(comes(d, s))
            def _(d=d):
                took_shares(len(bundles[g]), recv_w1.at[g, d, s])
                if s + 1 < steps:

                    @pl.when(sends(d, s + 1))
                    def _():
                        for k in bundles[g]:
                            first_leg(g, k, d, s + 1).start()

                for j in direct:
                    for k in bundles[g]:
                        second_leg(g, k, d, s, j).start()

    def relays(g, s):
        for d in range(2):

            @pl.when(comes(d, s))
            def _(d=d):
                took_shares(2 * len(bundles[g]), recv_w2.at[g, 0, d, s])
                for j in relayed:
                    for k in bundles[g]:
                        second_leg(g, k, d, s, j).start()

    def shares_on(g, s):
        for d in range(2):

            @pl.when(comes(d, s))
            def _(d=d):
                took_shares(len(bundles[g]), recv_w2.at[g, 1, d, s])
                for k in bundles[g]:
                    pair_leg(g, k, d, s).start()

    def wait_plane(g, m):
        if m == 0:
            for k in bundles[g]:
                stored[k].wait()
            took_shares(groups_ep * len(bundles[g]), recv_wp.at[g, 0, chips - 1])
            return
        plane = across(z, m)
        d = (plane > z).astype(jnp.int32)
        s = (plane - z) * (2 * d - 1) - 1
        took_shares(groups_ep * len(bundles[g]), recv_wp.at[g, d, s])

    def shares_left():
        took_shares(3 * groups_ep, send_wp.at[0, chips - 1])
        for s in range(steps):
            for d in range(2):

                @pl.when(sends(d, s))
                def _(d=d, s=s):
                    took_shares(3, send_w1.at[d, s])

                @pl.when(comes(d, s))
                def _(d=d, s=s):
                    took_shares(9, send_w2.at[d, s])
                    took_shares(3 * groups_ep, send_wp.at[d, s])

    length = mixer_in.shape[0]
    rim = padded.shape[1] - length
    lane_blocks = padded.shape[0]

    def norm_stage():
        for copy in mixer_loads:
            copy.wait()
        some = min(64, length)

        @pl.loop(0, length // some)
        def _(step):
            place = pl.ds(pl.multiple_of(step * some, some), some)
            normed[place, :] = rms_scale(mixer_in[place, :], pre_gain[...]).astype(jnp.bfloat16)

    def glu_stage(m):
        wait_plane(0, m)
        wide = 2 * value_own.shape[1]
        place = pl.ds(pl.multiple_of(across(z, m) * wide, wide), wide)
        rows = normed[...]
        value = jnp.dot(rows, value_full[:, place], preferred_element_type=jnp.float32)
        gate = jnp.dot(rows, gate_full[:, place], preferred_element_type=jnp.float32)
        glu = (value * jax.nn.sigmoid(gate)).astype(jnp.bfloat16)
        for i in range(wide // lanes):
            padded[across(z, m) * (wide // lanes) + i, pl.ds(rim, length), :] = glu[
                :, i * lanes : (i + 1) * lanes
            ].astype(jnp.float32)
        tail_out[:, place] = glu[length - rim :, :]

    def halo():
        return remote(
            tail_out, tail_in, send_h, recv_h, after // groups_tp, lax.rem(after, groups_tp)
        )

    def halo_start():
        pl.when(me < devices - 1)(lambda: halo().start())

    def conv_start():
        @pl.when(me > 0)
        def _():
            halo().wait_recv()
            for i in range(lane_blocks):
                padded[i, pl.ds(0, rim), :] = tail_in[:, i * lanes : (i + 1) * lanes].astype(
                    jnp.float32
                )

        @pl.when(me == 0)
        def _():
            padded[:, pl.ds(0, rim), :] = jnp.zeros((lane_blocks, rim, lanes), jnp.float32)

    def conv_stage(part):
        taps = conv_kernel.shape[0]
        here = lane_blocks // chips

        @pl.loop(part * here, (part + 1) * here)
        def _(step):
            place = pl.ds(pl.multiple_of(step * lanes, lanes), lanes)
            total = jnp.zeros((length, lanes), jnp.float32)
            for tap in range(taps):
                rows = padded[step, pl.ds(rim - taps + 1 + tap, length), :]
                total = total + conv_kernel[pl.ds(tap, 1), place] * rows
            conv[:, place] = total

    def act_stage():
        some = min(64, length)

        @pl.loop(0, length // some)
        def _(step):
            place = pl.ds(pl.multiple_of(step * some, some), some)
            block = conv[place, :]
            centred = block - jnp.mean(block, axis=-1, keepdims=True)
            var = jnp.mean(centred * centred, axis=-1, keepdims=True)
            scaled = centred * lax.rsqrt(var + LAYER_EPSILON) * chan_gain[...]
            act[place, :] = (scaled * jax.nn.sigmoid(scaled)).astype(jnp.bfloat16)

    def out_stage(m):
        wait_plane(1, m)
        wide = out_own.shape[1]
        start = across(z, m) * 2 * wide
        for i in range(2):
            place = pl.ds(pl.multiple_of(start + i * wide, wide), wide)
            projected[:, place] = jnp.dot(
                act[...], out_full[:, place], preferred_element_type=jnp.float32
            )

    def mixed_stage():
        some = min(64, length)

        @pl.loop(0, length // some)
        def _(step):
            place = pl.ds(pl.multiple_of(step * some, some), some)
            mixed[place, :] = rms_scale(projected[place, :], mix_gain[...]).astype(jnp.bfloat16)

    total = groups_tp * slots
    tile = min(512, units)
    tiles = units // tile
    down_tile = min(512, width)

    def pick_stage(j):
        took(rows_all.at[0, pl.ds(0, chips)], recv_rp.at[j])
        if j == 0:
            for copy in loads:
                copy.wait()
        every = groups_tp * tokens
        block = rows_all[j].reshape(every, width + lanes)
        facts = block[:, width:].astype(jnp.float32)
        slot_ids = lax.broadcasted_iota(jnp.int32, (every, total), 1).astype(jnp.float32)
        owner = lax.broadcasted_iota(jnp.int32, (every, 1), 0) // tokens
        first = (owner * slots).astype(jnp.float32)
        low = (q * slots).astype(jnp.float32)
        pick = jnp.zeros((every, total), jnp.float32)
        for k in range(top_count):
            local = facts[:, k : k + 1] - low
            mine = (local >= 0.0) & (local < float(slots))
            target = jnp.where(mine, local + first, -1.0)
            pick = pick + (target == slot_ids).astype(jnp.float32)
        picked[...] = jnp.dot(
            pick.T.astype(jnp.bfloat16), block[:, :width], preferred_element_type=jnp.float32
        ).astype(jnp.bfloat16)

    def up_stage(j, expert):
        @pl.loop(0, tiles)
        def _(unit):
            step = expert * tiles + unit
            place = pl.ds(pl.multiple_of(unit * tile, tile), tile)
            rows = picked[...]
            gate = jnp.dot(rows, gate_vmem[expert, :, place], preferred_element_type=jnp.float32)
            up = jnp.dot(rows, up_vmem[expert, :, place], preferred_element_type=jnp.float32)
            gate = jnp.minimum(gate, CLAMP_LIMIT)
            up = jnp.clip(up, -CLAMP_LIMIT, CLAMP_LIMIT)
            unit_act = (up + 1.0) * gate * jax.nn.sigmoid(SWISH_ALPHA * gate)
            slot = lax.rem(lax.broadcasted_iota(jnp.int32, unit_act.shape, 0), slots)
            mine = (slot >= expert * capacity) & (slot < (expert + 1) * capacity)
            hidden[:, pl.ds(pl.multiple_of(step * tile, tile), tile)] = jnp.where(
                mine, unit_act, 0.0
            ).astype(jnp.bfloat16)

    def down_stage(j):
        @pl.loop(0, width // down_tile)
        def _(step):
            place = pl.ds(pl.multiple_of(step * down_tile, down_tile), down_tile)
            weight = down_vmem[:, :, place].reshape(local_experts * units, down_tile)
            part = jnp.dot(hidden[...], weight, preferred_element_type=jnp.float32)
            partial[j, :, :, place] = part.astype(jnp.bfloat16).reshape(
                groups_tp, slots, down_tile
            )

        for owner in owners:
            sum_pair(j, owner).start()

    owners = []
    for i in range(chips):
        owners += [o for o in (chips - 1 - i, i) if o not in owners]

    def sum_pair(j, owner):
        return remote(
            partial.at[j, owner * 2 + 1 - core],
            pair_in.at[j, owner],
            send_p.at[j],
            recv_p.at[j],
            q,
            partner,
        )

    def owner_of(d, step):
        return z + chips - 1 - step if d == 0 else z + step - chips + 1

    def sum_leg(j, d, step):
        owner = owner_of(d, step)
        return remote(
            partial.at[j, owner * 2 + core],
            ring_in.at[j, d, owner],
            send_z.at[d, step],
            recv_z.at[j, d, step],
            q,
            beside(d),
        )

    def behind(d):
        return z > 0 if d == 0 else z < chips - 1

    def add_to(j, owner, other):
        place = partial.at[j, owner * 2 + core]
        both = place[...].astype(jnp.float32) + other[...].astype(jnp.float32)
        place[...] = both.astype(jnp.bfloat16)

    def add_line(j, d, owner, step):
        took(partial.at[j, t], recv_z.at[j, d, step])
        add_to(j, owner, ring_in.at[j, d, owner])

    def send_sums(j, step):
        if step == 0:
            took(pair_in.at[j], recv_p.at[j])
        for d in range(2):
            far = z if d == 0 else chips - 1 - z

            @pl.when(far <= step)
            def _(d=d):
                owner = owner_of(d, step)
                add_to(j, owner, pair_in.at[j, owner])
                if step:
                    pl.when(behind(d))(lambda: add_line(j, d, owner, step - 1))
                sum_leg(j, d, step).start()

    def back_leg(j):
        return remote(
            partial.at[j, t], back_in.at[j - 1], send_b, recv_b, across(q, j), t
        )

    def own_sums(j):
        add_to(j, z, pair_in.at[j, z])
        for d in range(2):
            pl.when(behind(d))(lambda d=d: add_line(j, d, z, chips - 2))
        if j:
            back_leg(j).start()

    def sums_left():
        for j in range(groups_ep):
            took(pair_in.at[j], send_p.at[j])
        for d in range(2):
            far = z if d == 0 else chips - 1 - z
            for step in range(steps):
                pl.when(far <= step)(
                    lambda d=d, step=step: took(partial.at[:, 0], send_z.at[d, step])
                )
        took(back_in, send_b)

    def routed_stage():
        took(back_in, recv_b)
        facts = info[...]
        total_rows = jnp.zeros((tokens, width), jnp.float32)
        slot_ids = lax.broadcasted_iota(jnp.int32, (tokens, slots), 1)
        for j in range(groups_ep):
            block = partial[0, t] if j == 0 else back_in[j - 1]
            low = across(q, j) * slots
            shared = jnp.zeros((tokens, slots), jnp.float32)
            for k in range(top_count):
                here = facts[:, k : k + 1] == (slot_ids + low).astype(jnp.float32)
                share_of = facts[:, top_count + k : top_count + k + 1]
                shared = shared + jnp.where(here, share_of, 0.0)
            high = shared.astype(jnp.bfloat16)
            rest = (shared - high.astype(jnp.float32)).astype(jnp.bfloat16)
            for term in (high, rest):
                total_rows = total_rows + jnp.dot(
                    term, block, preferred_element_type=jnp.float32
                )
        routed[...] = rms_scale(total_rows, expert_gain[...]).astype(jnp.bfloat16)

    steps = chips - 1
    rows_start()
    rows_here(0)
    rows_beside(0)
    rows_far(0)
    rows_here(1)
    rows_here(2)
    rows_beside(1)
    norm_stage()
    passes(0, 0)
    rows_beside(2)
    rows_here(3)
    own_legs(1)
    pick_stage(0)
    up_stage(0, 0)
    up_stage(0, 1)
    takes(0, 0)
    rows_beside(3)
    down_stage(0)
    pick_stage(1)
    up_stage(1, 0)
    passes(1, 0)
    send_sums(0, 0)
    up_stage(1, 1)
    down_stage(1)
    pick_stage(2)
    own_legs(0)
    takes(0, 1)
    send_sums(1, 0)
    relays(0, 0)
    up_stage(2, 0)
    up_stage(2, 1)
    takes(1, 0)
    down_stage(2)
    rows_far(1)
    rows_far(2)
    send_sums(2, 0)
    rows_far(3)
    pick_stage(3)
    takes(0, 2)
    send_sums(1, 1)
    up_stage(3, 0)
    up_stage(3, 1)
    relays(0, 1)
    send_sums(0, 1)
    takes(1, 1)
    send_sums(0, 2)
    down_stage(3)
    send_sums(3, 0)
    send_sums(2, 1)
    relays(0, 2)
    takes(1, 2)
    send_sums(3, 1)
    shares_on(0, 0)
    send_sums(1, 2)
    glu_stage(0)
    glu_stage(1)
    relays(1, 0)
    send_sums(3, 2)
    shares_on(0, 1)
    send_sums(2, 2)
    own_sums(0)
    relays(1, 1)
    shares_on(0, 2)
    relays(1, 2)
    glu_stage(3)
    glu_stage(2)
    own_sums(3)
    halo_start()
    conv_start()
    own_sums(1)
    conv_stage(3)
    shares_on(1, 0)
    conv_stage(2)
    conv_stage(0)
    shares_on(1, 1)
    own_sums(2)
    conv_stage(1)
    shares_on(1, 2)
    act_stage()
    out_stage(1)
    out_stage(0)
    out_stage(2)
    out_stage(3)
    mixed_stage()
    routed_stage()

    rows_left()
    shares_left()
    pl.when(me < devices - 1)(lambda: halo().wait_send())
    sums_left()


def fused(
    mixer_in,
    pre_gain,
    glu_value,
    glu_gate,
    conv_kernel,
    chan_gain,
    out_weight,
    mix_gain,
    expert_in,
    ffn_gain,
    routing,
    route_weight,
    gate_proj,
    up_proj,
    down_proj,
    expert_gain,
    capacity,
    slots,
):
    groups_ep, groups_tp = lax.axis_size("ep"), lax.axis_size("tp")
    chips = groups_tp // 2
    tokens, width = expert_in.shape
    length, channels = mixer_in.shape[0], conv_kernel.shape[1]
    units = gate_proj.shape[2] * gate_proj.shape[0]
    half, full = jnp.bfloat16, jnp.float32
    dma = pltpu.SemaphoreType.DMA
    rim = -(-(conv_kernel.shape[0] - 1) // 8) * 8
    vmem = pl.BlockSpec(memory_space=pltpu.VMEM)

    def gathered(shard):
        return pltpu.VMEM((shard.shape[0], groups_tp * shard.shape[1]), half)

    return pl.pallas_call(
        functools.partial(fused_kernel, groups_ep, groups_tp, capacity),
        out_shape=[
            jax.ShapeDtypeStruct(mixer_in.shape, half),
            jax.ShapeDtypeStruct(expert_in.shape, half),
        ],
        in_specs=[pl.BlockSpec(memory_space=pltpu.HBM)] * 16,
        out_specs=[vmem] * 2,
        scratch_shapes=[
            pltpu.VMEM(expert_in.shape, half),
            pltpu.VMEM((1, width), full),
            pltpu.VMEM(routing.shape[::-1], routing.dtype),
            pltpu.VMEM(route_weight.shape[::-1], full),
            pltpu.VMEM((1, width), full),
            pltpu.VMEM((1, width), full),
            pltpu.VMEM(conv_kernel.shape, full),
            pltpu.VMEM((1, channels), full),
            pltpu.VMEM((1, width), full),
            gathered(glu_value),
            gathered(glu_gate),
            gathered(out_weight),
            pltpu.VMEM(mixer_in.shape, half),
            pltpu.VMEM(mixer_in.shape, half),
            pltpu.VMEM((channels // 128, rim + length, 128), full),
            pltpu.VMEM((rim, channels), half),
            pltpu.VMEM((rim, channels), half),
            pltpu.VMEM((length, channels), full),
            pltpu.VMEM((length, channels), half),
            pltpu.VMEM(mixer_in.shape, full),
            pltpu.VMEM((tokens, 128), full),
            pltpu.VMEM((groups_ep, groups_tp, tokens, width + 128), half),
            pltpu.VMEM((groups_tp * slots, width), half),
            pltpu.VMEM((groups_tp * slots, units), half),
            pltpu.VMEM((groups_ep, groups_tp, slots, width), half),
            pltpu.VMEM((groups_ep, chips, slots, width), half),
            pltpu.VMEM((groups_ep, 2, chips, slots, width), half),
            pltpu.VMEM((groups_ep - 1, slots, width), half),
            pltpu.VMEM(gate_proj.shape, half),
            pltpu.VMEM(up_proj.shape, half),
            pltpu.VMEM(down_proj.shape, half),
            dma((13,)),
            dma((3,)),
            dma,
            dma,
            dma((4,)),
            dma((chips,)),
            dma((chips,)),
            dma((chips,)),
            dma((groups_ep,)),
            dma((2, chips - 1)),
            dma((2, 2, chips - 1)),
            dma((2, chips - 1)),
            dma((2, 2, 2, chips - 1)),
            dma((2, chips)),
            dma((2, 2, chips)),
            dma((groups_ep,)),
            dma((groups_ep,)),
            dma((2, chips - 1)),
            dma((groups_ep, 2, chips - 1)),
            dma,
            dma,
        ],
        compiler_params=pltpu.CompilerParams(
            collective_id=0, has_side_effects=True, vmem_limit_bytes=60 * 1024 * 1024
        ),
    )(
        expert_in,
        ffn_gain[None],
        routing.T,
        route_weight.T,
        expert_gain[None],
        mixer_in,
        pre_gain[None],
        conv_kernel,
        chan_gain[None],
        mix_gain[None],
        glu_value,
        glu_gate,
        out_weight,
        gate_proj,
        up_proj,
        down_proj,
    )


def mixer(full, mixer_in, pre_gain, conv_kernel, chan_gain, mix_gain):
    value_full, gate_full, out_full = full
    normed_mix = rms_scale(mixer_in, pre_gain).astype(jnp.bfloat16)
    value_pre = jnp.dot(normed_mix, value_full, preferred_element_type=jnp.float32)
    gate_mix = jnp.dot(normed_mix, gate_full, preferred_element_type=jnp.float32)
    gated_rows = (value_pre * jax.nn.sigmoid(gate_mix)).astype(jnp.bfloat16)
    kernel_width = conv_kernel.shape[0]
    length = gated_rows.shape[0]
    rim_rows = passed_along(gated_rows[length - (kernel_width - 1) :], ("ep", "tp"), 1)
    padded = jnp.concatenate([rim_rows, gated_rows], axis=0).astype(jnp.float32)
    conv_sum = jnp.zeros((length, gated_rows.shape[1]), jnp.float32)
    for offset in range(kernel_width):
        conv_sum = conv_sum + conv_kernel[offset] * padded[offset : offset + length]
    row_mean = jnp.mean(conv_sum, axis=-1, keepdims=True)
    centred = conv_sum - row_mean
    row_var = jnp.mean(centred * centred, axis=-1, keepdims=True)
    activated = jax.nn.silu(centred * lax.rsqrt(row_var + LAYER_EPSILON) * chan_gain).astype(
        jnp.bfloat16
    )
    projected = jnp.dot(activated, out_full, preferred_element_type=jnp.float32)
    mixed = rms_scale(projected, mix_gain).astype(jnp.bfloat16)
    return mixed


def on_device(
    mixer_in,
    pre_gain,
    glu_value,
    glu_gate,
    conv_kernel,
    chan_gain,
    out_weight,
    mix_gain,
    expert_in,
    ffn_gain,
    routing,
    route_weight,
    gate_proj,
    up_proj,
    down_proj,
    expert_gain,
):
    groups_ep = lax.axis_size("ep")
    local_experts = gate_proj.shape[0]
    experts = local_experts * groups_ep
    token_rows, top_count = routing.shape
    capacity = max(2, 3 * token_rows * top_count // (2 * experts))
    slots = -(-local_experts * capacity // 8) * 8
    chips = lax.axis_size("tp") // 2
    lined_up = all(w.shape[1] % 128 == 0 for w in (glu_value, glu_gate, out_weight))
    two_way = groups_ep == 4 and chips > 1 and chips & (chips - 1) == 0
    if lined_up and two_way and groups_ep * slots <= 256:
        return tuple(
            fused(
                mixer_in,
                pre_gain,
                glu_value,
                glu_gate,
                conv_kernel,
                chan_gain,
                out_weight,
                mix_gain,
                expert_in,
                ffn_gain,
                routing,
                route_weight,
                gate_proj,
                up_proj,
                down_proj,
                expert_gain,
                capacity,
                slots,
            )
        )
    flat_route = routing.reshape(-1)
    onehot = (flat_route[:, None] == jnp.arange(experts, dtype=jnp.int32)[None, :]).astype(
        jnp.int32
    )
    before = jnp.cumsum(onehot, axis=0) - onehot
    rank_within = jnp.sum(before * onehot, axis=1)
    slot_index = (
        flat_route // local_experts * slots + flat_route % local_experts * capacity + rank_within
    ).reshape(token_rows, top_count)
    slot_ids = jnp.arange(groups_ep * slots, dtype=jnp.int32)
    chosen = slot_index[None, :, :] == slot_ids[:, None, None]
    pick_matrix = jnp.sum(chosen.astype(jnp.float32), axis=2).astype(jnp.bfloat16)
    normed_exp = rms_scale(expert_in, ffn_gain).astype(jnp.bfloat16)
    outgoing = jnp.dot(pick_matrix, normed_exp, preferred_element_type=jnp.float32).astype(
        jnp.bfloat16
    )
    full, mixed, returned = exchange(
        mixer_in,
        pre_gain,
        conv_kernel,
        chan_gain,
        mix_gain,
        outgoing,
        glu_value,
        glu_gate,
        out_weight,
        gate_proj,
        up_proj,
        down_proj,
        capacity,
    )
    if mixed is None:
        mixed = mixer(full, mixer_in, pre_gain, conv_kernel, chan_gain, mix_gain)
    combined = jnp.zeros((token_rows, returned.shape[1]), jnp.float32)
    for column in range(top_count):
        combined = combined + route_weight[:, column][:, None] * returned[
            slot_index[:, column]
        ].astype(jnp.float32)
    routed = rms_scale(combined, expert_gain).astype(jnp.bfloat16)
    return (mixed, routed)


def solution(mesh):
    in_specs = (
        P(("ep", "tp"), None),
        P(),
        P(None, "tp"),
        P(None, "tp"),
        P(),
        P(),
        P(None, "tp"),
        P(),
        P(("ep", "tp"), None),
        P(),
        P(("ep", "tp"), None),
        P(("ep", "tp"), None),
        P("ep", None, "tp"),
        P("ep", None, "tp"),
        P("ep", "tp", None),
        P(),
    )
    out_specs = (P(("ep", "tp"), None), P(("ep", "tp"), None))
    return jax.shard_map(
        on_device, mesh=mesh, in_specs=in_specs, out_specs=out_specs, check_vma=False
    )
```

```python
import functools

import jax
import jax.numpy as jnp
from jax import lax
from jax.experimental import pallas as pl
from jax.experimental.pallas import tpu as pltpu
from jax.sharding import PartitionSpec as P

RMS_EPSILON = 1e-06
LAYER_EPSILON = 1e-05
CLAMP_LIMIT = 7.0
SWISH_ALPHA = 1.702


def passed_along(value, axis, steps):
    count = lax.axis_size(axis)
    initial, last = (max(0, -steps), min(count, count - steps))
    return lax.ppermute(value, axis, [(source, source + steps) for source in range(initial, last)])


def rms_scale(values, gain_row):
    values = values.astype(jnp.float32)
    return (
        values
        * lax.rsqrt(jnp.mean(values * values, axis=-1, keepdims=True) + RMS_EPSILON)
        * gain_row
    )


def columns(ref, owner, width, rows):
    if len(ref.shape) == 3:
        return ref.at[owner, rows, :]
    return ref.at[rows, pl.ds(pl.multiple_of(owner * width, width), width)]


def exchange_kernel(
    groups_ep,
    groups_tp,
    capacity,
    inside,
    outgoing,
    mixer_in,
    pre_gain,
    conv_kernel,
    chan_gain,
    mix_gain,
    value_own,
    gate_own,
    out_own,
    gate_hbm,
    up_hbm,
    down_hbm,
    *rest,
):
    if inside:
        mixed, returned, value_full, gate_full, out_full, *rest = rest
        normed, padded, conv, act, projected, *rest = rest
    else:
        value_full, gate_full, out_full, returned, *rest = rest
    (
    rows_all,
    hidden,
    partial,
    pair_in,
    ring_in,
    back_out,
    back_in,
    gate_vmem,
    up_vmem,
    down_vmem,
    load_sem,
    stage_sem,
    send_h,
    recv_h,
    own_sem,
    send_a,
    recv_a,
    send_r,
    recv_r,
    send_rp,
    recv_rp,
    send_w1,
    recv_w1,
    send_w2,
    recv_w2,
    send_wp,
    recv_wp,
    send_p,
    recv_p,
    send_z,
    recv_z,
    send_b,
    recv_b,
    ) = rest
    q = lax.axis_index("ep")
    t = lax.axis_index("tp")
    chips = groups_tp // 2
    z, core = t // 2, t % 2
    partner = z * 2 + 1 - core
    chunk, width = rows_all.shape[1], rows_all.shape[2]
    slots = chunk // groups_ep
    local_experts, _, units = gate_vmem.shape

    def remote(src, dst, send, recv, ep, tp):
        return pltpu.make_async_remote_copy(
            src_ref=src,
            dst_ref=dst,
            send_sem=send,
            recv_sem=recv,
            device_id=(ep, tp),
            device_id_type=pl.DeviceIdType.MESH,
        )

    barrier = pltpu.get_barrier_semaphore()
    others = [(lax.rem(q + i, groups_ep), t) for i in range(1, groups_ep)]
    others += [(q, lax.rem(z + i, chips) * 2 + core) for i in range(1, chips)]
    others += [(q, partner)]
    me, devices = q * groups_tp + t, groups_ep * groups_tp
    after, ahead = lax.rem(me + 1, devices), lax.rem(me + devices - 1, devices)
    others += [(n // groups_tp, lax.rem(n, groups_tp)) for n in (after, ahead)]

    def greet(ep, tp):
        pl.semaphore_signal(
            barrier, inc=1, device_id=(ep, tp), device_id_type=pl.DeviceIdType.MESH
        )

    for ep, tp in others:
        greet(ep, tp)

    loads = [
        pltpu.make_async_copy(src, dst, load_sem.at[i])
        for i, (src, dst) in enumerate(
            ((gate_hbm, gate_vmem), (up_hbm, up_vmem), (down_hbm, down_vmem))
        )
    ]
    weights = ((value_own, value_full), (gate_own, gate_full), (out_own, out_full))
    pl.semaphore_wait(barrier, len(others))

    def slot_rows(index):
        return pl.ds(pl.multiple_of(index * slots, slots), slots)

    own_rows = pltpu.make_async_copy(
        outgoing.at[slot_rows(q), :], rows_all.at[t, slot_rows(q), :], own_sem
    )
    own_rows.start()
    a_copies = []
    for i in range(1, groups_ep):
        there = lax.rem(q + i, groups_ep)
        copy = remote(
            outgoing.at[slot_rows(there), :],
            rows_all.at[t, slot_rows(q), :],
            send_a.at[i],
            recv_a.at[i],
            there,
            t,
        )
        copy.start()
        a_copies.append(copy)

    def sends(d, s):
        return (z >= s) & (z < chips - 1) if d == 0 else (z + s < chips) & (z > 0)

    def comes(d, s):
        return z >= 1 + s if d == 0 else z + 1 + s < chips

    def sent(d, s):
        return (z - s if d == 0 else z + s) * 2 + core

    def came(d, s):
        return sent(d, s + 1)

    def beside(d):
        return t + 2 if d == 0 else t - 2

    def quarter(k, index, cut=0):
        own = weights[k][0]
        part = own.shape[0] // groups_ep
        if cut == 0:
            return pl.ds(pl.multiple_of(index * part, part), part)
        half = part // 2
        return pl.ds(pl.multiple_of(index * part + (cut - 1) * half, half), half)

    def first_leg(k, d, s):
        own, full = weights[k]
        place = columns(full, sent(d, s), own.shape[1], quarter(k, q))
        src = own.at[quarter(k, q), :] if s == 0 else place
        return remote(src, place, send_w1.at[k, d, s], recv_w1.at[k, d, s], q, beside(d))

    flip_low = q + 1 - 2 * lax.rem(q, 2)
    flip_high = q + 2 - 4 * lax.rem(q // 2, 2)
    square = groups_ep == 4

    def second_leg(k, d, s, j):
        own, full = weights[k]
        piece, there, cut = q, lax.rem(q + j, groups_ep), 0
        if square:
            piece = (flip_high, q, q, flip_low)[j]
            there = (flip_low, flip_low, flip_high, flip_high)[j]
            cut = (2, 0, 0, 1)[j]
        place = columns(full, came(d, s), own.shape[1], quarter(k, piece, cut))
        return remote(
            place, place, send_w2.at[k, d, s, j], recv_w2.at[k, d, s, j], there, t
        )

    direct = (1, 2) if square else tuple(range(1, groups_ep))
    relayed = (0, 3) if square else ()

    def own_leg(k):
        own, full = weights[k]
        place = columns(full, t, own.shape[1], pl.ds(0, own.shape[0]))
        last = chips - 1
        return remote(own, place, send_wp.at[k, 0, last], recv_wp.at[k, 0, last], q, partner)

    def pair_leg(k, d, s):
        own, full = weights[k]
        place = columns(full, came(d, s), own.shape[1], pl.ds(0, own.shape[0]))
        return remote(place, place, send_wp.at[k, d, s], recv_wp.at[k, d, s], q, partner)

    def pass_on(k, s):
        for d in range(2):
            pl.when(sends(d, s))(lambda d=d: first_leg(k, d, s).start())

    def take(k, s):
        for d in range(2):

            @pl.when(comes(d, s))
            def _(d=d):
                first_leg(k, d, s).wait_recv()
                for j in direct:
                    second_leg(k, d, s, j).start()

    def relay(k, s):
        for d in range(2):

            @pl.when(comes(d, s))
            def _(d=d):
                for j in direct:
                    second_leg(k, d, s, j).wait_recv()
                for j in relayed:
                    second_leg(k, d, s, j).start()

    def share(k, s):
        for d in range(2):

            @pl.when(comes(d, s))
            def _(d=d):
                for j in relayed:
                    second_leg(k, d, s, j).wait_recv()
                pair_leg(k, d, s).start()

    def row_leg(d, s):
        place = rows_all.at[sent(d, s)]
        return remote(place, place, send_r.at[d, s], recv_r.at[d, s], q, beside(d))

    def row_pair(d, s):
        place = rows_all.at[came(d, s)]
        return remote(place, place, send_rp.at[d, s], recv_rp.at[d, s], q, partner)

    def own_pair():
        place, last = rows_all.at[t], chips - 1
        return remote(place, place, send_rp.at[0, last], recv_rp.at[0, last], q, partner)

    def rows_on(s):
        for d in range(2):
            pl.when(sends(d, s))(lambda d=d: row_leg(d, s).start())

    def rows_in(s):
        for d in range(2):
            pl.when(comes(d, s))(lambda d=d: row_leg(d, s).wait_recv())

    def rows_share(s):
        for d in range(2):
            pl.when(comes(d, s))(lambda d=d: row_pair(d, s).start())

    steps = chips - 1
    for k in (0,):
        pass_on(k, 0)
    stored = [
        pltpu.make_async_copy(
            own, columns(full, t, own.shape[1], pl.ds(0, own.shape[0])), stage_sem.at[k]
        )
        for k, (own, full) in enumerate(weights)
    ]
    for copy in loads + stored:
        copy.start()
    if inside:
        rim = padded.shape[0] - mixer_in.shape[0]
        length = mixer_in.shape[0]
        normed[...] = rms_scale(mixer_in[...], pre_gain[...]).astype(jnp.bfloat16)

        @pl.when(me == 0)
        def _():
            padded[pl.ds(0, rim), :] = jnp.zeros((rim, padded.shape[1]), jnp.float32)

    def halo():
        return remote(
            padded.at[pl.ds(length, rim), :],
            padded.at[pl.ds(0, rim), :],
            send_h,
            recv_h,
            after // groups_tp,
            lax.rem(after, groups_tp),
        )

    def wait_weight(k):
        stored[k].wait()
        own_leg(k).wait_recv()
        for s in range(steps):
            for d in range(2):
                pl.when(comes(d, s))(lambda d=d, s=s: pair_leg(k, d, s).wait_recv())

    def glu_stage():
        wait_weight(0)
        wait_weight(1)
        wide = min(256, value_full.shape[1])

        @pl.loop(0, value_full.shape[1] // wide)
        def _(step):
            place = pl.ds(pl.multiple_of(step * wide, wide), wide)
            rows = normed[...]
            value = jnp.dot(rows, value_full[:, place], preferred_element_type=jnp.float32)
            gate = jnp.dot(rows, gate_full[:, place], preferred_element_type=jnp.float32)
            glu = (value * jax.nn.sigmoid(gate)).astype(jnp.bfloat16)
            padded[pl.ds(rim, length), place] = glu.astype(jnp.float32)

        pl.when(me < devices - 1)(lambda: halo().start())

    def conv_stage():
        pl.when(me > 0)(lambda: halo().wait_recv())
        taps = conv_kernel.shape[0]

        @pl.loop(0, conv.shape[1] // 128)
        def _(step):
            place = pl.ds(pl.multiple_of(step * 128, 128), 128)
            total = jnp.zeros((length, 128), jnp.float32)
            for tap in range(taps):
                rows = padded[pl.ds(rim - taps + 1 + tap, length), place]
                total = total + conv_kernel[pl.ds(tap, 1), place] * rows
            conv[:, place] = total

        some = min(64, length)

        @pl.loop(0, length // some)
        def _(step):
            place = pl.ds(pl.multiple_of(step * some, some), some)
            block = conv[place, :]
            centred = block - jnp.mean(block, axis=-1, keepdims=True)
            var = jnp.mean(centred * centred, axis=-1, keepdims=True)
            scaled = centred * lax.rsqrt(var + LAYER_EPSILON) * chan_gain[...]
            act[place, :] = (scaled * jax.nn.sigmoid(scaled)).astype(jnp.bfloat16)

    def out_stage():
        wait_weight(2)
        wide = min(256, out_full.shape[1])

        @pl.loop(0, out_full.shape[1] // wide)
        def _(step):
            place = pl.ds(pl.multiple_of(step * wide, wide), wide)
            projected[:, place] = jnp.dot(
                act[...], out_full[:, place], preferred_element_type=jnp.float32
            )

        some = min(64, length)

        @pl.loop(0, length // some)
        def _(step):
            place = pl.ds(pl.multiple_of(step * some, some), some)
            mixed[place, :] = rms_scale(projected[place, :], mix_gain[...]).astype(jnp.bfloat16)

    own_rows.wait()
    for copy in a_copies:
        copy.wait_recv()
    rows_on(0)
    pass_on(1, 0)
    pass_on(2, 0)
    own_pair().start()
    for k in range(3):
        own_leg(k).start()

    take(0, 0)
    for s in range(steps):
        rows_in(s)
        if s + 1 < steps:
            rows_on(s + 1)
        rows_share(s)
        if s == min(1, steps - 1):
            take(1, 0)
            take(2, 0)
            if steps > 1:
                for k in range(3):
                    pass_on(k, 1)
            for k in range(3):
                relay(k, 0)
    own_pair().wait_recv()
    for s in range(steps):
        for d in range(2):
            pl.when(comes(d, s))(lambda d=d: row_pair(d, s).wait_recv())
    for copy in loads:
        copy.wait()

    total = groups_tp * chunk
    tile = min(256, units)
    tiles = units // tile

    @pl.loop(0, local_experts * tiles)
    def _(step):
        expert, unit = step // tiles, step % tiles
        place = pl.ds(pl.multiple_of(unit * tile, tile), tile)
        rows = rows_all[...].reshape(total, width)
        gate = jnp.dot(rows, gate_vmem[expert, :, place], preferred_element_type=jnp.float32)
        up = jnp.dot(rows, up_vmem[expert, :, place], preferred_element_type=jnp.float32)
        gate = jnp.minimum(gate, CLAMP_LIMIT)
        up = jnp.clip(up, -CLAMP_LIMIT, CLAMP_LIMIT)
        act = (up + 1.0) * gate * jax.nn.sigmoid(SWISH_ALPHA * gate)
        slot = lax.rem(lax.broadcasted_iota(jnp.int32, act.shape, 0), slots)
        mine = (slot >= expert * capacity) & (slot < (expert + 1) * capacity)
        hidden[:, pl.ds(pl.multiple_of(step * tile, tile), tile)] = jnp.where(
            mine, act, 0.0
        ).astype(jnp.bfloat16)

    for k in range(3):
        if steps > 1:
            take(k, 1)
        if steps > 2:
            pass_on(k, 2)
    for k in range(3):
        share(k, 0)

    down_tile = min(256, width)

    @pl.loop(0, width // down_tile)
    def _(step):
        place = pl.ds(pl.multiple_of(step * down_tile, down_tile), down_tile)
        weight = down_vmem[:, :, place].reshape(local_experts * units, down_tile)
        part = jnp.dot(hidden[...], weight, preferred_element_type=jnp.float32)
        partial[:, :, place] = part.astype(jnp.bfloat16).reshape(groups_tp, chunk, down_tile)

    def sum_pair(owner):
        return remote(
            partial.at[owner * 2 + 1 - core],
            pair_in.at[owner],
            send_p.at[owner],
            recv_p.at[owner],
            q,
            partner,
        )

    def sum_leg(d, owner):
        return remote(
            partial.at[owner * 2 + core],
            ring_in.at[d, owner],
            send_z.at[d, owner],
            recv_z.at[d, owner],
            q,
            beside(d),
        )

    def behind(d):
        return z > 0 if d == 0 else z < chips - 1

    def add_pair(owner):
        sum_pair(owner).wait_recv()
        place = partial.at[owner * 2 + core]
        both = place[...].astype(jnp.float32) + pair_in[owner].astype(jnp.float32)
        place[...] = both.astype(jnp.bfloat16)

    def add_line(d, owner):
        sum_leg(d, owner).wait_recv()
        place = partial.at[owner * 2 + core]
        both = place[...].astype(jnp.float32) + ring_in[d, owner].astype(jnp.float32)
        place[...] = both.astype(jnp.bfloat16)

    def send_sums(step):
        for d in range(2):
            far = z if d == 0 else chips - 1 - z
            owner = z + chips - 1 - step if d == 0 else z + step - chips + 1

            @pl.when(far <= step)
            def _(d=d, owner=owner):
                add_pair(owner)
                pl.when(behind(d))(lambda: add_line(d, owner))
                sum_leg(d, owner).start()

    order = []
    for j in range(chips):
        order += [o for o in (chips - 1 - j, j) if o not in order]
    for owner in order:
        sum_pair(owner).start()
    for s in range(2, steps):
        for k in range(3):
            take(k, s)
            if s + 1 < steps:
                pass_on(k, s + 1)
    send_sums(0)
    for k in range(3):
        if steps > 1:
            relay(k, 1)
    if steps > 1:
        send_sums(1)
    for k in range(3):
        if steps > 1:
            share(k, 1)
        for s in range(2, steps):
            relay(k, s)
    for s in range(2, steps):
        for k in range(3):
            share(k, s)
    if inside:
        glu_stage()
    for step in range(2, steps):
        send_sums(step)
    if inside:
        conv_stage()
    add_pair(z)
    if inside:
        out_stage()
    for d in range(2):
        pl.when(behind(d))(lambda d=d: add_line(d, z))
    summed = partial[t].astype(jnp.float32)
    back_out[...] = summed.astype(jnp.bfloat16)

    def back_leg(i):
        there = lax.rem(q + i, groups_ep)
        return remote(
            back_out.at[slot_rows(there), :],
            back_in.at[slot_rows(q), :],
            send_b.at[i],
            recv_b.at[i],
            there,
            t,
        )

    for i in range(1, groups_ep):
        back_leg(i).start()
    back_in[slot_rows(q), :] = back_out[slot_rows(q), :]
    for i in range(1, groups_ep):
        back_leg(i).wait_recv()
    returned[...] = back_in[...]

    for k in range(3):
        own_leg(k).wait_send()
        if not inside:
            wait_weight(k)
    if inside:
        pl.when(me < devices - 1)(lambda: halo().wait_send())
    own_pair().wait_send()
    for s in range(steps):
        for d in range(2):

            @pl.when(sends(d, s))
            def _(d=d, s=s):
                row_leg(d, s).wait_send()
                for k in range(3):
                    first_leg(k, d, s).wait_send()

            @pl.when(comes(d, s))
            def _(d=d, s=s):
                row_pair(d, s).wait_send()
                for k in range(3):
                    for j in direct + relayed:
                        second_leg(k, d, s, j).wait_send()
                    pair_leg(k, d, s).wait_send()
    for owner in range(chips):
        sum_pair(owner).wait_send()
        pl.when(z < owner)(lambda owner=owner: sum_leg(0, owner).wait_send())
        pl.when(z > owner)(lambda owner=owner: sum_leg(1, owner).wait_send())
    for i in range(1, groups_ep):
        a_copies[i - 1].wait_send()
        back_leg(i).wait_send()


def exchange(
    mixer_in,
    pre_gain,
    conv_kernel,
    chan_gain,
    mix_gain,
    outgoing,
    glu_value,
    glu_gate,
    out_weight,
    gate_proj,
    up_proj,
    down_proj,
    capacity,
):
    groups_ep, groups_tp = lax.axis_size("ep"), lax.axis_size("tp")
    chips = groups_tp // 2
    chunk, width = outgoing.shape
    units = gate_proj.shape[2] * gate_proj.shape[0]
    half = jnp.bfloat16

    def gathered(shard):
        rows, cols = shard.shape
        if cols % 128:
            return jax.ShapeDtypeStruct((groups_tp, rows, cols), half)
        return jax.ShapeDtypeStruct((rows, groups_tp * cols), half)

    own = (glu_value, glu_gate, out_weight)
    dma = pltpu.SemaphoreType.DMA
    inside = glu_value.shape[1] % 128 == 0 and out_weight.shape[1] % 128 == 0
    full_shapes = [gathered(shard) for shard in own]
    back_shape = jax.ShapeDtypeStruct((chunk, width), half)
    length, channels = mixer_in.shape[0], conv_kernel.shape[1]
    rim = -(-(conv_kernel.shape[0] - 1) // 8) * 8
    anywhere, vmem = pl.BlockSpec(memory_space=pl.ANY), pl.BlockSpec(memory_space=pltpu.VMEM)
    own_scratch = []
    if inside:
        own_scratch = [pltpu.VMEM(shape.shape, half) for shape in full_shapes] + [
            pltpu.VMEM(mixer_in.shape, half),
            pltpu.VMEM((rim + length, channels), jnp.float32),
            pltpu.VMEM((length, channels), jnp.float32),
            pltpu.VMEM((length, channels), half),
            pltpu.VMEM(mixer_in.shape, jnp.float32),
        ]
        mixer_specs = [vmem] * 5
    else:
        mixer_specs = [anywhere] * 5
    outs = pl.pallas_call(
        functools.partial(exchange_kernel, groups_ep, groups_tp, capacity, inside),
        out_shape=[jax.ShapeDtypeStruct(mixer_in.shape, half), back_shape]
        if inside
        else full_shapes + [back_shape],
        in_specs=[vmem] + mixer_specs + [anywhere] * 6,
        out_specs=[vmem] * 2 if inside else [anywhere] * 3 + [vmem],
        scratch_shapes=own_scratch
        + [
            pltpu.VMEM((groups_tp, chunk, width), half),
            pltpu.VMEM((groups_tp * chunk, units), half),
            pltpu.VMEM((groups_tp, chunk, width), half),
            pltpu.VMEM((chips, chunk, width), half),
            pltpu.VMEM((2, chips, chunk, width), half),
            pltpu.VMEM((chunk, width), half),
            pltpu.VMEM((chunk, width), half),
            pltpu.VMEM(gate_proj.shape, half),
            pltpu.VMEM(up_proj.shape, half),
            pltpu.VMEM(down_proj.shape, half),
            dma((3,)),
            dma((3,)),
            dma,
            dma,
            dma,
            dma((groups_ep,)),
            dma((groups_ep,)),
            dma((2, chips)),
            dma((2, chips)),
            dma((2, chips)),
            dma((2, chips)),
            dma((3, 2, chips)),
            dma((3, 2, chips)),
            dma((3, 2, chips, groups_ep)),
            dma((3, 2, chips, groups_ep)),
            dma((3, 2, chips)),
            dma((3, 2, chips)),
            dma((chips,)),
            dma((chips,)),
            dma((2, chips)),
            dma((2, chips)),
            dma((groups_ep,)),
            dma((groups_ep,)),
        ],
        compiler_params=pltpu.CompilerParams(
            collective_id=0, has_side_effects=True, vmem_limit_bytes=60 * 1024 * 1024
        ),
    )(
        outgoing,
        mixer_in,
        pre_gain[None],
        conv_kernel,
        chan_gain[None],
        mix_gain[None],
        *own,
        gate_proj,
        up_proj,
        down_proj,
    )
    if inside:
        return None, outs[0], outs[1]
    full = [
        value if value.ndim == 2 else value.transpose(1, 0, 2).reshape(value.shape[1], -1)
        for value in outs[:3]
    ]
    return full, None, outs[3]


def flipped(index, bit):
    return index + bit - 2 * bit * lax.rem(index // bit, 2)


def across(index, distance):
    bit = 1
    while bit <= distance:
        if distance & bit:
            index = flipped(index, bit)
        bit *= 2
    return index


def fused_kernel(
    groups_ep,
    groups_tp,
    capacity,
    expert_in_hbm,
    ffn_gain_hbm,
    routes_hbm,
    shares_hbm,
    expert_gain_hbm,
    mixer_hbm,
    pre_gain_hbm,
    conv_kernel_hbm,
    chan_gain_hbm,
    value_own,
    gate_own,
    out_own,
    gate_hbm,
    up_hbm,
    down_hbm,
    projected_hbm,
    routed_hbm,
    expert_in,
    ffn_gain,
    routes,
    shares,
    expert_gain,
    pre_gain,
    conv_kernel,
    chan_gain,
    value_full,
    gate_full,
    out_full,
    mixer_in,
    normed,
    padded,
    tail_out,
    tail_in,
    conv,
    act,
    projected,
    routed,
    info,
    rows_all,
    picked,
    hidden,
    partial,
    pair_in,
    ring_in,
    back_in,
    gate_vmem,
    up_vmem,
    down_vmem,
    load_sem,
    stage_sem,
    out_sem,
    send_h,
    recv_h,
    send_rows,
    recv_rz,
    recv_rx,
    recv_rd,
    recv_rp,
    send_w1,
    recv_w1,
    send_w2,
    recv_w2,
    send_wp,
    recv_wp,
    send_p,
    recv_p,
    send_z,
    recv_z,
    send_b,
    recv_b,
):
    q = lax.axis_index("ep")
    t = lax.axis_index("tp")
    chips = groups_tp // 2
    z, core = t // 2, t % 2
    partner = z * 2 + 1 - core
    tokens, width = expert_in.shape
    slots = partial.shape[2]
    local_experts, _, units = gate_vmem.shape
    top_count = routes.shape[0]
    half_tokens = tokens // 2

    def remote(src, dst, send, recv, ep, tp):
        return pltpu.make_async_remote_copy(
            src_ref=src,
            dst_ref=dst,
            send_sem=send,
            recv_sem=recv,
            device_id=(ep, tp),
            device_id_type=pl.DeviceIdType.MESH,
        )

    barrier = pltpu.get_barrier_semaphore()
    others = [(lax.rem(q + i, groups_ep), t) for i in range(1, groups_ep)]
    others += [(q, lax.rem(z + i, chips) * 2 + core) for i in range(1, chips)]
    others += [(q, partner)]
    me, devices = q * groups_tp + t, groups_ep * groups_tp
    after, ahead = lax.rem(me + 1, devices), lax.rem(me + devices - 1, devices)
    others += [(n // groups_tp, lax.rem(n, groups_tp)) for n in (after, ahead)]
    for ep, tp in others:
        pl.semaphore_signal(
            barrier, inc=1, device_id=(ep, tp), device_id_type=pl.DeviceIdType.MESH
        )

    weights = ((value_own, value_full), (gate_own, gate_full), (out_own, out_full))
    stored = [
        pltpu.make_async_copy(
            own, columns(full, t, own.shape[1], pl.ds(0, own.shape[0])), stage_sem.at[k]
        )
        for k, (own, full) in enumerate(weights)
    ]
    def loaded(number, src, dst):
        return pltpu.make_async_copy(src, dst, load_sem.at[number])

    row_loads = [
        loaded(i, src, dst)
        for i, (src, dst) in enumerate(
            (
                (expert_in_hbm, expert_in),
                (ffn_gain_hbm, ffn_gain),
                (routes_hbm, routes),
                (shares_hbm, shares),
            )
        )
    ]
    mixer_loads = [
        loaded(4 + i, src, dst)
        for i, (src, dst) in enumerate(
            (
                (mixer_hbm, mixer_in),
                (pre_gain_hbm, pre_gain),
                (conv_kernel_hbm, conv_kernel),
                (chan_gain_hbm, chan_gain),
                (expert_gain_hbm, expert_gain),
            )
        )
    ]
    loads = [
        loaded(9 + i, src, dst)
        for i, (src, dst) in enumerate(
            ((gate_hbm, gate_vmem), (up_hbm, up_vmem), (down_hbm, down_vmem))
        )
    ]
    for copy in row_loads + mixer_loads + stored + loads:
        copy.start()
    for copy in row_loads:
        copy.wait()

    rows_all[0, t, :, pl.ds(0, width)] = rms_scale(expert_in[...], ffn_gain[...]).astype(
        jnp.bfloat16
    )
    lanes = 128
    expert_ids = lax.broadcasted_iota(jnp.int32, (lanes, tokens), 0)
    chosen = [routes[pl.ds(k, 1), :] == expert_ids for k in range(top_count)]
    named = sum(c.astype(jnp.float32) for c in chosen)
    earlier = lax.broadcasted_iota(jnp.int32, (tokens, tokens), 0) < lax.broadcasted_iota(
        jnp.int32, (tokens, tokens), 1
    )
    rank = jnp.dot(
        named.astype(jnp.bfloat16),
        earlier.astype(jnp.float32).astype(jnp.bfloat16),
        preferred_element_type=jnp.float32,
    )
    group_ids = expert_ids // local_experts
    base = group_ids * slots + (expert_ids - group_ids * local_experts) * capacity
    spot = rank + base.astype(jnp.float32)
    facts = jnp.zeros((lanes, tokens), jnp.float32)
    for k in range(top_count):
        slot = jnp.sum(jnp.where(chosen[k], spot, 0.0), axis=0, keepdims=True)
        facts = facts + jnp.where(expert_ids == k, slot, 0.0)
        facts = facts + jnp.where(expert_ids == top_count + k, shares[pl.ds(k, 1), :], 0.0)
    info[...] = facts.T
    rows_all[0, t, :, pl.ds(width, lanes)] = info[...].astype(jnp.bfloat16)

    pl.semaphore_wait(barrier, len(others))

    def took(ref, sem):
        remote(ref, ref, sem, sem, q, partner).wait_send()

    def row_z(m):
        place = rows_all.at[0, t]
        return remote(place, place, send_rows.at[0], recv_rz.at[m], q, across(z, m) * 2 + core)

    def row_beside(b, m):
        owner = across(z, m) * 2 + core
        return remote(
            rows_all.at[0, owner],
            rows_all.at[1 + b, owner],
            send_rows.at[1],
            recv_rx.at[m],
            flipped(q, 1 + b),
            t,
        )

    def row_far(b, m):
        owner = across(z, m) * 2 + core
        some = pl.ds(b * half_tokens, half_tokens)
        return remote(
            rows_all.at[2 - b, owner, some, :],
            rows_all.at[3, owner, some, :],
            send_rows.at[2],
            recv_rd.at[m],
            flipped(q, 1 + b),
            t,
        )

    def row_pair(j, m):
        place = rows_all.at[j, across(z, m) * 2 + core]
        return remote(place, place, send_rows.at[3], recv_rp.at[j], q, partner)

    def rows_start():
        for m in range(1, chips):
            row_z(m).start()

    def rows_here(m):
        if m:
            took(rows_all.at[0, t], recv_rz.at[m])
        for b in range(2):
            row_beside(b, m).start()
        row_pair(0, m).start()

    def rows_beside(m):
        took(rows_all.at[0, pl.ds(0, 2)], recv_rx.at[m])
        for b in range(2):
            row_far(1 - b, m).start()
            row_pair(1 + b, m).start()

    def rows_far(m):
        took(rows_all.at[0, t], recv_rd.at[m])
        row_pair(3, m).start()

    def rows_left():
        took(rows_all.at[0, pl.ds(0, chips - 1)], send_rows.at[0])
        took(rows_all.at[0, pl.ds(0, 2 * chips)], send_rows.at[1])
        took(rows_all.at[0, pl.ds(0, chips)], send_rows.at[2])
        took(rows_all.at[:, pl.ds(0, chips)], send_rows.at[3])

    def sends(d, s):
        return (z >= s) & (z < chips - 1) if d == 0 else (z + s < chips) & (z > 0)

    def comes(d, s):
        return z >= 1 + s if d == 0 else z + 1 + s < chips

    def sent(d, s):
        return (z - s if d == 0 else z + s) * 2 + core

    def came(d, s):
        return sent(d, s + 1)

    def beside(d):
        return t + 2 if d == 0 else t - 2

    def quarter(k, index, cut=0):
        own = weights[k][0]
        part = own.shape[0] // groups_ep
        if cut == 0:
            return pl.ds(pl.multiple_of(index * part, part), part)
        half = part // 2
        return pl.ds(pl.multiple_of(index * part + (cut - 1) * half, half), half)

    bundles = ((0, 1), (2,))

    side = lax.rem(lax.rem(q, 2) + q // 2, 2)

    def piece_rows(g, k):
        if g == 0:
            return quarter(k, q)
        half = weights[k][0].shape[0] // 2
        return pl.ds(pl.multiple_of(side * half, half), half)

    def first_leg(g, k, d, s):
        own, full = weights[k]
        rows = piece_rows(g, k)
        place = columns(full, sent(d, s), own.shape[1], rows)
        src = own.at[rows, :] if s == 0 else place
        return remote(src, place, send_w1.at[d, s], recv_w1.at[g, d, s], q, beside(d))

    flip_low, flip_high = flipped(q, 1), flipped(q, 2)
    direct, relayed = (1, 2), (0, 3)

    def second_leg(g, k, d, s, j):
        own, full = weights[k]
        piece = (flip_high, q, q, flip_low)[j]
        there = (flip_low, flip_low, flip_high, flip_high)[j]
        cut = (2, 0, 0, 1)[j]
        if g:
            piece, cut = side * 2 + j - 1, 0
        place = columns(full, came(d, s), own.shape[1], quarter(k, piece, cut))
        kind = 0 if j in direct else 1
        return remote(
            place, place, send_w2.at[d, s], recv_w2.at[g, kind, d, s], there, t
        )

    def own_leg(g, k):
        own, full = weights[k]
        place = columns(full, t, own.shape[1], pl.ds(0, own.shape[0]))
        last = chips - 1
        return remote(own, place, send_wp.at[0, last], recv_wp.at[g, 0, last], q, partner)

    def pair_leg(g, k, d, s):
        own, full = weights[k]
        place = columns(full, came(d, s), own.shape[1], pl.ds(0, own.shape[0]))
        return remote(place, place, send_wp.at[d, s], recv_wp.at[g, d, s], q, partner)

    share_rows, share_wide = value_own.shape

    def took_shares(quarters, sem):
        tall = max(r for r in range(1, groups_ep + 1) if quarters % r == 0)
        rows = pl.ds(0, share_rows // groups_ep * tall)
        took(value_full.at[rows, pl.ds(0, quarters // tall * share_wide)], sem)

    def passes(g, s):
        for d in range(2):

            @pl.when(sends(d, s))
            def _(d=d):
                for k in bundles[g]:
                    first_leg(g, k, d, s).start()

    def own_legs(g):
        for k in bundles[g]:
            own_leg(g, k).start()

    def takes(g, s):
        for d in range(2):

            @pl.when(comes(d, s))
            def _(d=d):
                took_shares(2, recv_w1.at[g, d, s])
                if s + 1 < steps:

                    @pl.when(sends(d, s + 1))
                    def _():
                        for k in bundles[g]:
                            first_leg(g, k, d, s + 1).start()

                for j in direct:
                    for k in bundles[g]:
                        second_leg(g, k, d, s, j).start()

    def relays(g, s):
        for d in range(2):

            @pl.when(comes(d, s))
            def _(d=d):
                took_shares(2 * len(bundles[g]), recv_w2.at[g, 0, d, s])
                for j in relayed:
                    for k in bundles[g]:
                        second_leg(g, k, d, s, j).start()

    def shares_on(g, s):
        for d in range(2):

            @pl.when(comes(d, s))
            def _(d=d):
                took_shares(2, recv_w2.at[g, 1 - g, d, s])
                for k in bundles[g]:
                    pair_leg(g, k, d, s).start()

    def wait_plane(g, m):
        if m == 0:
            for k in bundles[g]:
                stored[k].wait()
            took_shares(groups_ep * len(bundles[g]), recv_wp.at[g, 0, chips - 1])
            return
        plane = across(z, m)
        d = (plane > z).astype(jnp.int32)
        s = (plane - z) * (2 * d - 1) - 1
        took_shares(groups_ep * len(bundles[g]), recv_wp.at[g, d, s])

    def shares_left():
        took_shares(3 * groups_ep, send_wp.at[0, chips - 1])
        for s in range(steps):
            for d in range(2):

                @pl.when(sends(d, s))
                def _(d=d, s=s):
                    took_shares(4, send_w1.at[d, s])

                @pl.when(comes(d, s))
                def _(d=d, s=s):
                    took_shares(8, send_w2.at[d, s])
                    took_shares(3 * groups_ep, send_wp.at[d, s])

    length = mixer_in.shape[0]
    rim = padded.shape[1] - length
    lane_blocks = padded.shape[0]

    def norm_stage():
        for copy in mixer_loads:
            copy.wait()
        some = min(64, length)

        @pl.loop(0, length // some)
        def _(step):
            place = pl.ds(pl.multiple_of(step * some, some), some)
            normed[place, :] = rms_scale(mixer_in[place, :], pre_gain[...]).astype(jnp.bfloat16)

    def glu_stage(m):
        wait_plane(0, m)
        wide = 2 * value_own.shape[1]
        place = pl.ds(pl.multiple_of(across(z, m) * wide, wide), wide)
        rows = normed[...]
        value = jnp.dot(rows, value_full[:, place], preferred_element_type=jnp.float32)
        gate = jnp.dot(rows, gate_full[:, place], preferred_element_type=jnp.float32)
        glu = (value * jax.nn.sigmoid(gate)).astype(jnp.bfloat16)
        for i in range(wide // lanes):
            padded[across(z, m) * (wide // lanes) + i, pl.ds(rim, length), :] = glu[
                :, i * lanes : (i + 1) * lanes
            ].astype(jnp.float32)
        tail_out[:, place] = glu[length - rim :, :]

    def halo():
        return remote(
            tail_out, tail_in, send_h, recv_h, after // groups_tp, lax.rem(after, groups_tp)
        )

    def halo_start():
        pl.when(me < devices - 1)(lambda: halo().start())

    def conv_start():
        @pl.when(me > 0)
        def _():
            halo().wait_recv()
            for i in range(lane_blocks):
                padded[i, pl.ds(0, rim), :] = tail_in[:, i * lanes : (i + 1) * lanes].astype(
                    jnp.float32
                )

        @pl.when(me == 0)
        def _():
            padded[:, pl.ds(0, rim), :] = jnp.zeros((lane_blocks, rim, lanes), jnp.float32)

    def conv_stage(part):
        taps = conv_kernel.shape[0]
        here = lane_blocks // chips

        @pl.loop(part * here, (part + 1) * here)
        def _(step):
            place = pl.ds(pl.multiple_of(step * lanes, lanes), lanes)
            total = jnp.zeros((length, lanes), jnp.float32)
            for tap in range(taps):
                rows = padded[step, pl.ds(rim - taps + 1 + tap, length), :]
                total = total + conv_kernel[pl.ds(tap, 1), place] * rows
            conv[:, place] = total

    def act_stage():
        some = min(64, length)

        @pl.loop(0, length // some)
        def _(step):
            place = pl.ds(pl.multiple_of(step * some, some), some)
            block = conv[place, :]
            centred = block - jnp.mean(block, axis=-1, keepdims=True)
            var = jnp.mean(centred * centred, axis=-1, keepdims=True)
            scaled = centred * lax.rsqrt(var + LAYER_EPSILON) * chan_gain[...]
            act[place, :] = (scaled * jax.nn.sigmoid(scaled)).astype(jnp.bfloat16)

    def out_stage(m):
        wait_plane(1, m)
        wide = out_own.shape[1]
        start = across(z, m) * 2 * wide
        for i in range(2):
            place = pl.ds(pl.multiple_of(start + i * wide, wide), wide)
            projected[:, place] = jnp.dot(
                act[...], out_full[:, place], preferred_element_type=jnp.float32
            )
        projected_out(m).start()

    def projected_out(m):
        both = 2 * out_own.shape[1]
        place = pl.ds(pl.multiple_of(across(z, m) * both, both), both)
        return pltpu.make_async_copy(
            projected.at[:, place], projected_hbm.at[:, place], out_sem.at[m]
        )

    total = groups_tp * slots
    tile = min(512, units)
    tiles = units // tile
    down_tile = min(512, width)

    def pick_stage(j):
        took(rows_all.at[0, pl.ds(0, chips)], recv_rp.at[j])
        if j == 0:
            for copy in loads:
                copy.wait()
        every = groups_tp * tokens
        block = rows_all[j].reshape(every, width + lanes)
        facts = block[:, width:].astype(jnp.float32)
        slot_ids = lax.broadcasted_iota(jnp.int32, (every, total), 1).astype(jnp.float32)
        owner = lax.broadcasted_iota(jnp.int32, (every, 1), 0) // tokens
        first = (owner * slots).astype(jnp.float32)
        low = (q * slots).astype(jnp.float32)
        pick = jnp.zeros((every, total), jnp.float32)
        for k in range(top_count):
            local = facts[:, k : k + 1] - low
            mine = (local >= 0.0) & (local < float(slots))
            target = jnp.where(mine, local + first, -1.0)
            pick = pick + (target == slot_ids).astype(jnp.float32)
        picked[...] = jnp.dot(
            pick.T.astype(jnp.bfloat16), block[:, :width], preferred_element_type=jnp.float32
        ).astype(jnp.bfloat16)

    def up_stage(j, expert):
        @pl.loop(0, tiles)
        def _(unit):
            step = expert * tiles + unit
            place = pl.ds(pl.multiple_of(unit * tile, tile), tile)
            rows = picked[...]
            gate = jnp.dot(rows, gate_vmem[expert, :, place], preferred_element_type=jnp.float32)
            up = jnp.dot(rows, up_vmem[expert, :, place], preferred_element_type=jnp.float32)
            gate = jnp.minimum(gate, CLAMP_LIMIT)
            up = jnp.clip(up, -CLAMP_LIMIT, CLAMP_LIMIT)
            unit_act = (up + 1.0) * gate * jax.nn.sigmoid(SWISH_ALPHA * gate)
            slot = lax.rem(lax.broadcasted_iota(jnp.int32, unit_act.shape, 0), slots)
            mine = (slot >= expert * capacity) & (slot < (expert + 1) * capacity)
            hidden[:, pl.ds(pl.multiple_of(step * tile, tile), tile)] = jnp.where(
                mine, unit_act, 0.0
            ).astype(jnp.bfloat16)

    def down_stage(j):
        @pl.loop(0, width // down_tile)
        def _(step):
            place = pl.ds(pl.multiple_of(step * down_tile, down_tile), down_tile)
            weight = down_vmem[:, :, place].reshape(local_experts * units, down_tile)
            part = jnp.dot(hidden[...], weight, preferred_element_type=jnp.float32)
            partial[j, :, :, place] = part.astype(jnp.bfloat16).reshape(
                groups_tp, slots, down_tile
            )

        for owner in owners:
            sum_pair(j, owner).start()

    owners = []
    for i in range(chips):
        owners += [o for o in (chips - 1 - i, i) if o not in owners]

    def sum_pair(j, owner):
        return remote(
            partial.at[j, owner * 2 + 1 - core],
            pair_in.at[j, owner],
            send_p.at[j],
            recv_p.at[j],
            q,
            partner,
        )

    def owner_of(d, step):
        return z + chips - 1 - step if d == 0 else z + step - chips + 1

    def sum_leg(j, d, step):
        owner = owner_of(d, step)
        return remote(
            partial.at[j, owner * 2 + core],
            ring_in.at[j, d, owner],
            send_z.at[d, step],
            recv_z.at[j, d, step],
            q,
            beside(d),
        )

    def behind(d):
        return z > 0 if d == 0 else z < chips - 1

    def add_to(j, owner, other):
        place = partial.at[j, owner * 2 + core]
        both = place[...].astype(jnp.float32) + other[...].astype(jnp.float32)
        place[...] = both.astype(jnp.bfloat16)

    def add_line(j, d, owner, step):
        took(partial.at[j, t], recv_z.at[j, d, step])
        add_to(j, owner, ring_in.at[j, d, owner])

    def send_sums(j, step):
        if step == 0:
            took(pair_in.at[j], recv_p.at[j])
        for d in range(2):
            far = z if d == 0 else chips - 1 - z

            @pl.when(far <= step)
            def _(d=d):
                owner = owner_of(d, step)
                add_to(j, owner, pair_in.at[j, owner])
                if step:
                    pl.when(behind(d))(lambda: add_line(j, d, owner, step - 1))
                sum_leg(j, d, step).start()

    def back_leg(j):
        return remote(
            partial.at[j, t], back_in.at[j - 1], send_b, recv_b, across(q, j), t
        )

    def own_sums(j):
        add_to(j, z, pair_in.at[j, z])
        for d in range(2):
            pl.when(behind(d))(lambda d=d: add_line(j, d, z, chips - 2))
        if j:
            back_leg(j).start()

    def sums_left():
        for j in range(groups_ep):
            took(pair_in.at[j], send_p.at[j])
        for d in range(2):
            far = z if d == 0 else chips - 1 - z
            for step in range(steps):
                pl.when(far <= step)(
                    lambda d=d, step=step: took(partial.at[:, 0], send_z.at[d, step])
                )
        took(back_in, send_b)

    def routed_stage():
        took(back_in, recv_b)
        facts = info[...]
        total_rows = jnp.zeros((tokens, width), jnp.float32)
        slot_ids = lax.broadcasted_iota(jnp.int32, (tokens, slots), 1)
        for j in range(groups_ep):
            block = partial[0, t] if j == 0 else back_in[j - 1]
            low = across(q, j) * slots
            shared = jnp.zeros((tokens, slots), jnp.float32)
            for k in range(top_count):
                here = facts[:, k : k + 1] == (slot_ids + low).astype(jnp.float32)
                share_of = facts[:, top_count + k : top_count + k + 1]
                shared = shared + jnp.where(here, share_of, 0.0)
            high = shared.astype(jnp.bfloat16)
            rest = (shared - high.astype(jnp.float32)).astype(jnp.bfloat16)
            for term in (high, rest):
                total_rows = total_rows + jnp.dot(
                    term, block, preferred_element_type=jnp.float32
                )
        routed[...] = rms_scale(total_rows, expert_gain[...]).astype(jnp.bfloat16)
        routed_out().start()

    def routed_out():
        return pltpu.make_async_copy(routed, routed_hbm, out_sem.at[chips])

    steps = chips - 1
    rows_start()
    rows_here(0)
    rows_beside(0)
    rows_here(1)
    rows_far(0)
    passes(0, 0)
    rows_beside(1)
    rows_here(2)
    passes(1, 0)
    rows_here(3)
    norm_stage()
    pick_stage(0)
    own_legs(1)
    rows_beside(2)
    up_stage(0, 0)
    up_stage(0, 1)
    rows_beside(3)
    takes(0, 0)
    down_stage(0)
    pick_stage(1)
    rows_far(1)
    up_stage(1, 0)
    send_sums(0, 0)
    rows_far(2)
    up_stage(1, 1)
    down_stage(1)
    send_sums(0, 1)
    takes(0, 1)
    pick_stage(2)
    send_sums(1, 0)
    takes(1, 0)
    up_stage(2, 0)
    up_stage(2, 1)
    down_stage(2)
    send_sums(2, 0)
    rows_far(3)
    send_sums(0, 2)
    send_sums(2, 1)
    relays(0, 0)
    pick_stage(3)
    up_stage(3, 0)
    up_stage(3, 1)
    down_stage(3)
    send_sums(2, 2)
    takes(0, 2)
    send_sums(3, 0)
    send_sums(1, 1)
    send_sums(3, 1)
    relays(0, 1)
    own_legs(0)
    relays(0, 2)
    shares_on(1, 0)
    takes(1, 1)
    shares_on(0, 0)
    send_sums(1, 2)
    glu_stage(0)
    own_sums(0)
    shares_on(0, 1)
    send_sums(3, 2)
    glu_stage(1)
    shares_on(0, 2)
    takes(1, 2)
    glu_stage(3)
    own_sums(2)
    glu_stage(2)
    halo_start()
    shares_on(1, 1)
    own_sums(1)
    own_sums(3)
    conv_start()
    conv_stage(2)
    shares_on(1, 2)
    conv_stage(0)
    conv_stage(3)
    conv_stage(1)
    act_stage()
    out_stage(1)
    out_stage(2)
    out_stage(3)
    out_stage(0)
    routed_stage()

    rows_left()
    shares_left()
    pl.when(me < devices - 1)(lambda: halo().wait_send())
    sums_left()
    for m in range(chips):
        projected_out(m).wait()
    routed_out().wait()


def finish_kernel(
    projected_hbm,
    routed_hbm,
    gain_hbm,
    mixed_hbm,
    routed_out_hbm,
    projected,
    routed,
    gain,
    mixed,
    in_sem,
    out_sem,
):
    length = projected.shape[0]
    parts = mixed_hbm.shape[0] // min(64, mixed_hbm.shape[0])
    some = length // parts

    def row_copy(i, src, dst, sem):
        rows = pl.ds(i * some, some)
        return pltpu.make_async_copy(src.at[rows, :], dst.at[rows, :], sem.at[i])

    gain_in = pltpu.make_async_copy(gain_hbm, gain, in_sem.at[parts])
    routed_in = pltpu.make_async_copy(routed_hbm, routed, in_sem.at[parts + 1])
    routed_back = pltpu.make_async_copy(routed, routed_out_hbm, out_sem.at[parts])
    gain_in.start()
    for i in range(parts):
        row_copy(i, projected_hbm, projected, in_sem).start()
    routed_in.start()
    gain_in.wait()
    for i in range(parts):
        row_copy(i, projected_hbm, projected, in_sem).wait()
        rows = pl.ds(i * some, some)
        mixed[rows, :] = rms_scale(projected[rows, :], gain[...]).astype(jnp.bfloat16)
        row_copy(i, mixed, mixed_hbm, out_sem).start()
    routed_in.wait()
    routed_back.start()
    for i in range(parts):
        row_copy(i, mixed, mixed_hbm, out_sem).wait()
    routed_back.wait()


def fused(
    mixer_in,
    pre_gain,
    glu_value,
    glu_gate,
    conv_kernel,
    chan_gain,
    out_weight,
    mix_gain,
    expert_in,
    ffn_gain,
    routing,
    route_weight,
    gate_proj,
    up_proj,
    down_proj,
    expert_gain,
    capacity,
    slots,
):
    groups_ep, groups_tp = lax.axis_size("ep"), lax.axis_size("tp")
    chips = groups_tp // 2
    tokens, width = expert_in.shape
    length, channels = mixer_in.shape[0], conv_kernel.shape[1]
    units = gate_proj.shape[2] * gate_proj.shape[0]
    half, full = jnp.bfloat16, jnp.float32
    dma = pltpu.SemaphoreType.DMA
    rim = -(-(conv_kernel.shape[0] - 1) // 8) * 8
    anywhere = pl.BlockSpec(memory_space=pl.ANY)

    def gathered(shard):
        return pltpu.VMEM((shard.shape[0], groups_tp * shard.shape[1]), half)

    projected, routed = pl.pallas_call(
        functools.partial(fused_kernel, groups_ep, groups_tp, capacity),
        out_shape=[
            jax.ShapeDtypeStruct(mixer_in.shape, full),
            jax.ShapeDtypeStruct(expert_in.shape, half),
        ],
        in_specs=[anywhere] * 15,
        out_specs=[anywhere] * 2,
        scratch_shapes=[
            pltpu.VMEM(expert_in.shape, half),
            pltpu.VMEM((1, width), full),
            pltpu.VMEM(routing.shape[::-1], routing.dtype),
            pltpu.VMEM(route_weight.shape[::-1], full),
            pltpu.VMEM((1, width), full),
            pltpu.VMEM((1, width), full),
            pltpu.VMEM(conv_kernel.shape, full),
            pltpu.VMEM((1, channels), full),
            gathered(glu_value),
            gathered(glu_gate),
            gathered(out_weight),
            pltpu.VMEM(mixer_in.shape, half),
            pltpu.VMEM(mixer_in.shape, half),
            pltpu.VMEM((channels // 128, rim + length, 128), full),
            pltpu.VMEM((rim, channels), half),
            pltpu.VMEM((rim, channels), half),
            pltpu.VMEM((length, channels), full),
            pltpu.VMEM((length, channels), half),
            pltpu.VMEM(mixer_in.shape, full),
            pltpu.VMEM(expert_in.shape, half),
            pltpu.VMEM((tokens, 128), full),
            pltpu.VMEM((groups_ep, groups_tp, tokens, width + 128), half),
            pltpu.VMEM((groups_tp * slots, width), half),
            pltpu.VMEM((groups_tp * slots, units), half),
            pltpu.VMEM((groups_ep, groups_tp, slots, width), half),
            pltpu.VMEM((groups_ep, chips, slots, width), half),
            pltpu.VMEM((groups_ep, 2, chips, slots, width), half),
            pltpu.VMEM((groups_ep - 1, slots, width), half),
            pltpu.VMEM(gate_proj.shape, half),
            pltpu.VMEM(up_proj.shape, half),
            pltpu.VMEM(down_proj.shape, half),
            dma((12,)),
            dma((3,)),
            dma((chips + 1,)),
            dma,
            dma,
            dma((4,)),
            dma((chips,)),
            dma((chips,)),
            dma((chips,)),
            dma((groups_ep,)),
            dma((2, chips - 1)),
            dma((2, 2, chips - 1)),
            dma((2, chips - 1)),
            dma((2, 2, 2, chips - 1)),
            dma((2, chips)),
            dma((2, 2, chips)),
            dma((groups_ep,)),
            dma((groups_ep,)),
            dma((2, chips - 1)),
            dma((groups_ep, 2, chips - 1)),
            dma,
            dma,
        ],
        compiler_params=pltpu.CompilerParams(
            collective_id=0, has_side_effects=True, vmem_limit_bytes=60 * 1024 * 1024
        ),
    )(
        expert_in,
        ffn_gain[None],
        routing.T,
        route_weight.T,
        expert_gain[None],
        mixer_in,
        pre_gain[None],
        conv_kernel,
        chan_gain[None],
        glu_value,
        glu_gate,
        out_weight,
        gate_proj,
        up_proj,
        down_proj,
    )
    parts = length // min(64, length)
    return pl.pallas_call(
        finish_kernel,
        out_shape=[
            jax.ShapeDtypeStruct(mixer_in.shape, half),
            jax.ShapeDtypeStruct(expert_in.shape, half),
        ],
        in_specs=[anywhere] * 3,
        out_specs=[anywhere] * 2,
        scratch_shapes=[
            pltpu.VMEM(mixer_in.shape, full),
            pltpu.VMEM(expert_in.shape, half),
            pltpu.VMEM((1, width), full),
            pltpu.VMEM(mixer_in.shape, half),
            dma((parts + 2,)),
            dma((parts + 1,)),
        ],
        compiler_params=pltpu.CompilerParams(vmem_limit_bytes=60 * 1024 * 1024),
    )(projected, routed, mix_gain[None])


def mixer(full, mixer_in, pre_gain, conv_kernel, chan_gain, mix_gain):
    value_full, gate_full, out_full = full
    normed_mix = rms_scale(mixer_in, pre_gain).astype(jnp.bfloat16)
    value_pre = jnp.dot(normed_mix, value_full, preferred_element_type=jnp.float32)
    gate_mix = jnp.dot(normed_mix, gate_full, preferred_element_type=jnp.float32)
    gated_rows = (value_pre * jax.nn.sigmoid(gate_mix)).astype(jnp.bfloat16)
    kernel_width = conv_kernel.shape[0]
    length = gated_rows.shape[0]
    rim_rows = passed_along(gated_rows[length - (kernel_width - 1) :], ("ep", "tp"), 1)
    padded = jnp.concatenate([rim_rows, gated_rows], axis=0).astype(jnp.float32)
    conv_sum = jnp.zeros((length, gated_rows.shape[1]), jnp.float32)
    for offset in range(kernel_width):
        conv_sum = conv_sum + conv_kernel[offset] * padded[offset : offset + length]
    row_mean = jnp.mean(conv_sum, axis=-1, keepdims=True)
    centred = conv_sum - row_mean
    row_var = jnp.mean(centred * centred, axis=-1, keepdims=True)
    activated = jax.nn.silu(centred * lax.rsqrt(row_var + LAYER_EPSILON) * chan_gain).astype(
        jnp.bfloat16
    )
    projected = jnp.dot(activated, out_full, preferred_element_type=jnp.float32)
    mixed = rms_scale(projected, mix_gain).astype(jnp.bfloat16)
    return mixed


def on_device(
    mixer_in,
    pre_gain,
    glu_value,
    glu_gate,
    conv_kernel,
    chan_gain,
    out_weight,
    mix_gain,
    expert_in,
    ffn_gain,
    routing,
    route_weight,
    gate_proj,
    up_proj,
    down_proj,
    expert_gain,
):
    groups_ep = lax.axis_size("ep")
    local_experts = gate_proj.shape[0]
    experts = local_experts * groups_ep
    token_rows, top_count = routing.shape
    capacity = max(2, 3 * token_rows * top_count // (2 * experts))
    slots = -(-local_experts * capacity // 8) * 8
    chips = lax.axis_size("tp") // 2
    lined_up = all(w.shape[1] % 128 == 0 for w in (glu_value, glu_gate, out_weight))
    two_way = groups_ep == 4 and chips > 1 and chips & (chips - 1) == 0
    if lined_up and two_way and groups_ep * slots <= 256:
        return tuple(
            fused(
                mixer_in,
                pre_gain,
                glu_value,
                glu_gate,
                conv_kernel,
                chan_gain,
                out_weight,
                mix_gain,
                expert_in,
                ffn_gain,
                routing,
                route_weight,
                gate_proj,
                up_proj,
                down_proj,
                expert_gain,
                capacity,
                slots,
            )
        )
    flat_route = routing.reshape(-1)
    onehot = (flat_route[:, None] == jnp.arange(experts, dtype=jnp.int32)[None, :]).astype(
        jnp.int32
    )
    before = jnp.cumsum(onehot, axis=0) - onehot
    rank_within = jnp.sum(before * onehot, axis=1)
    slot_index = (
        flat_route // local_experts * slots + flat_route % local_experts * capacity + rank_within
    ).reshape(token_rows, top_count)
    slot_ids = jnp.arange(groups_ep * slots, dtype=jnp.int32)
    chosen = slot_index[None, :, :] == slot_ids[:, None, None]
    pick_matrix = jnp.sum(chosen.astype(jnp.float32), axis=2).astype(jnp.bfloat16)
    normed_exp = rms_scale(expert_in, ffn_gain).astype(jnp.bfloat16)
    outgoing = jnp.dot(pick_matrix, normed_exp, preferred_element_type=jnp.float32).astype(
        jnp.bfloat16
    )
    full, mixed, returned = exchange(
        mixer_in,
        pre_gain,
        conv_kernel,
        chan_gain,
        mix_gain,
        outgoing,
        glu_value,
        glu_gate,
        out_weight,
        gate_proj,
        up_proj,
        down_proj,
        capacity,
    )
    if mixed is None:
        mixed = mixer(full, mixer_in, pre_gain, conv_kernel, chan_gain, mix_gain)
    combined = jnp.zeros((token_rows, returned.shape[1]), jnp.float32)
    for column in range(top_count):
        combined = combined + route_weight[:, column][:, None] * returned[
            slot_index[:, column]
        ].astype(jnp.float32)
    routed = rms_scale(combined, expert_gain).astype(jnp.bfloat16)
    return (mixed, routed)


def solution(mesh):
    in_specs = (
        P(("ep", "tp"), None),
        P(),
        P(None, "tp"),
        P(None, "tp"),
        P(),
        P(),
        P(None, "tp"),
        P(),
        P(("ep", "tp"), None),
        P(),
        P(("ep", "tp"), None),
        P(("ep", "tp"), None),
        P("ep", None, "tp"),
        P("ep", None, "tp"),
        P("ep", "tp", None),
        P(),
    )
    out_specs = (P(("ep", "tp"), None), P(("ep", "tp"), None))
    return jax.shard_map(
        on_device, mesh=mesh, in_specs=in_specs, out_specs=out_specs, check_vma=False
    )
```

```python
import functools

import jax
import jax.numpy as jnp
from jax import lax
from jax.experimental import pallas as pl
from jax.experimental.pallas import tpu as pltpu
from jax.sharding import PartitionSpec as P

RMS_EPSILON = 1e-06
LAYER_EPSILON = 1e-05
CLAMP_LIMIT = 7.0
SWISH_ALPHA = 1.702


def passed_along(value, axis, steps):
    count = lax.axis_size(axis)
    initial, last = (max(0, -steps), min(count, count - steps))
    return lax.ppermute(value, axis, [(source, source + steps) for source in range(initial, last)])


def rms_scale(values, gain_row):
    values = values.astype(jnp.float32)
    return (
        values
        * lax.rsqrt(jnp.mean(values * values, axis=-1, keepdims=True) + RMS_EPSILON)
        * gain_row
    )


def columns(ref, owner, width, rows):
    if len(ref.shape) == 3:
        return ref.at[owner, rows, :]
    return ref.at[rows, pl.ds(pl.multiple_of(owner * width, width), width)]


def exchange_kernel(
    groups_ep,
    groups_tp,
    capacity,
    inside,
    outgoing,
    mixer_in,
    pre_gain,
    conv_kernel,
    chan_gain,
    mix_gain,
    value_own,
    gate_own,
    out_own,
    gate_hbm,
    up_hbm,
    down_hbm,
    *rest,
):
    if inside:
        mixed, returned, value_full, gate_full, out_full, *rest = rest
        normed, padded, conv, act, projected, *rest = rest
    else:
        value_full, gate_full, out_full, returned, *rest = rest
    (
    rows_all,
    hidden,
    partial,
    pair_in,
    ring_in,
    back_out,
    back_in,
    gate_vmem,
    up_vmem,
    down_vmem,
    load_sem,
    stage_sem,
    send_h,
    recv_h,
    own_sem,
    send_a,
    recv_a,
    send_r,
    recv_r,
    send_rp,
    recv_rp,
    send_w1,
    recv_w1,
    send_w2,
    recv_w2,
    send_wp,
    recv_wp,
    send_p,
    recv_p,
    send_z,
    recv_z,
    send_b,
    recv_b,
    ) = rest
    q = lax.axis_index("ep")
    t = lax.axis_index("tp")
    chips = groups_tp // 2
    z, core = t // 2, t % 2
    partner = z * 2 + 1 - core
    chunk, width = rows_all.shape[1], rows_all.shape[2]
    slots = chunk // groups_ep
    local_experts, _, units = gate_vmem.shape

    def remote(src, dst, send, recv, ep, tp):
        return pltpu.make_async_remote_copy(
            src_ref=src,
            dst_ref=dst,
            send_sem=send,
            recv_sem=recv,
            device_id=(ep, tp),
            device_id_type=pl.DeviceIdType.MESH,
        )

    barrier = pltpu.get_barrier_semaphore()
    others = [(lax.rem(q + i, groups_ep), t) for i in range(1, groups_ep)]
    others += [(q, lax.rem(z + i, chips) * 2 + core) for i in range(1, chips)]
    others += [(q, partner)]
    me, devices = q * groups_tp + t, groups_ep * groups_tp
    after, ahead = lax.rem(me + 1, devices), lax.rem(me + devices - 1, devices)
    others += [(n // groups_tp, lax.rem(n, groups_tp)) for n in (after, ahead)]

    def greet(ep, tp):
        pl.semaphore_signal(
            barrier, inc=1, device_id=(ep, tp), device_id_type=pl.DeviceIdType.MESH
        )

    for ep, tp in others:
        greet(ep, tp)

    loads = [
        pltpu.make_async_copy(src, dst, load_sem.at[i])
        for i, (src, dst) in enumerate(
            ((gate_hbm, gate_vmem), (up_hbm, up_vmem), (down_hbm, down_vmem))
        )
    ]
    weights = ((value_own, value_full), (gate_own, gate_full), (out_own, out_full))
    pl.semaphore_wait(barrier, len(others))

    def slot_rows(index):
        return pl.ds(pl.multiple_of(index * slots, slots), slots)

    own_rows = pltpu.make_async_copy(
        outgoing.at[slot_rows(q), :], rows_all.at[t, slot_rows(q), :], own_sem
    )
    own_rows.start()
    a_copies = []
    for i in range(1, groups_ep):
        there = lax.rem(q + i, groups_ep)
        copy = remote(
            outgoing.at[slot_rows(there), :],
            rows_all.at[t, slot_rows(q), :],
            send_a.at[i],
            recv_a.at[i],
            there,
            t,
        )
        copy.start()
        a_copies.append(copy)

    def sends(d, s):
        return (z >= s) & (z < chips - 1) if d == 0 else (z + s < chips) & (z > 0)

    def comes(d, s):
        return z >= 1 + s if d == 0 else z + 1 + s < chips

    def sent(d, s):
        return (z - s if d == 0 else z + s) * 2 + core

    def came(d, s):
        return sent(d, s + 1)

    def beside(d):
        return t + 2 if d == 0 else t - 2

    def quarter(k, index, cut=0):
        own = weights[k][0]
        part = own.shape[0] // groups_ep
        if cut == 0:
            return pl.ds(pl.multiple_of(index * part, part), part)
        half = part // 2
        return pl.ds(pl.multiple_of(index * part + (cut - 1) * half, half), half)

    def first_leg(k, d, s):
        own, full = weights[k]
        place = columns(full, sent(d, s), own.shape[1], quarter(k, q))
        src = own.at[quarter(k, q), :] if s == 0 else place
        return remote(src, place, send_w1.at[k, d, s], recv_w1.at[k, d, s], q, beside(d))

    flip_low = q + 1 - 2 * lax.rem(q, 2)
    flip_high = q + 2 - 4 * lax.rem(q // 2, 2)
    square = groups_ep == 4

    def second_leg(k, d, s, j):
        own, full = weights[k]
        piece, there, cut = q, lax.rem(q + j, groups_ep), 0
        if square:
            piece = (flip_high, q, q, flip_low)[j]
            there = (flip_low, flip_low, flip_high, flip_high)[j]
            cut = (2, 0, 0, 1)[j]
        place = columns(full, came(d, s), own.shape[1], quarter(k, piece, cut))
        return remote(
            place, place, send_w2.at[k, d, s, j], recv_w2.at[k, d, s, j], there, t
        )

    direct = (1, 2) if square else tuple(range(1, groups_ep))
    relayed = (0, 3) if square else ()

    def own_leg(k):
        own, full = weights[k]
        place = columns(full, t, own.shape[1], pl.ds(0, own.shape[0]))
        last = chips - 1
        return remote(own, place, send_wp.at[k, 0, last], recv_wp.at[k, 0, last], q, partner)

    def pair_leg(k, d, s):
        own, full = weights[k]
        place = columns(full, came(d, s), own.shape[1], pl.ds(0, own.shape[0]))
        return remote(place, place, send_wp.at[k, d, s], recv_wp.at[k, d, s], q, partner)

    def pass_on(k, s):
        for d in range(2):
            pl.when(sends(d, s))(lambda d=d: first_leg(k, d, s).start())

    def take(k, s):
        for d in range(2):

            @pl.when(comes(d, s))
            def _(d=d):
                first_leg(k, d, s).wait_recv()
                for j in direct:
                    second_leg(k, d, s, j).start()

    def relay(k, s):
        for d in range(2):

            @pl.when(comes(d, s))
            def _(d=d):
                for j in direct:
                    second_leg(k, d, s, j).wait_recv()
                for j in relayed:
                    second_leg(k, d, s, j).start()

    def share(k, s):
        for d in range(2):

            @pl.when(comes(d, s))
            def _(d=d):
                for j in relayed:
                    second_leg(k, d, s, j).wait_recv()
                pair_leg(k, d, s).start()

    def row_leg(d, s):
        place = rows_all.at[sent(d, s)]
        return remote(place, place, send_r.at[d, s], recv_r.at[d, s], q, beside(d))

    def row_pair(d, s):
        place = rows_all.at[came(d, s)]
        return remote(place, place, send_rp.at[d, s], recv_rp.at[d, s], q, partner)

    def own_pair():
        place, last = rows_all.at[t], chips - 1
        return remote(place, place, send_rp.at[0, last], recv_rp.at[0, last], q, partner)

    def rows_on(s):
        for d in range(2):
            pl.when(sends(d, s))(lambda d=d: row_leg(d, s).start())

    def rows_in(s):
        for d in range(2):
            pl.when(comes(d, s))(lambda d=d: row_leg(d, s).wait_recv())

    def rows_share(s):
        for d in range(2):
            pl.when(comes(d, s))(lambda d=d: row_pair(d, s).start())

    steps = chips - 1
    for k in (0,):
        pass_on(k, 0)
    stored = [
        pltpu.make_async_copy(
            own, columns(full, t, own.shape[1], pl.ds(0, own.shape[0])), stage_sem.at[k]
        )
        for k, (own, full) in enumerate(weights)
    ]
    for copy in loads + stored:
        copy.start()
    if inside:
        rim = padded.shape[0] - mixer_in.shape[0]
        length = mixer_in.shape[0]
        normed[...] = rms_scale(mixer_in[...], pre_gain[...]).astype(jnp.bfloat16)

        @pl.when(me == 0)
        def _():
            padded[pl.ds(0, rim), :] = jnp.zeros((rim, padded.shape[1]), jnp.float32)

    def halo():
        return remote(
            padded.at[pl.ds(length, rim), :],
            padded.at[pl.ds(0, rim), :],
            send_h,
            recv_h,
            after // groups_tp,
            lax.rem(after, groups_tp),
        )

    def wait_weight(k):
        stored[k].wait()
        own_leg(k).wait_recv()
        for s in range(steps):
            for d in range(2):
                pl.when(comes(d, s))(lambda d=d, s=s: pair_leg(k, d, s).wait_recv())

    def glu_stage():
        wait_weight(0)
        wait_weight(1)
        wide = min(256, value_full.shape[1])

        @pl.loop(0, value_full.shape[1] // wide)
        def _(step):
            place = pl.ds(pl.multiple_of(step * wide, wide), wide)
            rows = normed[...]
            value = jnp.dot(rows, value_full[:, place], preferred_element_type=jnp.float32)
            gate = jnp.dot(rows, gate_full[:, place], preferred_element_type=jnp.float32)
            glu = (value * jax.nn.sigmoid(gate)).astype(jnp.bfloat16)
            padded[pl.ds(rim, length), place] = glu.astype(jnp.float32)

        pl.when(me < devices - 1)(lambda: halo().start())

    def conv_stage():
        pl.when(me > 0)(lambda: halo().wait_recv())
        taps = conv_kernel.shape[0]

        @pl.loop(0, conv.shape[1] // 128)
        def _(step):
            place = pl.ds(pl.multiple_of(step * 128, 128), 128)
            total = jnp.zeros((length, 128), jnp.float32)
            for tap in range(taps):
                rows = padded[pl.ds(rim - taps + 1 + tap, length), place]
                total = total + conv_kernel[pl.ds(tap, 1), place] * rows
            conv[:, place] = total

        some = min(64, length)

        @pl.loop(0, length // some)
        def _(step):
            place = pl.ds(pl.multiple_of(step * some, some), some)
            block = conv[place, :]
            centred = block - jnp.mean(block, axis=-1, keepdims=True)
            var = jnp.mean(centred * centred, axis=-1, keepdims=True)
            scaled = centred * lax.rsqrt(var + LAYER_EPSILON) * chan_gain[...]
            act[place, :] = (scaled * jax.nn.sigmoid(scaled)).astype(jnp.bfloat16)

    def out_stage():
        wait_weight(2)
        wide = min(256, out_full.shape[1])

        @pl.loop(0, out_full.shape[1] // wide)
        def _(step):
            place = pl.ds(pl.multiple_of(step * wide, wide), wide)
            projected[:, place] = jnp.dot(
                act[...], out_full[:, place], preferred_element_type=jnp.float32
            )

        some = min(64, length)

        @pl.loop(0, length // some)
        def _(step):
            place = pl.ds(pl.multiple_of(step * some, some), some)
            mixed[place, :] = rms_scale(projected[place, :], mix_gain[...]).astype(jnp.bfloat16)

    own_rows.wait()
    for copy in a_copies:
        copy.wait_recv()
    rows_on(0)
    pass_on(1, 0)
    pass_on(2, 0)
    own_pair().start()
    for k in range(3):
        own_leg(k).start()

    take(0, 0)
    for s in range(steps):
        rows_in(s)
        if s + 1 < steps:
            rows_on(s + 1)
        rows_share(s)
        if s == min(1, steps - 1):
            take(1, 0)
            take(2, 0)
            if steps > 1:
                for k in range(3):
                    pass_on(k, 1)
            for k in range(3):
                relay(k, 0)
    own_pair().wait_recv()
    for s in range(steps):
        for d in range(2):
            pl.when(comes(d, s))(lambda d=d: row_pair(d, s).wait_recv())
    for copy in loads:
        copy.wait()

    total = groups_tp * chunk
    tile = min(256, units)
    tiles = units // tile

    @pl.loop(0, local_experts * tiles)
    def _(step):
        expert, unit = step // tiles, step % tiles
        place = pl.ds(pl.multiple_of(unit * tile, tile), tile)
        rows = rows_all[...].reshape(total, width)
        gate = jnp.dot(rows, gate_vmem[expert, :, place], preferred_element_type=jnp.float32)
        up = jnp.dot(rows, up_vmem[expert, :, place], preferred_element_type=jnp.float32)
        gate = jnp.minimum(gate, CLAMP_LIMIT)
        up = jnp.clip(up, -CLAMP_LIMIT, CLAMP_LIMIT)
        act = (up + 1.0) * gate * jax.nn.sigmoid(SWISH_ALPHA * gate)
        slot = lax.rem(lax.broadcasted_iota(jnp.int32, act.shape, 0), slots)
        mine = (slot >= expert * capacity) & (slot < (expert + 1) * capacity)
        hidden[:, pl.ds(pl.multiple_of(step * tile, tile), tile)] = jnp.where(
            mine, act, 0.0
        ).astype(jnp.bfloat16)

    for k in range(3):
        if steps > 1:
            take(k, 1)
        if steps > 2:
            pass_on(k, 2)
    for k in range(3):
        share(k, 0)

    down_tile = min(256, width)

    @pl.loop(0, width // down_tile)
    def _(step):
        place = pl.ds(pl.multiple_of(step * down_tile, down_tile), down_tile)
        weight = down_vmem[:, :, place].reshape(local_experts * units, down_tile)
        part = jnp.dot(hidden[...], weight, preferred_element_type=jnp.float32)
        partial[:, :, place] = part.astype(jnp.bfloat16).reshape(groups_tp, chunk, down_tile)

    def sum_pair(owner):
        return remote(
            partial.at[owner * 2 + 1 - core],
            pair_in.at[owner],
            send_p.at[owner],
            recv_p.at[owner],
            q,
            partner,
        )

    def sum_leg(d, owner):
        return remote(
            partial.at[owner * 2 + core],
            ring_in.at[d, owner],
            send_z.at[d, owner],
            recv_z.at[d, owner],
            q,
            beside(d),
        )

    def behind(d):
        return z > 0 if d == 0 else z < chips - 1

    def add_pair(owner):
        sum_pair(owner).wait_recv()
        place = partial.at[owner * 2 + core]
        both = place[...].astype(jnp.float32) + pair_in[owner].astype(jnp.float32)
        place[...] = both.astype(jnp.bfloat16)

    def add_line(d, owner):
        sum_leg(d, owner).wait_recv()
        place = partial.at[owner * 2 + core]
        both = place[...].astype(jnp.float32) + ring_in[d, owner].astype(jnp.float32)
        place[...] = both.astype(jnp.bfloat16)

    def send_sums(step):
        for d in range(2):
            far = z if d == 0 else chips - 1 - z
            owner = z + chips - 1 - step if d == 0 else z + step - chips + 1

            @pl.when(far <= step)
            def _(d=d, owner=owner):
                add_pair(owner)
                pl.when(behind(d))(lambda: add_line(d, owner))
                sum_leg(d, owner).start()

    order = []
    for j in range(chips):
        order += [o for o in (chips - 1 - j, j) if o not in order]
    for owner in order:
        sum_pair(owner).start()
    for s in range(2, steps):
        for k in range(3):
            take(k, s)
            if s + 1 < steps:
                pass_on(k, s + 1)
    send_sums(0)
    for k in range(3):
        if steps > 1:
            relay(k, 1)
    if steps > 1:
        send_sums(1)
    for k in range(3):
        if steps > 1:
            share(k, 1)
        for s in range(2, steps):
            relay(k, s)
    for s in range(2, steps):
        for k in range(3):
            share(k, s)
    if inside:
        glu_stage()
    for step in range(2, steps):
        send_sums(step)
    if inside:
        conv_stage()
    add_pair(z)
    if inside:
        out_stage()
    for d in range(2):
        pl.when(behind(d))(lambda d=d: add_line(d, z))
    summed = partial[t].astype(jnp.float32)
    back_out[...] = summed.astype(jnp.bfloat16)

    def back_leg(i):
        there = lax.rem(q + i, groups_ep)
        return remote(
            back_out.at[slot_rows(there), :],
            back_in.at[slot_rows(q), :],
            send_b.at[i],
            recv_b.at[i],
            there,
            t,
        )

    for i in range(1, groups_ep):
        back_leg(i).start()
    back_in[slot_rows(q), :] = back_out[slot_rows(q), :]
    for i in range(1, groups_ep):
        back_leg(i).wait_recv()
    returned[...] = back_in[...]

    for k in range(3):
        own_leg(k).wait_send()
        if not inside:
            wait_weight(k)
    if inside:
        pl.when(me < devices - 1)(lambda: halo().wait_send())
    own_pair().wait_send()
    for s in range(steps):
        for d in range(2):

            @pl.when(sends(d, s))
            def _(d=d, s=s):
                row_leg(d, s).wait_send()
                for k in range(3):
                    first_leg(k, d, s).wait_send()

            @pl.when(comes(d, s))
            def _(d=d, s=s):
                row_pair(d, s).wait_send()
                for k in range(3):
                    for j in direct + relayed:
                        second_leg(k, d, s, j).wait_send()
                    pair_leg(k, d, s).wait_send()
    for owner in range(chips):
        sum_pair(owner).wait_send()
        pl.when(z < owner)(lambda owner=owner: sum_leg(0, owner).wait_send())
        pl.when(z > owner)(lambda owner=owner: sum_leg(1, owner).wait_send())
    for i in range(1, groups_ep):
        a_copies[i - 1].wait_send()
        back_leg(i).wait_send()


def exchange(
    mixer_in,
    pre_gain,
    conv_kernel,
    chan_gain,
    mix_gain,
    outgoing,
    glu_value,
    glu_gate,
    out_weight,
    gate_proj,
    up_proj,
    down_proj,
    capacity,
):
    groups_ep, groups_tp = lax.axis_size("ep"), lax.axis_size("tp")
    chips = groups_tp // 2
    chunk, width = outgoing.shape
    units = gate_proj.shape[2] * gate_proj.shape[0]
    half = jnp.bfloat16

    def gathered(shard):
        rows, cols = shard.shape
        if cols % 128:
            return jax.ShapeDtypeStruct((groups_tp, rows, cols), half)
        return jax.ShapeDtypeStruct((rows, groups_tp * cols), half)

    own = (glu_value, glu_gate, out_weight)
    dma = pltpu.SemaphoreType.DMA
    inside = glu_value.shape[1] % 128 == 0 and out_weight.shape[1] % 128 == 0
    full_shapes = [gathered(shard) for shard in own]
    back_shape = jax.ShapeDtypeStruct((chunk, width), half)
    length, channels = mixer_in.shape[0], conv_kernel.shape[1]
    rim = -(-(conv_kernel.shape[0] - 1) // 8) * 8
    anywhere, vmem = pl.BlockSpec(memory_space=pl.ANY), pl.BlockSpec(memory_space=pltpu.VMEM)
    own_scratch = []
    if inside:
        own_scratch = [pltpu.VMEM(shape.shape, half) for shape in full_shapes] + [
            pltpu.VMEM(mixer_in.shape, half),
            pltpu.VMEM((rim + length, channels), jnp.float32),
            pltpu.VMEM((length, channels), jnp.float32),
            pltpu.VMEM((length, channels), half),
            pltpu.VMEM(mixer_in.shape, jnp.float32),
        ]
        mixer_specs = [vmem] * 5
    else:
        mixer_specs = [anywhere] * 5
    outs = pl.pallas_call(
        functools.partial(exchange_kernel, groups_ep, groups_tp, capacity, inside),
        out_shape=[jax.ShapeDtypeStruct(mixer_in.shape, half), back_shape]
        if inside
        else full_shapes + [back_shape],
        in_specs=[vmem] + mixer_specs + [anywhere] * 6,
        out_specs=[vmem] * 2 if inside else [anywhere] * 3 + [vmem],
        scratch_shapes=own_scratch
        + [
            pltpu.VMEM((groups_tp, chunk, width), half),
            pltpu.VMEM((groups_tp * chunk, units), half),
            pltpu.VMEM((groups_tp, chunk, width), half),
            pltpu.VMEM((chips, chunk, width), half),
            pltpu.VMEM((2, chips, chunk, width), half),
            pltpu.VMEM((chunk, width), half),
            pltpu.VMEM((chunk, width), half),
            pltpu.VMEM(gate_proj.shape, half),
            pltpu.VMEM(up_proj.shape, half),
            pltpu.VMEM(down_proj.shape, half),
            dma((3,)),
            dma((3,)),
            dma,
            dma,
            dma,
            dma((groups_ep,)),
            dma((groups_ep,)),
            dma((2, chips)),
            dma((2, chips)),
            dma((2, chips)),
            dma((2, chips)),
            dma((3, 2, chips)),
            dma((3, 2, chips)),
            dma((3, 2, chips, groups_ep)),
            dma((3, 2, chips, groups_ep)),
            dma((3, 2, chips)),
            dma((3, 2, chips)),
            dma((chips,)),
            dma((chips,)),
            dma((2, chips)),
            dma((2, chips)),
            dma((groups_ep,)),
            dma((groups_ep,)),
        ],
        compiler_params=pltpu.CompilerParams(
            collective_id=0, has_side_effects=True, vmem_limit_bytes=60 * 1024 * 1024
        ),
    )(
        outgoing,
        mixer_in,
        pre_gain[None],
        conv_kernel,
        chan_gain[None],
        mix_gain[None],
        *own,
        gate_proj,
        up_proj,
        down_proj,
    )
    if inside:
        return None, outs[0], outs[1]
    full = [
        value if value.ndim == 2 else value.transpose(1, 0, 2).reshape(value.shape[1], -1)
        for value in outs[:3]
    ]
    return full, None, outs[3]


def flipped(index, bit):
    return index + bit - 2 * bit * lax.rem(index // bit, 2)


def across(index, distance):
    bit = 1
    while bit <= distance:
        if distance & bit:
            index = flipped(index, bit)
        bit *= 2
    return index


def fused_kernel(
    groups_ep,
    groups_tp,
    capacity,
    expert_in_hbm,
    ffn_gain_hbm,
    routes_hbm,
    shares_hbm,
    expert_gain_hbm,
    mixer_hbm,
    pre_gain_hbm,
    conv_kernel_hbm,
    chan_gain_hbm,
    value_own,
    gate_own,
    out_own,
    gate_hbm,
    up_hbm,
    down_hbm,
    projected_hbm,
    routed_hbm,
    expert_in,
    ffn_gain,
    routes,
    shares,
    expert_gain,
    pre_gain,
    conv_kernel,
    chan_gain,
    value_full,
    gate_full,
    out_full,
    mixer_in,
    normed,
    padded,
    tail_out,
    tail_in,
    conv,
    act,
    projected,
    routed,
    info,
    rows_all,
    picked,
    hidden,
    partial,
    pair_in,
    ring_in,
    back_in,
    gate_vmem,
    up_vmem,
    down_vmem,
    load_sem,
    stage_sem,
    out_sem,
    send_h,
    recv_h,
    send_rows,
    recv_rz,
    recv_rx,
    recv_rd,
    recv_rp,
    send_w1,
    recv_w1,
    send_w2,
    recv_w2,
    send_wp,
    recv_wp,
    send_p,
    recv_p,
    send_z,
    recv_z,
    send_b,
    recv_b,
):
    q = lax.axis_index("ep")
    t = lax.axis_index("tp")
    chips = groups_tp // 2
    z, core = t // 2, t % 2
    partner = z * 2 + 1 - core
    tokens, width = expert_in.shape
    slots = partial.shape[2]
    local_experts, _, units = gate_vmem.shape
    top_count = routes.shape[0]
    half_tokens = tokens // 2

    def remote(src, dst, send, recv, ep, tp):
        return pltpu.make_async_remote_copy(
            src_ref=src,
            dst_ref=dst,
            send_sem=send,
            recv_sem=recv,
            device_id=(ep, tp),
            device_id_type=pl.DeviceIdType.MESH,
        )

    barrier = pltpu.get_barrier_semaphore()
    others = [(lax.rem(q + i, groups_ep), t) for i in range(1, groups_ep)]
    others += [(q, lax.rem(z + i, chips) * 2 + core) for i in range(1, chips)]
    others += [(q, partner)]
    me, devices = q * groups_tp + t, groups_ep * groups_tp
    after, ahead = lax.rem(me + 1, devices), lax.rem(me + devices - 1, devices)
    others += [(n // groups_tp, lax.rem(n, groups_tp)) for n in (after, ahead)]
    for ep, tp in others:
        pl.semaphore_signal(
            barrier, inc=1, device_id=(ep, tp), device_id_type=pl.DeviceIdType.MESH
        )

    weights = ((value_own, value_full), (gate_own, gate_full), (out_own, out_full))
    stored = [
        pltpu.make_async_copy(
            own, columns(full, t, own.shape[1], pl.ds(0, own.shape[0])), stage_sem.at[k]
        )
        for k, (own, full) in enumerate(weights)
    ]
    def loaded(number, src, dst):
        return pltpu.make_async_copy(src, dst, load_sem.at[number])

    row_loads = [
        loaded(i, src, dst)
        for i, (src, dst) in enumerate(
            (
                (expert_in_hbm, expert_in),
                (ffn_gain_hbm, ffn_gain),
                (routes_hbm, routes),
                (shares_hbm, shares),
            )
        )
    ]
    mixer_loads = [
        loaded(4 + i, src, dst)
        for i, (src, dst) in enumerate(
            (
                (mixer_hbm, mixer_in),
                (pre_gain_hbm, pre_gain),
                (conv_kernel_hbm, conv_kernel),
                (chan_gain_hbm, chan_gain),
                (expert_gain_hbm, expert_gain),
            )
        )
    ]
    loads = [
        loaded(9 + i, src, dst)
        for i, (src, dst) in enumerate(
            ((gate_hbm, gate_vmem), (up_hbm, up_vmem), (down_hbm, down_vmem))
        )
    ]
    for copy in row_loads + mixer_loads + stored + loads:
        copy.start()
    for copy in row_loads:
        copy.wait()

    rows_all[0, t, :, pl.ds(0, width)] = rms_scale(expert_in[...], ffn_gain[...]).astype(
        jnp.bfloat16
    )
    lanes = 128
    expert_ids = lax.broadcasted_iota(jnp.int32, (lanes, tokens), 0)
    chosen = [routes[pl.ds(k, 1), :] == expert_ids for k in range(top_count)]
    named = sum(c.astype(jnp.float32) for c in chosen)
    earlier = lax.broadcasted_iota(jnp.int32, (tokens, tokens), 0) < lax.broadcasted_iota(
        jnp.int32, (tokens, tokens), 1
    )
    rank = jnp.dot(
        named.astype(jnp.bfloat16),
        earlier.astype(jnp.float32).astype(jnp.bfloat16),
        preferred_element_type=jnp.float32,
    )
    group_ids = expert_ids // local_experts
    base = group_ids * slots + (expert_ids - group_ids * local_experts) * capacity
    spot = rank + base.astype(jnp.float32)
    facts = jnp.zeros((lanes, tokens), jnp.float32)
    for k in range(top_count):
        slot = jnp.sum(jnp.where(chosen[k], spot, 0.0), axis=0, keepdims=True)
        facts = facts + jnp.where(expert_ids == k, slot, 0.0)
        facts = facts + jnp.where(expert_ids == top_count + k, shares[pl.ds(k, 1), :], 0.0)
    info[...] = facts.T
    rows_all[0, t, :, pl.ds(width, lanes)] = info[...].astype(jnp.bfloat16)

    pl.semaphore_wait(barrier, len(others))

    def took(ref, sem):
        remote(ref, ref, sem, sem, q, partner).wait_send()

    def row_z(m):
        place = rows_all.at[0, t]
        return remote(place, place, send_rows.at[0], recv_rz.at[m], q, across(z, m) * 2 + core)

    def row_beside(b, m):
        owner = across(z, m) * 2 + core
        return remote(
            rows_all.at[0, owner],
            rows_all.at[1 + b, owner],
            send_rows.at[1],
            recv_rx.at[m],
            flipped(q, 1 + b),
            t,
        )

    def row_far(b, m):
        owner = across(z, m) * 2 + core
        some = pl.ds(b * half_tokens, half_tokens)
        return remote(
            rows_all.at[2 - b, owner, some, :],
            rows_all.at[3, owner, some, :],
            send_rows.at[2],
            recv_rd.at[m],
            flipped(q, 1 + b),
            t,
        )

    def row_pair(j, m):
        place = rows_all.at[j, across(z, m) * 2 + core]
        return remote(place, place, send_rows.at[3], recv_rp.at[j], q, partner)

    def rows_start():
        for m in range(1, chips):
            row_z(m).start()

    def rows_here(m):
        if m:
            took(rows_all.at[0, t], recv_rz.at[m])
        for b in range(2):
            row_beside(b, m).start()
        row_pair(0, m).start()

    def rows_beside(m):
        took(rows_all.at[0, pl.ds(0, 2)], recv_rx.at[m])
        for b in range(2):
            row_far(1 - b, m).start()
            row_pair(1 + b, m).start()

    def rows_far(m):
        took(rows_all.at[0, t], recv_rd.at[m])
        row_pair(3, m).start()

    def rows_left():
        took(rows_all.at[0, pl.ds(0, chips - 1)], send_rows.at[0])
        took(rows_all.at[0, pl.ds(0, 2 * chips)], send_rows.at[1])
        took(rows_all.at[0, pl.ds(0, chips)], send_rows.at[2])
        took(rows_all.at[:, pl.ds(0, chips)], send_rows.at[3])

    def sends(d, s):
        return (z >= s) & (z < chips - 1) if d == 0 else (z + s < chips) & (z > 0)

    def comes(d, s):
        return z >= 1 + s if d == 0 else z + 1 + s < chips

    def sent(d, s):
        return (z - s if d == 0 else z + s) * 2 + core

    def came(d, s):
        return sent(d, s + 1)

    def beside(d):
        return t + 2 if d == 0 else t - 2

    def quarter(k, index, cut=0):
        own = weights[k][0]
        part = own.shape[0] // groups_ep
        if cut == 0:
            return pl.ds(pl.multiple_of(index * part, part), part)
        half = part // 2
        return pl.ds(pl.multiple_of(index * part + (cut - 1) * half, half), half)

    bundles = ((0, 1), (2,))

    side = lax.rem(lax.rem(q, 2) + q // 2, 2)

    def piece_rows(g, k):
        if g == 0:
            return quarter(k, q)
        half = weights[k][0].shape[0] // 2
        return pl.ds(pl.multiple_of(side * half, half), half)

    def first_leg(g, k, d, s):
        own, full = weights[k]
        rows = piece_rows(g, k)
        place = columns(full, sent(d, s), own.shape[1], rows)
        src = own.at[rows, :] if s == 0 else place
        return remote(src, place, send_w1.at[d, s], recv_w1.at[g, d, s], q, beside(d))

    flip_low, flip_high = flipped(q, 1), flipped(q, 2)
    direct, relayed = (1, 2), (0, 3)

    def second_leg(g, k, d, s, j):
        own, full = weights[k]
        piece = (flip_high, q, q, flip_low)[j]
        there = (flip_low, flip_low, flip_high, flip_high)[j]
        cut = (2, 0, 0, 1)[j]
        if g:
            piece, cut = side * 2 + j - 1, 0
        place = columns(full, came(d, s), own.shape[1], quarter(k, piece, cut))
        kind = 0 if j in direct else 1
        return remote(
            place, place, send_w2, recv_w2.at[g, kind, d, s], there, t
        )

    def own_leg(g, k):
        own, full = weights[k]
        place = columns(full, t, own.shape[1], pl.ds(0, own.shape[0]))
        last = chips - 1
        return remote(own, place, send_wp.at[k], recv_wp.at[g, 0, last], q, partner)

    def pair_leg(g, k, d, s):
        own, full = weights[k]
        place = columns(full, came(d, s), own.shape[1], pl.ds(0, own.shape[0]))
        return remote(place, place, send_wp.at[k], recv_wp.at[g, d, s], q, partner)

    share_rows, share_wide = value_own.shape

    def took_shares(quarters, sem):
        tall = max(r for r in range(1, groups_ep + 1) if quarters % r == 0)
        rows = pl.ds(0, share_rows // groups_ep * tall)
        took(value_full.at[rows, pl.ds(0, quarters // tall * share_wide)], sem)

    def passes(g, s):
        for d in range(2):

            @pl.when(sends(d, s))
            def _(d=d):
                for k in bundles[g]:
                    first_leg(g, k, d, s).start()

    def own_legs(g):
        for k in bundles[g]:
            own_leg(g, k).start()

    def takes(g, s):
        for d in range(2):

            @pl.when(comes(d, s))
            def _(d=d):
                took_shares(2, recv_w1.at[g, d, s])
                if s + 1 < steps:

                    @pl.when(sends(d, s + 1))
                    def _():
                        for k in bundles[g]:
                            first_leg(g, k, d, s + 1).start()

                for j in direct:
                    for k in bundles[g]:
                        second_leg(g, k, d, s, j).start()

    def relays(g, s):
        for d in range(2):

            @pl.when(comes(d, s))
            def _(d=d):
                took_shares(2 * len(bundles[g]), recv_w2.at[g, 0, d, s])
                for j in relayed:
                    for k in bundles[g]:
                        second_leg(g, k, d, s, j).start()

    def shares_on(g, s):
        for d in range(2):

            @pl.when(comes(d, s))
            def _(d=d):
                took_shares(2, recv_w2.at[g, 1 - g, d, s])
                for k in bundles[g]:
                    pair_leg(g, k, d, s).start()

    def wait_plane(g, m):
        if m == 0:
            for k in bundles[g]:
                stored[k].wait()
            took_shares(groups_ep * len(bundles[g]), recv_wp.at[g, 0, chips - 1])
            return
        plane = across(z, m)
        d = (plane > z).astype(jnp.int32)
        s = (plane - z) * (2 * d - 1) - 1
        took_shares(groups_ep * len(bundles[g]), recv_wp.at[g, d, s])

    def shares_left():
        took_shares(8 * steps, send_w2)
        for k in range(3):
            took_shares(groups_ep * chips, send_wp.at[k])
        for s in range(steps):
            for d in range(2):

                @pl.when(sends(d, s))
                def _(d=d, s=s):
                    took_shares(4, send_w1.at[d, s])

    length = mixer_in.shape[0]
    rim = padded.shape[1] - length
    lane_blocks = padded.shape[0]

    def norm_stage():
        for copy in mixer_loads:
            copy.wait()
        some = min(64, length)

        @pl.loop(0, length // some)
        def _(step):
            place = pl.ds(pl.multiple_of(step * some, some), some)
            normed[place, :] = rms_scale(mixer_in[place, :], pre_gain[...]).astype(jnp.bfloat16)

    def glu_stage(m):
        wait_plane(0, m)
        wide = 2 * value_own.shape[1]
        place = pl.ds(pl.multiple_of(across(z, m) * wide, wide), wide)
        rows = normed[...]
        value = jnp.dot(rows, value_full[:, place], preferred_element_type=jnp.float32)
        gate = jnp.dot(rows, gate_full[:, place], preferred_element_type=jnp.float32)
        glu = (value * jax.nn.sigmoid(gate)).astype(jnp.bfloat16)
        for i in range(wide // lanes):
            padded[across(z, m) * (wide // lanes) + i, pl.ds(rim, length), :] = glu[
                :, i * lanes : (i + 1) * lanes
            ].astype(jnp.float32)
        tail_out[:, place] = glu[length - rim :, :]
        pl.when(me < devices - 1)(lambda: halo(place).start())

    def halo(place):
        return remote(
            tail_out.at[:, place],
            tail_in.at[:, place],
            send_h,
            recv_h,
            after // groups_tp,
            lax.rem(after, groups_tp),
        )

    taps = conv_kernel.shape[0]
    some = min(64, length)
    head_steps = -(-rim // some)

    def conv_rows(step, start, count):
        place = pl.ds(pl.multiple_of(step * lanes, lanes), lanes)
        total = jnp.zeros((count, lanes), jnp.float32)
        for tap in range(taps):
            rows = padded[step, pl.ds(rim + start - taps + 1 + tap, count), :]
            total = total + conv_kernel[pl.ds(tap, 1), place] * rows
        conv[pl.ds(start, count), place] = total

    def conv_stage(part):
        here = lane_blocks // chips

        @pl.loop(part * here, (part + 1) * here)
        def _(step):
            conv_rows(step, rim, length - rim)

    def conv_head():
        @pl.when(me > 0)
        def _():
            took(tail_in, recv_h)
            for i in range(lane_blocks):
                padded[i, pl.ds(0, rim), :] = tail_in[:, i * lanes : (i + 1) * lanes].astype(
                    jnp.float32
                )

        @pl.when(me == 0)
        def _():
            padded[:, pl.ds(0, rim), :] = jnp.zeros((lane_blocks, rim, lanes), jnp.float32)

        @pl.loop(0, lane_blocks)
        def _(step):
            conv_rows(step, 0, rim)

    def act_rows(first, last):
        @pl.loop(first, last)
        def _(step):
            place = pl.ds(pl.multiple_of(step * some, some), some)
            block = conv[place, :]
            centred = block - jnp.mean(block, axis=-1, keepdims=True)
            var = jnp.mean(centred * centred, axis=-1, keepdims=True)
            scaled = centred * lax.rsqrt(var + LAYER_EPSILON) * chan_gain[...]
            act[place, :] = (scaled * jax.nn.sigmoid(scaled)).astype(jnp.bfloat16)

    def act_tail():
        act_rows(head_steps, length // some)

    def act_head():
        act_rows(0, head_steps)

    def out_stage(m):
        wait_plane(1, m)
        wide = out_own.shape[1]
        start = across(z, m) * 2 * wide
        for i in range(2):
            place = pl.ds(pl.multiple_of(start + i * wide, wide), wide)
            projected[:, place] = jnp.dot(
                act[...], out_full[:, place], preferred_element_type=jnp.float32
            )
        projected_out(m).start()

    def projected_out(m):
        both = 2 * out_own.shape[1]
        place = pl.ds(pl.multiple_of(across(z, m) * both, both), both)
        return pltpu.make_async_copy(
            projected.at[:, place], projected_hbm.at[:, place], out_sem.at[m]
        )

    total = groups_tp * slots
    tile = min(512, units)
    tiles = units // tile
    down_tile = min(512, width)

    def pick_stage(j):
        took(rows_all.at[0, pl.ds(0, chips)], recv_rp.at[j])
        if j == 0:
            for copy in loads:
                copy.wait()
        every = groups_tp * tokens
        block = rows_all[j].reshape(every, width + lanes)
        facts = block[:, width:].astype(jnp.float32)
        slot_ids = lax.broadcasted_iota(jnp.int32, (every, total), 1).astype(jnp.float32)
        owner = lax.broadcasted_iota(jnp.int32, (every, 1), 0) // tokens
        first = (owner * slots).astype(jnp.float32)
        low = (q * slots).astype(jnp.float32)
        pick = jnp.zeros((every, total), jnp.float32)
        for k in range(top_count):
            local = facts[:, k : k + 1] - low
            mine = (local >= 0.0) & (local < float(slots))
            target = jnp.where(mine, local + first, -1.0)
            pick = pick + (target == slot_ids).astype(jnp.float32)
        picked[...] = jnp.dot(
            pick.T.astype(jnp.bfloat16), block[:, :width], preferred_element_type=jnp.float32
        ).astype(jnp.bfloat16)

    def up_stage(j, expert):
        @pl.loop(0, tiles)
        def _(unit):
            step = expert * tiles + unit
            place = pl.ds(pl.multiple_of(unit * tile, tile), tile)
            rows = picked[...]
            gate = jnp.dot(rows, gate_vmem[expert, :, place], preferred_element_type=jnp.float32)
            up = jnp.dot(rows, up_vmem[expert, :, place], preferred_element_type=jnp.float32)
            gate = jnp.minimum(gate, CLAMP_LIMIT)
            up = jnp.clip(up, -CLAMP_LIMIT, CLAMP_LIMIT)
            unit_act = (up + 1.0) * gate * jax.nn.sigmoid(SWISH_ALPHA * gate)
            slot = lax.rem(lax.broadcasted_iota(jnp.int32, unit_act.shape, 0), slots)
            mine = (slot >= expert * capacity) & (slot < (expert + 1) * capacity)
            hidden[:, pl.ds(pl.multiple_of(step * tile, tile), tile)] = jnp.where(
                mine, unit_act, 0.0
            ).astype(jnp.bfloat16)

    def down_stage(j):
        @pl.loop(0, width // down_tile)
        def _(step):
            place = pl.ds(pl.multiple_of(step * down_tile, down_tile), down_tile)
            weight = down_vmem[:, :, place].reshape(local_experts * units, down_tile)
            part = jnp.dot(hidden[...], weight, preferred_element_type=jnp.float32)
            partial[j, :, :, place] = part.astype(jnp.bfloat16).reshape(
                groups_tp, slots, down_tile
            )

        for owner in owners:
            sum_pair(j, owner).start()

    owners = []
    for i in range(chips):
        owners += [o for o in (chips - 1 - i, i) if o not in owners]

    def sum_pair(j, owner):
        return remote(
            partial.at[j, owner * 2 + 1 - core],
            pair_in.at[j, owner],
            send_p,
            recv_p.at[j],
            q,
            partner,
        )

    def owner_of(d, step):
        return z + chips - 1 - step if d == 0 else z + step - chips + 1

    def sum_leg(j, d, step):
        owner = owner_of(d, step)
        return remote(
            partial.at[j, owner * 2 + core],
            ring_in.at[j, d, owner],
            send_z,
            recv_z.at[j, d, step],
            q,
            beside(d),
        )

    def behind(d):
        return z > 0 if d == 0 else z < chips - 1

    def add_to(j, owner, other):
        place = partial.at[j, owner * 2 + core]
        both = place[...].astype(jnp.float32) + other[...].astype(jnp.float32)
        place[...] = both.astype(jnp.bfloat16)

    def add_line(j, d, owner, step):
        took(partial.at[j, t], recv_z.at[j, d, step])
        add_to(j, owner, ring_in.at[j, d, owner])

    def send_sums(j, step):
        if step == 0:
            took(pair_in.at[j], recv_p.at[j])
        for d in range(2):
            far = z if d == 0 else chips - 1 - z

            @pl.when(far <= step)
            def _(d=d):
                owner = owner_of(d, step)
                add_to(j, owner, pair_in.at[j, owner])
                if step:
                    pl.when(behind(d))(lambda: add_line(j, d, owner, step - 1))
                sum_leg(j, d, step).start()

    def back_leg(j):
        return remote(
            partial.at[j, t], back_in.at[j - 1], send_b, recv_b, across(q, j), t
        )

    def own_sums(j):
        add_to(j, z, pair_in.at[j, z])
        for d in range(2):
            pl.when(behind(d))(lambda d=d: add_line(j, d, z, chips - 2))
        if j:
            back_leg(j).start()

    def sums_left():
        took(pair_in, send_p)
        took(pair_in.at[:, pl.ds(0, steps)], send_z)
        took(back_in, send_b)

    def routed_stage():
        took(back_in, recv_b)
        facts = info[...]
        total_rows = jnp.zeros((tokens, width), jnp.float32)
        slot_ids = lax.broadcasted_iota(jnp.int32, (tokens, slots), 1)
        for j in range(groups_ep):
            block = partial[0, t] if j == 0 else back_in[j - 1]
            low = across(q, j) * slots
            shared = jnp.zeros((tokens, slots), jnp.float32)
            for k in range(top_count):
                here = facts[:, k : k + 1] == (slot_ids + low).astype(jnp.float32)
                share_of = facts[:, top_count + k : top_count + k + 1]
                shared = shared + jnp.where(here, share_of, 0.0)
            high = shared.astype(jnp.bfloat16)
            rest = (shared - high.astype(jnp.float32)).astype(jnp.bfloat16)
            for term in (high, rest):
                total_rows = total_rows + jnp.dot(
                    term, block, preferred_element_type=jnp.float32
                )
        routed[...] = rms_scale(total_rows, expert_gain[...]).astype(jnp.bfloat16)
        routed_out().start()

    def routed_out():
        return pltpu.make_async_copy(routed, routed_hbm, out_sem.at[chips])

    steps = chips - 1
    rows_start()
    passes(0, 0)
    passes(1, 0)
    rows_here(0)
    norm_stage()
    rows_beside(0)
    rows_here(1)
    rows_here(2)
    rows_beside(1)
    rows_here(3)
    pick_stage(0)
    own_legs(0)
    rows_beside(2)
    up_stage(0, 0)
    rows_far(1)
    up_stage(0, 1)
    rows_beside(3)
    takes(0, 0)
    down_stage(0)
    pick_stage(1)
    up_stage(1, 0)
    send_sums(0, 0)
    up_stage(1, 1)
    rows_far(3)
    down_stage(1)
    takes(0, 1)
    pick_stage(2)
    send_sums(0, 1)
    rows_far(0)
    send_sums(1, 0)
    send_sums(1, 1)
    up_stage(2, 0)
    rows_far(2)
    takes(1, 0)
    up_stage(2, 1)
    down_stage(2)
    pick_stage(3)
    relays(0, 0)
    send_sums(0, 2)
    send_sums(2, 0)
    up_stage(3, 0)
    up_stage(3, 1)
    send_sums(2, 1)
    takes(0, 2)
    down_stage(3)
    shares_on(1, 0)
    own_legs(1)
    relays(0, 1)
    send_sums(3, 0)
    relays(0, 2)
    takes(1, 1)
    send_sums(3, 1)
    glu_stage(0)
    shares_on(0, 0)
    send_sums(3, 2)
    own_sums(0)
    send_sums(1, 2)
    shares_on(0, 1)
    glu_stage(1)
    shares_on(0, 2)
    takes(1, 2)
    send_sums(2, 2)
    own_sums(3)
    glu_stage(3)
    glu_stage(2)
    own_sums(1)
    conv_stage(3)
    shares_on(1, 1)
    conv_stage(1)
    own_sums(2)
    conv_stage(0)
    conv_stage(2)
    shares_on(1, 2)
    act_tail()
    conv_head()
    act_head()
    out_stage(0)
    out_stage(2)
    out_stage(3)
    out_stage(1)
    routed_stage()

    rows_left()
    shares_left()
    pl.when(me < devices - 1)(lambda: took(tail_out, send_h))
    sums_left()
    for m in range(chips):
        projected_out(m).wait()
    routed_out().wait()


def finish_kernel(
    projected_hbm,
    routed_hbm,
    gain_hbm,
    mixed_hbm,
    routed_out_hbm,
    projected,
    routed,
    gain,
    mixed,
    in_sem,
    out_sem,
):
    length = projected.shape[0]
    parts = mixed_hbm.shape[0] // min(64, mixed_hbm.shape[0])
    some = length // parts

    def row_copy(i, src, dst, sem):
        rows = pl.ds(i * some, some)
        return pltpu.make_async_copy(src.at[rows, :], dst.at[rows, :], sem.at[i])

    gain_in = pltpu.make_async_copy(gain_hbm, gain, in_sem.at[parts])
    routed_in = pltpu.make_async_copy(routed_hbm, routed, in_sem.at[parts + 1])
    routed_back = pltpu.make_async_copy(routed, routed_out_hbm, out_sem.at[parts])
    gain_in.start()
    for i in range(parts):
        row_copy(i, projected_hbm, projected, in_sem).start()
    routed_in.start()
    gain_in.wait()
    for i in range(parts):
        row_copy(i, projected_hbm, projected, in_sem).wait()
        rows = pl.ds(i * some, some)
        mixed[rows, :] = rms_scale(projected[rows, :], gain[...]).astype(jnp.bfloat16)
        row_copy(i, mixed, mixed_hbm, out_sem).start()
    routed_in.wait()
    routed_back.start()
    for i in range(parts):
        row_copy(i, mixed, mixed_hbm, out_sem).wait()
    routed_back.wait()


def fused(
    mixer_in,
    pre_gain,
    glu_value,
    glu_gate,
    conv_kernel,
    chan_gain,
    out_weight,
    mix_gain,
    expert_in,
    ffn_gain,
    routing,
    route_weight,
    gate_proj,
    up_proj,
    down_proj,
    expert_gain,
    capacity,
    slots,
):
    groups_ep, groups_tp = lax.axis_size("ep"), lax.axis_size("tp")
    chips = groups_tp // 2
    tokens, width = expert_in.shape
    length, channels = mixer_in.shape[0], conv_kernel.shape[1]
    units = gate_proj.shape[2] * gate_proj.shape[0]
    half, full = jnp.bfloat16, jnp.float32
    dma = pltpu.SemaphoreType.DMA
    rim = -(-(conv_kernel.shape[0] - 1) // 8) * 8
    anywhere = pl.BlockSpec(memory_space=pl.ANY)

    def gathered(shard):
        return pltpu.VMEM((shard.shape[0], groups_tp * shard.shape[1]), half)

    projected, routed = pl.pallas_call(
        functools.partial(fused_kernel, groups_ep, groups_tp, capacity),
        out_shape=[
            jax.ShapeDtypeStruct(mixer_in.shape, full),
            jax.ShapeDtypeStruct(expert_in.shape, half),
        ],
        in_specs=[anywhere] * 15,
        out_specs=[anywhere] * 2,
        scratch_shapes=[
            pltpu.VMEM(expert_in.shape, half),
            pltpu.VMEM((1, width), full),
            pltpu.VMEM(routing.shape[::-1], routing.dtype),
            pltpu.VMEM(route_weight.shape[::-1], full),
            pltpu.VMEM((1, width), full),
            pltpu.VMEM((1, width), full),
            pltpu.VMEM(conv_kernel.shape, full),
            pltpu.VMEM((1, channels), full),
            gathered(glu_value),
            gathered(glu_gate),
            gathered(out_weight),
            pltpu.VMEM(mixer_in.shape, half),
            pltpu.VMEM(mixer_in.shape, half),
            pltpu.VMEM((channels // 128, rim + length, 128), full),
            pltpu.VMEM((rim, channels), half),
            pltpu.VMEM((rim, channels), half),
            pltpu.VMEM((length, channels), full),
            pltpu.VMEM((length, channels), half),
            pltpu.VMEM(mixer_in.shape, full),
            pltpu.VMEM(expert_in.shape, half),
            pltpu.VMEM((tokens, 128), full),
            pltpu.VMEM((groups_ep, groups_tp, tokens, width + 128), half),
            pltpu.VMEM((groups_tp * slots, width), half),
            pltpu.VMEM((groups_tp * slots, units), half),
            pltpu.VMEM((groups_ep, groups_tp, slots, width), half),
            pltpu.VMEM((groups_ep, chips, slots, width), half),
            pltpu.VMEM((groups_ep, 2, chips, slots, width), half),
            pltpu.VMEM((groups_ep - 1, slots, width), half),
            pltpu.VMEM(gate_proj.shape, half),
            pltpu.VMEM(up_proj.shape, half),
            pltpu.VMEM(down_proj.shape, half),
            dma((12,)),
            dma((3,)),
            dma((chips + 1,)),
            dma,
            dma,
            dma((4,)),
            dma((chips,)),
            dma((chips,)),
            dma((chips,)),
            dma((groups_ep,)),
            dma((2, chips - 1)),
            dma((2, 2, chips - 1)),
            dma,
            dma((2, 2, 2, chips - 1)),
            dma((3,)),
            dma((2, 2, chips)),
            dma,
            dma((groups_ep,)),
            dma,
            dma((groups_ep, 2, chips - 1)),
            dma,
            dma,
        ],
        compiler_params=pltpu.CompilerParams(
            collective_id=0, has_side_effects=True, vmem_limit_bytes=60 * 1024 * 1024
        ),
    )(
        expert_in,
        ffn_gain[None],
        routing.T,
        route_weight.T,
        expert_gain[None],
        mixer_in,
        pre_gain[None],
        conv_kernel,
        chan_gain[None],
        glu_value,
        glu_gate,
        out_weight,
        gate_proj,
        up_proj,
        down_proj,
    )
    parts = length // min(64, length)
    return pl.pallas_call(
        finish_kernel,
        out_shape=[
            jax.ShapeDtypeStruct(mixer_in.shape, half),
            jax.ShapeDtypeStruct(expert_in.shape, half),
        ],
        in_specs=[anywhere] * 3,
        out_specs=[anywhere] * 2,
        scratch_shapes=[
            pltpu.VMEM(mixer_in.shape, full),
            pltpu.VMEM(expert_in.shape, half),
            pltpu.VMEM((1, width), full),
            pltpu.VMEM(mixer_in.shape, half),
            dma((parts + 2,)),
            dma((parts + 1,)),
        ],
        compiler_params=pltpu.CompilerParams(vmem_limit_bytes=60 * 1024 * 1024),
    )(projected, routed, mix_gain[None])


def mixer(full, mixer_in, pre_gain, conv_kernel, chan_gain, mix_gain):
    value_full, gate_full, out_full = full
    normed_mix = rms_scale(mixer_in, pre_gain).astype(jnp.bfloat16)
    value_pre = jnp.dot(normed_mix, value_full, preferred_element_type=jnp.float32)
    gate_mix = jnp.dot(normed_mix, gate_full, preferred_element_type=jnp.float32)
    gated_rows = (value_pre * jax.nn.sigmoid(gate_mix)).astype(jnp.bfloat16)
    kernel_width = conv_kernel.shape[0]
    length = gated_rows.shape[0]
    rim_rows = passed_along(gated_rows[length - (kernel_width - 1) :], ("ep", "tp"), 1)
    padded = jnp.concatenate([rim_rows, gated_rows], axis=0).astype(jnp.float32)
    conv_sum = jnp.zeros((length, gated_rows.shape[1]), jnp.float32)
    for offset in range(kernel_width):
        conv_sum = conv_sum + conv_kernel[offset] * padded[offset : offset + length]
    row_mean = jnp.mean(conv_sum, axis=-1, keepdims=True)
    centred = conv_sum - row_mean
    row_var = jnp.mean(centred * centred, axis=-1, keepdims=True)
    activated = jax.nn.silu(centred * lax.rsqrt(row_var + LAYER_EPSILON) * chan_gain).astype(
        jnp.bfloat16
    )
    projected = jnp.dot(activated, out_full, preferred_element_type=jnp.float32)
    mixed = rms_scale(projected, mix_gain).astype(jnp.bfloat16)
    return mixed


def on_device(
    mixer_in,
    pre_gain,
    glu_value,
    glu_gate,
    conv_kernel,
    chan_gain,
    out_weight,
    mix_gain,
    expert_in,
    ffn_gain,
    routing,
    route_weight,
    gate_proj,
    up_proj,
    down_proj,
    expert_gain,
):
    groups_ep = lax.axis_size("ep")
    local_experts = gate_proj.shape[0]
    experts = local_experts * groups_ep
    token_rows, top_count = routing.shape
    capacity = max(2, 3 * token_rows * top_count // (2 * experts))
    slots = -(-local_experts * capacity // 8) * 8
    chips = lax.axis_size("tp") // 2
    lined_up = all(w.shape[1] % 128 == 0 for w in (glu_value, glu_gate, out_weight))
    two_way = groups_ep == 4 and chips > 1 and chips & (chips - 1) == 0
    if lined_up and two_way and groups_ep * slots <= 256:
        return tuple(
            fused(
                mixer_in,
                pre_gain,
                glu_value,
                glu_gate,
                conv_kernel,
                chan_gain,
                out_weight,
                mix_gain,
                expert_in,
                ffn_gain,
                routing,
                route_weight,
                gate_proj,
                up_proj,
                down_proj,
                expert_gain,
                capacity,
                slots,
            )
        )
    flat_route = routing.reshape(-1)
    onehot = (flat_route[:, None] == jnp.arange(experts, dtype=jnp.int32)[None, :]).astype(
        jnp.int32
    )
    before = jnp.cumsum(onehot, axis=0) - onehot
    rank_within = jnp.sum(before * onehot, axis=1)
    slot_index = (
        flat_route // local_experts * slots + flat_route % local_experts * capacity + rank_within
    ).reshape(token_rows, top_count)
    slot_ids = jnp.arange(groups_ep * slots, dtype=jnp.int32)
    chosen = slot_index[None, :, :] == slot_ids[:, None, None]
    pick_matrix = jnp.sum(chosen.astype(jnp.float32), axis=2).astype(jnp.bfloat16)
    normed_exp = rms_scale(expert_in, ffn_gain).astype(jnp.bfloat16)
    outgoing = jnp.dot(pick_matrix, normed_exp, preferred_element_type=jnp.float32).astype(
        jnp.bfloat16
    )
    full, mixed, returned = exchange(
        mixer_in,
        pre_gain,
        conv_kernel,
        chan_gain,
        mix_gain,
        outgoing,
        glu_value,
        glu_gate,
        out_weight,
        gate_proj,
        up_proj,
        down_proj,
        capacity,
    )
    if mixed is None:
        mixed = mixer(full, mixer_in, pre_gain, conv_kernel, chan_gain, mix_gain)
    combined = jnp.zeros((token_rows, returned.shape[1]), jnp.float32)
    for column in range(top_count):
        combined = combined + route_weight[:, column][:, None] * returned[
            slot_index[:, column]
        ].astype(jnp.float32)
    routed = rms_scale(combined, expert_gain).astype(jnp.bfloat16)
    return (mixed, routed)


def solution(mesh):
    in_specs = (
        P(("ep", "tp"), None),
        P(),
        P(None, "tp"),
        P(None, "tp"),
        P(),
        P(),
        P(None, "tp"),
        P(),
        P(("ep", "tp"), None),
        P(),
        P(("ep", "tp"), None),
        P(("ep", "tp"), None),
        P("ep", None, "tp"),
        P("ep", None, "tp"),
        P("ep", "tp", None),
        P(),
    )
    out_specs = (P(("ep", "tp"), None), P(("ep", "tp"), None))
    return jax.shard_map(
        on_device, mesh=mesh, in_specs=in_specs, out_specs=out_specs, check_vma=False
    )
```
